32 devices in a mesh: sp: 8 (over z, x), tp: 4 (over y, core).
Axes of the slice: x: 2, y: 2, z: 4, core: 2. Of those that a mesh axis runs over, the one named last changes fastest.
Arguments:
- tokens: bfloat16 [2048, 4096], P('sp', 'tp'), may hold values from -6 to 6
- pre_gain: float32 [4096], replicated, may hold values from 0.1 to 1.9
- rate_factor: float32 [2048], P('sp'), may hold values from 0.5 to 2, as said below
- w_rec_in: bfloat16 [4096, 1024], P(None, 'tp'), may hold values from -0.09375 to 0.09375
- w_rec_gate: bfloat16 [4096, 1024], P(None, 'tp')
- conv_taps: float32 [4, 1024], P(None, 'tp'), may hold values from -3 to 3
- rate_maps: bfloat16 [8, 128, 128], P('tp'), may hold values from -0.5 to 0.5
- input_maps: bfloat16 [8, 128, 128], P('tp'), may hold values from -0.5 to 0.5
- decay_param: float32 [1024], P('tp'), as said below
- w_query: bfloat16 [4096, 1536], P(None, 'tp'), may hold values from -0.09375 to 0.09375
- w_latent: bfloat16 [4096, 512], replicated, may hold values from -0.09375 to 0.09375
- w_rope_key: bfloat16 [4096, 64], replicated, may hold values from -0.09375 to 0.09375
- latent_gain: float32 [512], replicated, may hold values from 0.7 to 100, as said below
- w_expand: bfloat16 [512, 2048], P(None, 'tp')
- rec_gain: float32 [1024], P('tp'), may hold values from 0.1 to 1.9
- att_gain: float32 [1024], P('tp'), may hold values from 0.1 to 1.9
- w_out_rec: bfloat16 [1024, 4096], P('tp'), may hold values from -0.125 to 0.125
- w_out_att: bfloat16 [1024, 4096], P('tp'), may hold values from -0.125 to 0.125
- post_gain: float32 [4096], replicated, may hold values from 0.1 to 1.9
Outputs:
- layer_out: bfloat16 [2048, 4096], P(('sp', 'tp'))
The draws below stay inside these ranges and needn't reach their ends.
Inputs may be any that keep to these rules, and one draw needn't show every extreme that they name: `rate_factor`: one positive factor for each position. `decay_param`: one parameter for each recurrent channel. `latent_gain`: one positive gain for each latent entry.
All inputs are finite; a program needn't handle non-finite values.
Results may differ from the reference program's by a relative error of at most 0.017.
The reference program's roundings to bfloat16 on the way count: a program that leaves them out, or rounds other values in their place, can miss the bound.
Values may be sent and summed in bfloat16 or wider, within the bound.
A program may use at most 128 MiB of HBM per device.

```python
import math
import jax
import jax.numpy as jnp
from jax import lax

D = 4096
LRU_W = 1024
LRU_BLK = 128
CONV = 4
HEADS = 8
NOPE = 128
ROPE = 64
VDIM = 128
LATENT = 512
TOK_DEV = 256
SEQ = 2048
N_TP = 4


def draw_rate_factor(key, part):
    span_rows = max(TOK_DEV // 2, 1)
    levels = jnp.exp(jax.random.uniform(key, (SEQ // span_rows,), jnp.float32, math.log(0.5), math.log(2.0)))
    return jnp.repeat(levels, span_rows, total_repeat_length=SEQ)


def draw_decay_param(key, part):
    choose_key, slow_key, fast_key = jax.random.split(key, 3)
    share = 0.5
    slow_mask = jax.random.uniform(choose_key, (LRU_W,), jnp.float32) < share
    slow_value = math.log(8.0 * SEQ) + jax.random.uniform(slow_key, (LRU_W,), jnp.float32, 0.5, 2.0)
    fast_value = jax.random.uniform(fast_key, (LRU_W,), jnp.float32, 4.5, 6.0)
    return jnp.where(slow_mask, slow_value, fast_value)


def draw_latent_gain(key, part):
    return jax.random.uniform(key, (LATENT,), jnp.float32, 0.7, 1.3)


def draw_w_rec_gate(key, part):
    base_key, factor_key = jax.random.split(key)
    base = jax.random.normal(base_key, (D, LRU_W), jnp.float32) / math.sqrt(D)
    factors = jnp.exp(jax.random.uniform(factor_key, (LRU_W // LRU_BLK,), jnp.float32, math.log(1.0 / 3.0), math.log(3.0)))
    return (base * jnp.repeat(factors, LRU_BLK, total_repeat_length=LRU_W)[None, :]).astype(jnp.bfloat16)


def draw_w_expand(key, part):
    base_key, factor_key = jax.random.split(key)
    base = jax.random.normal(base_key, (LATENT, HEADS, NOPE + VDIM), jnp.float32) / math.sqrt(LATENT)
    factors = jnp.exp(jax.random.uniform(factor_key, (HEADS,), jnp.float32, math.log(1.0 / 3.0), math.log(3.0)))
    columns = jnp.arange(NOPE + VDIM)
    scaling = jnp.where(columns[None, :] >= NOPE, factors[:, None], 1.0)
    return (base * scaling[None, :, :]).reshape(LATENT, HEADS * (NOPE + VDIM)).astype(jnp.bfloat16)


def level_of(own_key, dims, cuts, low, high):
    level = 1.0
    for dim, shards_of in cuts:
        steps = jax.random.uniform(jax.random.fold_in(jax.random.fold_in(own_key, 6), dim), (shards_of,), jnp.float32, low / len(cuts), high / len(cuts))
        level = level * jnp.repeat(jnp.exp(steps), dims[dim] // shards_of).reshape((-1,) + (1,) * (len(dims) - 1 - dim))
    return level


def scatter_about(stream_key, shape, width, reach, shards=(), held_as=jnp.bfloat16):
    drawn = jax.random.normal(stream_key, shape, jnp.float32) * width
    if len(shards) > 0:
        drawn = level_of(stream_key, shape, shards, -0.22, 0.18) * drawn
    return jnp.clip(drawn, min=-reach, max=reach).astype(held_as)


def setup_inputs(seed: int = 0) -> dict:
    key_list = jax.random.split(jax.random.key(seed), 20)
    tokens = scatter_about(key_list[0], (SEQ, D), 1.0, 6.0, ((0, 8), (1, 4)))
    pre_gain = jnp.clip(1.0 + 0.18 * jax.random.normal(key_list[1], (D,), jnp.float32), 0.1, 1.9)
    rate_factor = draw_rate_factor(jax.random.fold_in(key_list[19], 71), 0)
    w_rec_in = scatter_about(key_list[3], (D, LRU_W), D ** -0.5, 0.09375, ((1, 4),))
    w_rec_gate = draw_w_rec_gate(jax.random.fold_in(key_list[19], 71), 0)
    conv_taps = scatter_about(key_list[5], (CONV, LRU_W), 0.5, 3.0, ((1, 4),), jnp.float32)
    rate_maps = scatter_about(key_list[6], (LRU_W // LRU_BLK, LRU_BLK, LRU_BLK), LRU_BLK ** -0.5, 0.5, ((0, 4),))
    input_maps = scatter_about(key_list[7], (LRU_W // LRU_BLK, LRU_BLK, LRU_BLK), LRU_BLK ** -0.5, 0.5, ((0, 4),))
    decay_param = draw_decay_param(jax.random.fold_in(key_list[19], 71), 0)
    w_query = scatter_about(key_list[9], (D, HEADS * (NOPE + ROPE)), D ** -0.5, 0.09375, ((1, 4),))
    w_latent = scatter_about(key_list[10], (D, LATENT), D ** -0.5, 0.09375)
    w_rope_key = scatter_about(key_list[11], (D, ROPE), D ** -0.5, 0.09375)
    latent_gain = draw_latent_gain(jax.random.fold_in(key_list[19], 71), 0)
    w_expand = draw_w_expand(jax.random.fold_in(key_list[19], 71), 0)
    rec_gain = jnp.clip(1.0 + 0.18 * jax.random.normal(key_list[14], (LRU_W,), jnp.float32), 0.1, 1.9)
    att_gain = jnp.clip(1.0 + 0.18 * jax.random.normal(key_list[15], (HEADS * VDIM,), jnp.float32), 0.1, 1.9)
    w_out_rec = scatter_about(key_list[16], (LRU_W, D), (LRU_W + HEADS * VDIM) ** -0.5, 0.125, ((0, 4),))
    w_out_att = scatter_about(key_list[17], (HEADS * VDIM, D), (LRU_W + HEADS * VDIM) ** -0.5, 0.125, ((0, 4),))
    post_gain = jnp.clip(1.0 + 0.18 * jax.random.normal(key_list[18], (D,), jnp.float32), 0.1, 1.9)
    return {"tokens": tokens, "pre_gain": pre_gain, "rate_factor": rate_factor, "w_rec_in": w_rec_in, "w_rec_gate": w_rec_gate, "conv_taps": conv_taps, "rate_maps": rate_maps, "input_maps": input_maps, "decay_param": decay_param, "w_query": w_query, "w_latent": w_latent, "w_rope_key": w_rope_key, "latent_gain": latent_gain, "w_expand": w_expand, "rec_gain": rec_gain, "att_gain": att_gain, "w_out_rec": w_out_rec, "w_out_att": w_out_att, "post_gain": post_gain}


EPS = 1e-06
RATE_C = 8.0
THETA = 10000.0

def rms_inverse(values):
    return lax.rsqrt(lax.optimization_barrier(jnp.mean(values * values, axis=-1, keepdims=True)) + EPS)

def rotate(values, cosine, sine_part):
    half_width = values.shape[-1] // 2
    leading = values[..., :half_width]
    trailing = values[..., half_width:]
    return jnp.concatenate([leading * cosine - trailing * sine_part, trailing * cosine + leading * sine_part], axis=-1)

def angles(length, offset, span_width):
    frequency = 1.0 / THETA ** (jnp.arange(0, span_width, 2).astype(jnp.float32) / span_width)
    places = (offset + jnp.arange(length).astype(jnp.int32)).astype(jnp.float32)
    turned = places[:, None] * frequency[None, :]
    return (jnp.cos(turned), jnp.sin(turned))

def combine_steps(earlier, later):
    return (earlier[0] * later[0], later[0] * earlier[1] + later[1])

def attend_block(state_now, query_nope, query_rope, places, keys_nope, key_rope, values, key_root):
    maxima, totals, accumulated = state_now
    scaling = 1.0 / math.sqrt(query_nope.shape[-1] + query_rope.shape[-1])
    scores = jnp.einsum('qhd,khd->hqk', query_nope.astype(jnp.float32), keys_nope.astype(jnp.float32))
    scores = scores + jnp.einsum('qhd,kd->hqk', query_rope.astype(jnp.float32), key_rope.astype(jnp.float32))
    scores = scores * scaling
    key_places = key_root + jnp.arange(keys_nope.shape[0]).astype(jnp.int32)
    visible = key_places[None, :] <= places[:, None]
    scores = jnp.where(visible[None], scores, -jnp.inf)
    largest = jnp.maximum(maxima, lax.optimization_barrier(jnp.max(scores, axis=-1)))
    anchor = jnp.where(largest == -jnp.inf, 0.0, largest)
    weights = jnp.exp(scores - anchor[..., None])
    shrink = jnp.exp(maxima - anchor)
    totals = totals * shrink + lax.optimization_barrier(jnp.sum(weights, axis=-1))
    rounded = weights.astype(jnp.bfloat16).astype(jnp.float32)
    accumulated = accumulated * shrink[..., None] + jnp.einsum('hqk,khd->hqd', rounded, values.astype(jnp.float32))
    return (largest, totals, accumulated)

def reference(tokens, pre_gain, rate_factor, w_rec_in, w_rec_gate, conv_taps, rate_maps, input_maps, decay_param, w_query, w_latent, w_rope_key, latent_gain, w_expand, rec_gain, att_gain, w_out_rec, w_out_att, post_gain):
    tokens_wide = tokens.astype(jnp.float32)
    inverse = rms_inverse(tokens_wide)
    scaled = (tokens_wide * pre_gain).astype(jnp.bfloat16)

    def project(weight):
        return inverse * jnp.dot(scaled, weight, preferred_element_type=jnp.float32)
    rec_input = project(w_rec_in).astype(jnp.bfloat16)
    gate_value = project(w_rec_gate)
    query_raw = project(w_query)
    latent_raw = project(w_latent)
    rope_raw = project(w_rope_key)
    padded = jnp.concatenate([jnp.zeros((CONV - 1, LRU_W), jnp.bfloat16), rec_input], axis=0)
    convolved = conv_taps[0] * padded[0:SEQ].astype(jnp.float32)
    for tap_index in range(1, CONV):
        convolved = convolved + conv_taps[tap_index] * padded[tap_index:tap_index + SEQ].astype(jnp.float32)
    conv_low = lax.optimization_barrier(convolved.astype(jnp.bfloat16)).astype(jnp.float32)
    blocks = conv_low.reshape(SEQ, LRU_W // LRU_BLK, LRU_BLK)
    rate_gate = jax.nn.sigmoid(jnp.einsum('sbi,bij->sbj', blocks, rate_maps.astype(jnp.float32))).reshape(SEQ, LRU_W)
    entry_gate = jax.nn.sigmoid(jnp.einsum('sbi,bij->sbj', blocks, input_maps.astype(jnp.float32))).reshape(SEQ, LRU_W)
    log_keep = -RATE_C * rate_factor[:, None] * rate_gate * jax.nn.softplus(-decay_param)
    keep_rate = jnp.exp(log_keep)
    driven = jnp.sqrt(-jnp.expm1(2.0 * log_keep)) * entry_gate * convolved
    state_seq = lax.associative_scan(combine_steps, (keep_rate, driven), axis=0)[1]
    rec_out = state_seq * jax.nn.gelu(gate_value)
    rec_norm = (rec_out * rms_inverse(rec_out) * rec_gain).astype(jnp.bfloat16)
    cosine, sine_part = angles(SEQ, 0, ROPE)
    query_heads = query_raw.reshape(SEQ, HEADS, NOPE + ROPE)
    query_nope = query_heads[:, :, :NOPE].astype(jnp.bfloat16)
    query_rope = rotate(query_heads[:, :, NOPE:], cosine[:, None, :], sine_part[:, None, :]).astype(jnp.bfloat16)
    latent_norm = (latent_raw * rms_inverse(latent_raw) * latent_gain).astype(jnp.bfloat16)
    rope_key = rotate(rope_raw, cosine, sine_part).astype(jnp.bfloat16)
    expanded = jnp.dot(latent_norm, w_expand, preferred_element_type=jnp.float32).astype(jnp.bfloat16)
    expanded = expanded.reshape(SEQ, HEADS, NOPE + VDIM)
    keys_nope = expanded[:, :, :NOPE]
    values = expanded[:, :, NOPE:]
    query_span = math.gcd(SEQ, 256)
    block_count = SEQ // query_span

    def one_block(block_index):
        root = block_index * query_span
        block_nope = lax.dynamic_slice_in_dim(query_nope, root, query_span, 0)
        block_rope = lax.dynamic_slice_in_dim(query_rope, root, query_span, 0)
        places = root + jnp.arange(query_span).astype(jnp.int32)
        initial = (jnp.full((HEADS, query_span), -jnp.inf, jnp.float32), jnp.zeros((HEADS, query_span), jnp.float32), jnp.zeros((HEADS, query_span, VDIM), jnp.float32))
        maxima, totals, accumulated = attend_block(initial, block_nope, block_rope, places, keys_nope, rope_key, values, 0)
        return (accumulated / totals[..., None]).transpose(1, 0, 2)
    att_out = lax.map(one_block, jnp.arange(block_count).astype(jnp.int32)).reshape(SEQ, HEADS * VDIM)
    att_norm = (att_out * rms_inverse(att_out) * att_gain).astype(jnp.bfloat16)
    rec_width = LRU_W // N_TP
    att_width = HEADS * VDIM // N_TP
    mixed_sum = jnp.zeros((SEQ, D), jnp.float32)
    for member in range(N_TP):
        partial_value = jnp.dot(rec_norm[:, member * rec_width:(member + 1) * rec_width], w_out_rec[member * rec_width:(member + 1) * rec_width], preferred_element_type=jnp.float32)
        partial_value = partial_value + jnp.dot(att_norm[:, member * att_width:(member + 1) * att_width], w_out_att[member * att_width:(member + 1) * att_width], preferred_element_type=jnp.float32)
        mixed_sum = mixed_sum + lax.optimization_barrier(partial_value.astype(jnp.bfloat16)).astype(jnp.float32)
    return (mixed_sum * rms_inverse(mixed_sum) * post_gain).astype(jnp.bfloat16)
```

```python
import functools
import math

import jax
import jax.numpy as jnp
from jax import lax
from jax.experimental import pallas as pl
from jax.experimental.pallas import tpu as pltpu
from jax.sharding import PartitionSpec as P

NOPE = 128
ROPE = 64
VDIM = 128
LANES = 128

EPS = 1e-06
RATE_C = 8.0
THETA = 10000.0
CHUNKS = 4
COLS = 4

MESH = pl.DeviceIdType.MESH
F32 = jnp.float32
BF16 = jnp.bfloat16


def one_minus_exp(y):
    series = 1.0 + y * (1.0 / 8.0)
    for order in (7, 6, 5, 4, 3, 2):
        series = 1.0 + y * (1.0 / order) * series
    return jnp.where(y > -0.5, -y * series, 1.0 - jnp.exp(y))


def gelu_tanh(x):
    inner = math.sqrt(2.0 / math.pi) * (x + 0.044715 * (x * x * x))
    return 0.5 * x * (1.0 + jnp.tanh(inner))


def softplus(x):
    z = jnp.exp(-jnp.abs(x))
    w = z / (2.0 + z)
    w2 = w * w
    series = jnp.full_like(w, 1.0 / 17.0)
    for order in (15, 13, 11, 9, 7, 5, 3):
        series = 1.0 / order + w2 * series
    return jnp.maximum(x, 0.0) + 2.0 * (w + w * w2 * series)


def rotate(tile, cosine, sine):
    lane = lax.broadcasted_iota(jnp.int32, tile.shape, 1)
    half = ROPE // 2
    other = jnp.where(
        lane < half, pltpu.roll(tile, tile.shape[1] - half, 1), pltpu.roll(tile, half, 1)
    )
    return tile * cosine + other * sine


def fused_kernel(
    n_sp, n_tp, heads,
    tokens, pre_gain, rate_factor, w_rec, w_gate, taps_in, rmap_in, imap_in, decay_in, w_query,
    w_latent, w_rope, lat_gain_in, w_expand, rec_gain_in, att_gain_in, w_or, w_oa, post_gain_in,
    cos_in, sin_in,
    out_ref,
    tok, scaled, gain, rate, wrec, wgate, taps, rmap, imap, decay, wq, wlat, wrope, lgain, wexp,
    rgain, again, wor, woa, pgain, cosv, sinv,
    acc_lat, acc_rope, acc_rec, acc_gate, acc_q, sq, kv, qcat, padded, gated,
    m_ref, l_ref, o_ref, a_ref, b_ref, rb, ab,
    tail_tx, tail_rx, carry_tx, carry_rx, sq_tx, sq_rx, inv_r, inv_a,
    pr, comb, d2d_tx, d2d_rx, y_tx, y_rx, mixed,
    load_sem, own_tx, own_rx, tok_tx, tok_rx, fwd_tx, fwd_rx,
    kvz_tx, kvx_tx, kv_rx, kvd_tx, kvd_rx,
    tail_s, carry_s, carry_r, sq_s, sq_r, d2d_s, d2d_r, y_s, y_r,
):
    me = lax.axis_index("sp")
    tp = lax.axis_index("tp")
    n_y = n_tp // 2
    levels = n_sp // 2
    core = lax.rem(tp, 2)
    yy = lax.div(tp, 2)
    partner = tp + 1 - 2 * core
    column = lax.rem(me, 2)
    level = lax.div(me, 2)
    neighbour = me + 1 - 2 * column
    rows, feats = tokens.shape
    width = feats * n_tp
    latent = w_latent.shape[1]
    channels = w_rec.shape[1]
    rc = rows // CHUNKS
    hc = rc // 2
    rd = rows // n_tp
    cb = width // COLS

    pairs = (
        (tokens, tok.at[tp]), (pre_gain, gain), (w_latent, wlat), (w_rope, wrope), (w_rec, wrec),
        (w_gate, wgate), (w_query, wq), (lat_gain_in, lgain), (cos_in, cosv), (sin_in, sinv),
        (rate_factor, rate), (taps_in, taps), (rmap_in, rmap), (imap_in, imap), (decay_in, decay),
        (rec_gain_in, rgain), (att_gain_in, again), (w_expand, wexp), (w_or, wor), (w_oa, woa),
        (post_gain_in, pgain),
    )
    loads = [pltpu.make_async_copy(s, d, load_sem.at[i]) for i, (s, d) in enumerate(pairs)]
    for copy in loads:
        copy.start()

    barrier = pltpu.get_barrier_semaphore()
    for d in range(1, n_sp):
        pl.semaphore_signal(
            barrier, inc=1, device_id={"sp": lax.rem(me + d, n_sp)}, device_id_type=MESH
        )
    for d in range(1, n_tp):
        pl.semaphore_signal(
            barrier, inc=1, device_id={"tp": lax.rem(tp + d, n_tp)}, device_id_type=MESH
        )
    acc_rope[...] = jnp.zeros_like(acc_rope)
    acc_q[...] = jnp.zeros_like(acc_q)
    pl.semaphore_wait(barrier, n_sp + n_tp - 2)
    loads[0].wait()

    def remote(src, dst, send, recv, **where):
        return pltpu.make_async_remote_copy(
            src_ref=src, dst_ref=dst, send_sem=send, recv_sem=recv, device_id=where,
            device_id_type=MESH,
        )

    def chunk(r):
        return pl.ds(pl.multiple_of(r * rc, rc), rc)

    def half(r):
        return pl.ds(pl.multiple_of(r * rc + core * hc, hc), hc)

    def own_copy():
        return remote(tok.at[tp], tok.at[tp], own_tx, own_rx, tp=partner)

    def tok_copy(dy, r):
        to = 2 * lax.rem(yy + dy, n_y) + core
        part = tok.at[tp, chunk(r)]
        return remote(part, part, tok_tx.at[dy, r], tok_rx.at[dy, r], tp=to)

    def fwd_copy(dy, r):
        part = tok.at[2 * lax.rem(yy + n_y - dy, n_y) + core, chunk(r)]
        return remote(part, part, fwd_tx.at[dy, r], fwd_rx.at[dy, r], tp=partner)

    for step in range(CHUNKS):
        for dy in range(1, n_y):
            tok_copy(dy, CHUNKS - 1 - step).start()
    own_copy().start()

    def dot(a, b):
        return jnp.dot(a, b, preferred_element_type=F32)

    def scale_rows(blk, first, count):
        span = min(count, 32)

        def body(i, _):
            at = pl.ds(pl.multiple_of(first + i * span, span), span)
            x = tok[blk, at, :].astype(F32)
            scaled[at, :] = (x * gain[blk]).astype(BF16)
            sq[at, :] += jnp.sum(x * x, axis=1, keepdims=True)
            return 0

        lax.fori_loop(0, count // span, body, 0)

    def project(blk, at, weights):
        k = pl.ds(pl.multiple_of(blk * feats, feats), feats)
        x = scaled[at, :]
        for w, acc in weights:
            n = w.shape[1]
            acc[at, :n] += dot(x, w[k, :])

    early = ((wlat, acc_lat), (wrope, acc_rope))
    late = ((wrec, acc_rec), (wgate, acc_gate), (wq, acc_q))

    sq[...] = jnp.zeros_like(sq)
    acc_lat[...] = jnp.zeros_like(acc_lat)
    acc_rec[...] = jnp.zeros_like(acc_rec)
    acc_gate[...] = jnp.zeros_like(acc_gate)
    for copy in loads[1:17]:
        copy.wait()
    everything = pl.ds(0, rows)

    def own_chip(i, _):
        @pl.when(i == 1)
        def _():
            own_copy().wait()

        blk = 2 * yy + lax.rem(core + i, 2)
        scale_rows(blk, 0, rows)
        project(blk, everything, early + late)
        return 0

    lax.fori_loop(0, 2, own_chip, 0)

    def kvz_copy(dz, r):
        part = kv.at[me, half(r)]
        return remote(part, part, kvz_tx.at[dz, r], kv_rx.at[me, r], sp=me + 2 * dz)

    def kvx_copy(s, r):
        part = kv.at[s, half(r)]
        return remote(part, part, kvx_tx.at[s, r], kv_rx.at[s, r], sp=neighbour)

    def kvd_copy(s, r):
        part = kv.at[s, half(r)]
        return remote(part, part, kvd_tx.at[s, r], kvd_rx.at[s, r], tp=partner)

    def forward_z(r):
        def body(dz, _):
            s = me - 2 * dz
            kvx_copy(s, r).wait_recv()
            kvx_copy(s, r).start()
            kvd_copy(s, r).start()
            return 0

        lax.fori_loop(1, level + 1, body, 0)

    def forward_x(r):
        def body(dz, _):
            s = neighbour - 2 * dz
            kvx_copy(s, r).wait_recv()
            kvd_copy(s, r).start()
            return 0

        lax.fori_loop(1 - column, level + 1, body, 0)

    def tok_step(step, _):
        r = CHUNKS - 1 - step
        at = chunk(r)
        for dy in range(1, n_y):
            tok_copy(dy, r).wait_recv()
            fwd_copy(dy, r).start()
        for dy in range(1, n_y):
            fwd_copy(dy, r).wait_recv()
        for dy in range(1, n_y):
            for b in range(2):
                blk = 2 * lax.rem(yy + n_y - dy, n_y) + b
                scale_rows(blk, r * rc, rc)
                project(blk, at, early + late)
        inverse = lax.rsqrt(sq[at, :] * (1.0 / width) + EPS)
        cosine = cosv[at, :]
        sine = sinv[at, :]
        raw = acc_lat[at, :] * inverse
        norm = raw * lax.rsqrt(jnp.mean(raw * raw, axis=1, keepdims=True) + EPS) * lgain[...]
        kv[me, at, :latent] = norm.astype(BF16)
        kv[me, at, latent:] = rotate(acc_rope[at, :] * inverse, cosine, sine).astype(BF16)
        for dz in range(1, levels):
            @pl.when(level + dz < levels)
            def _():
                kvz_copy(dz, r).start()

        @pl.when(column == 0)
        def _():
            kvx_copy(me, r).start()

        low = (acc_rec[at, :] * inverse).astype(BF16)
        padded[pl.ds(pl.multiple_of(r * rc + 8, 8), rc), :] = low.astype(F32)
        gated[at, :] = gelu_tanh(acc_gate[at, :] * inverse)
        query = acc_q[at, :] * inverse
        total = query.shape[1]
        for h in range(heads):
            start = h * (NOPE + ROPE)
            turned = query if start == 0 else pltpu.roll(query, total - start, 1)
            qcat[h, at, :NOPE] = turned[:, :NOPE].astype(BF16)
            qcat[h, at, NOPE:] = rotate(turned[:, NOPE : NOPE + LANES], cosine, sine).astype(BF16)

        @pl.when(step == 0)
        def _():
            tail_tx[...] = padded[rows : rows + 8, :]

            @pl.when(me + 1 < n_sp)
            def _():
                tail_copy().start()

        @pl.when(step > 0)
        def _():
            forward_z(r + 1)
            forward_x(r + 1)

        return 0

    def tail_copy():
        return remote(tail_tx, tail_rx, tail_s.at[0], tail_s.at[1], sp=me + 1)

    lax.fori_loop(0, CHUNKS, tok_step, 0)

    @pl.when(me > 0)
    def _():
        tail_copy().wait_recv()
        padded[0:8, :] = tail_rx[...]

    @pl.when(me == 0)
    def _():
        padded[0:8, :] = jnp.zeros((8, channels), F32)

    count = taps.shape[0]
    conv = taps[0:1, :] * padded[9 - count : 9 - count + rows, :]
    for k in range(1, count):
        conv = conv + taps[k : k + 1, :] * padded[9 - count + k : 9 - count + k + rows, :]
    low = conv.astype(BF16)
    bw = rmap.shape[1]
    rates, entries = [], []
    for b in range(rmap.shape[0]):
        part = low[:, b * bw : (b + 1) * bw]
        rates.append(dot(part, rmap[b]))
        entries.append(dot(part, imap[b]))
    rate_gate = jax.nn.sigmoid(jnp.concatenate(rates, axis=1))
    entry = jax.nn.sigmoid(jnp.concatenate(entries, axis=1))
    eye = lax.broadcasted_iota(jnp.int32, (rows, rows), 0) == lax.broadcasted_iota(
        jnp.int32, (rows, rows), 1
    )

    def to_column(row):
        return jnp.sum(jnp.where(eye, row, 0.0), axis=1, keepdims=True)

    def to_row(col):
        return jnp.sum(jnp.where(eye, col, 0.0), axis=0, keepdims=True)

    log_keep = -RATE_C * to_column(rate[...]) * rate_gate * softplus(-decay[...])
    a = jnp.exp(log_keep)
    b = jnp.sqrt(one_minus_exp(2.0 * log_keep)) * entry * conv
    row = lax.broadcasted_iota(jnp.int32, (rows, channels), 0)
    d = 1
    while d < rows:
        inside = row >= d
        b = a * jnp.where(inside, pltpu.roll(b, d, 0), 0.0) + b
        a = a * jnp.where(inside, pltpu.roll(a, d, 0), 1.0)
        d *= 2
    a_ref[...] = a
    b_ref[...] = b
    carry_tx[...] = jnp.zeros_like(carry_tx)
    carry_tx[0:1, :] = a[rows - 1 :, :]
    carry_tx[1:2, :] = b[rows - 1 :, :]

    def carry_copy(d):
        return remote(
            carry_tx, carry_rx.at[me], carry_s.at[d], carry_r.at[me], sp=me + d
        )

    def carry_start(d, _):
        carry_copy(d).start()
        return 0

    lax.fori_loop(1, n_sp - me, carry_start, 0)

    forward_z(0)

    root = 1.0 / math.sqrt(NOPE + ROPE)

    def attend(s, diagonal):
        expanded = dot(kv[s, :, :latent], wexp[...]).astype(BF16)
        rope = kv[s, :, latent:]
        for h in range(heads):
            at = h * (NOPE + VDIM)
            keys = jnp.concatenate([expanded[:, at : at + NOPE], rope], axis=1)
            values = expanded[:, at + NOPE : at + NOPE + VDIM]
            scores = lax.dot_general(
                qcat[h], keys, (((1,), (1,)), ((), ())), preferred_element_type=F32
            ) * root
            if diagonal:
                q_at = lax.broadcasted_iota(jnp.int32, scores.shape, 0)
                k_at = lax.broadcasted_iota(jnp.int32, scores.shape, 1)
                scores = jnp.where(k_at <= q_at, scores, -jnp.inf)
                top = jnp.max(scores, axis=1, keepdims=True)
            else:
                old = m_ref[h]
                top = jnp.maximum(old, jnp.max(scores, axis=1, keepdims=True))
                shrink = jnp.exp(old - top)
            weights = jnp.exp(scores - top)
            total = jnp.sum(weights, axis=1, keepdims=True)
            mixed_values = dot(weights.astype(BF16), values)
            m_ref[h] = top
            if diagonal:
                l_ref[h] = total
                o_ref[h] = mixed_values
            else:
                l_ref[h] = l_ref[h] * shrink + total
                o_ref[h] = o_ref[h] * shrink + mixed_values

    for copy in loads[17:]:
        copy.wait()
    attend(me, True)
    forward_x(0)

    def earlier(j, _):
        s = me - j
        for r in range(CHUNKS):
            kvd_copy(s, r).wait_recv()
        attend(s, False)
        return 0

    lax.fori_loop(1, me + 1, earlier, 0)

    def join(s, carried):
        remote(carry_tx, carry_rx.at[s], carry_s.at[0], carry_r.at[s], sp=neighbour).wait_recv()
        return carry_rx[s, 0:1, :] * carried + carry_rx[s, 1:2, :]

    carried = lax.fori_loop(0, me, join, jnp.zeros((1, channels), F32))
    rec_out = (b_ref[...] + a_ref[...] * carried) * gated[...]
    rb[...] = (rec_out * rgain[...]).astype(BF16)
    sq_tx[...] = jnp.zeros_like(sq_tx)
    sq_tx[0:1, :] = to_row(jnp.sum(rec_out * rec_out, axis=1, keepdims=True))
    att_sq = jnp.zeros((rows, 1), F32)
    for h in range(heads):
        att = o_ref[h] / l_ref[h]
        att_sq = att_sq + jnp.sum(att * att, axis=1, keepdims=True)
        at = slice(h * VDIM, (h + 1) * VDIM)
        ab[:, at] = (att * again[:, at]).astype(BF16)
    sq_tx[1:2, :] = to_row(att_sq)

    def sq_copy(d):
        return remote(
            sq_tx, sq_rx.at[d], sq_s.at[d], sq_r.at[d], tp=lax.rem(tp + d, n_tp)
        )

    for d in range(1, n_tp):
        sq_copy(d).start()
    sums = sq_tx[...]
    for d in range(1, n_tp):
        sq_copy(d).wait_recv()
        sums = sums + sq_rx[d]
    scale = lax.rsqrt(sums * (1.0 / (channels * n_tp)) + EPS)
    inv_r[...] = to_column(scale[0:1, :])
    scale = lax.rsqrt(sums * (1.0 / (heads * VDIM * n_tp)) + EPS)
    inv_a[...] = to_column(scale[1:2, :])

    def d2d_copy(dy, c):
        return remote(
            d2d_tx.at[dy, c], d2d_rx.at[dy, c], d2d_s.at[dy, c], d2d_r.at[dy, c], tp=partner
        )

    def y_copy(dy, c):
        to = 2 * lax.rem(yy + dy, n_y) + core
        return remote(y_tx.at[dy, c], y_rx.at[dy, c], y_s.at[dy, c], y_r.at[dy, c], tp=to)

    def produce(dy, c):
        first = pl.multiple_of(2 * rd * lax.rem(yy + dy, n_y), 2 * rd)
        at = pl.ds(first, 2 * rd)
        cols = pl.ds(pl.multiple_of(c * cb, cb), cb)
        pr[...] = dot(rb[at, :], wor[:, cols]) * inv_r[at, :] + dot(
            ab[at, :], woa[:, cols]
        ) * inv_a[at, :]
        theirs = pl.ds(pl.multiple_of((1 - core) * rd, rd), rd)
        mine = pl.ds(pl.multiple_of(core * rd, rd), rd)
        d2d_tx[dy, c] = pr[theirs, :].astype(BF16)
        d2d_copy(dy, c).start()
        comb[dy, c] = pr[mine, :]

    def send_pair(dy, c):
        d2d_copy(dy, c).wait_recv()
        y_tx[dy, c] = (comb[dy, c] + d2d_rx[dy, c].astype(F32)).astype(BF16)
        y_copy(dy, c).start()

    for dy in range(1, n_y):
        def away(c, _):
            @pl.when(c < COLS)
            def _():
                produce(dy, c)

            @pl.when(c > 0)
            def _():
                send_pair(dy, c - 1)

            return 0

        lax.fori_loop(0, COLS + 1, away, 0)

    def home(c, _):
        produce(0, c)
        return 0

    lax.fori_loop(0, COLS, home, 0)

    def gather(c, total):
        d2d_copy(0, c).wait_recv()
        value = comb[0, c] + d2d_rx[0, c].astype(F32)
        for dy in range(1, n_y):
            y_copy(dy, c).wait_recv()
            value = value + y_rx[dy, c].astype(F32)
        mixed[c] = value
        return total + jnp.sum(value * value, axis=1, keepdims=True)

    total = lax.fori_loop(0, COLS, gather, jnp.zeros((rd, 1), F32))
    last = lax.rsqrt(total * (1.0 / width) + EPS)

    for c in range(COLS):
        at = slice(c * cb, (c + 1) * cb)
        out_ref[:, at] = (mixed[c] * last * pgain[:, at]).astype(BF16)

    def drain(r, _):
        for dy in range(1, n_y):
            tok_copy(dy, r).wait_send()
            fwd_copy(dy, r).wait_send()
        for dz in range(1, levels):
            @pl.when(level + dz < levels)
            def _():
                kvz_copy(dz, r).wait_send()

        @pl.when(column == 0)
        def _():
            kvx_copy(me, r).wait_send()

        def sent_z(dz, _):
            kvx_copy(me - 2 * dz, r).wait_send()
            kvd_copy(me - 2 * dz, r).wait_send()
            return 0

        lax.fori_loop(1, level + 1, sent_z, 0)

        def sent_x(dz, _):
            kvd_copy(neighbour - 2 * dz, r).wait_send()
            return 0

        lax.fori_loop(1 - column, level + 1, sent_x, 0)
        return 0

    lax.fori_loop(0, CHUNKS, drain, 0)

    @pl.when(me + 1 < n_sp)
    def _():
        tail_copy().wait_send()

    def carry_done(d, _):
        carry_copy(d).wait_send()
        return 0

    lax.fori_loop(1, n_sp - me, carry_done, 0)
    for d in range(1, n_tp):
        sq_copy(d).wait_send()

    def sums_done(c, _):
        for dy in range(n_y):
            d2d_copy(dy, c).wait_send()
            if dy > 0:
                y_copy(dy, c).wait_send()
        return 0

    lax.fori_loop(0, COLS, sums_done, 0)


def shards(
    tokens, pre_gain, rate_factor, w_rec_in, w_rec_gate, conv_taps, rate_maps, input_maps,
    decay_param, w_query, w_latent, w_rope_key, latent_gain, w_expand, rec_gain, att_gain,
    w_out_rec, w_out_att, post_gain,
):
    n_sp = lax.axis_size("sp")
    n_tp = lax.axis_size("tp")
    n_y = n_tp // 2
    rows, feats = tokens.shape
    width = feats * n_tp
    channels = w_rec_in.shape[1]
    latent = w_latent.shape[1]
    q_cols = w_query.shape[1]
    heads = q_cols // (NOPE + ROPE)
    q_pad = -(-q_cols // LANES) * LANES
    rd = rows // n_tp
    cb = width // COLS

    lane = jnp.arange(LANES)
    frequency = 1.0 / THETA ** ((2 * (lane % (ROPE // 2))).astype(F32) / ROPE)
    places = (lax.axis_index("sp") * rows + jnp.arange(rows)).astype(F32)
    turned = places[:, None] * frequency[None, :]
    cosine = jnp.where(lane < ROPE, jnp.cos(turned), 0.0)
    sine = jnp.sin(turned) * jnp.where(lane < ROPE // 2, -1.0, jnp.where(lane < ROPE, 1.0, 0.0))

    def row(v):
        return v.reshape(1, -1)

    args = (
        tokens, pre_gain.reshape(n_tp, 1, feats), row(rate_factor), w_rec_in, w_rec_gate,
        conv_taps, rate_maps, input_maps, row(decay_param), w_query, w_latent, w_rope_key,
        row(latent_gain), w_expand, row(rec_gain), row(att_gain), w_out_rec, w_out_att,
        row(post_gain), cosine, sine,
    )
    vm = pltpu.VMEM
    dma = pltpu.SemaphoreType.DMA

    def like(x):
        return vm(x.shape, x.dtype)

    scratch = [
        vm((n_tp, rows, feats), BF16), vm((rows, feats), BF16), like(args[1]), like(args[2]),
        like(args[3]), like(args[4]), like(args[5]), like(args[6]), like(args[7]), like(args[8]),
        like(args[9]), like(args[10]), like(args[11]), like(args[12]), like(args[13]),
        like(args[14]), like(args[15]), like(args[16]), like(args[17]), like(args[18]),
        like(args[19]), like(args[20]),
        vm((rows, latent), F32), vm((rows, LANES), F32), vm((rows, channels), F32),
        vm((rows, channels), F32), vm((rows, q_pad), F32), vm((rows, 1), F32),
        vm((n_sp, rows, latent + LANES), BF16), vm((heads, rows, NOPE + LANES), BF16),
        vm((rows + 8, channels), F32), vm((rows, channels), F32),
        vm((heads, rows, 1), F32), vm((heads, rows, 1), F32), vm((heads, rows, VDIM), F32),
        vm((rows, channels), F32), vm((rows, channels), F32),
        vm((rows, channels), BF16), vm((rows, heads * VDIM), BF16),
        vm((8, channels), F32), vm((8, channels), F32), vm((8, channels), F32),
        vm((n_sp, 8, channels), F32), vm((8, rows), F32), vm((n_tp, 8, rows), F32),
        vm((rows, 1), F32), vm((rows, 1), F32),
        vm((2 * rd, cb), F32), vm((n_y, COLS, rd, cb), F32), vm((n_y, COLS, rd, cb), BF16),
        vm((n_y, COLS, rd, cb), BF16), vm((n_y, COLS, rd, cb), BF16),
        vm((n_y, COLS, rd, cb), BF16), vm((COLS, rd, cb), F32),
        dma((len(args),)), dma, dma, dma((n_y, CHUNKS)), dma((n_y, CHUNKS)),
        dma((n_y, CHUNKS)), dma((n_y, CHUNKS)),
        dma((n_sp // 2, CHUNKS)), dma((n_sp, CHUNKS)), dma((n_sp, CHUNKS)),
        dma((n_sp, CHUNKS)), dma((n_sp, CHUNKS)),
        dma((2,)), dma((n_sp,)), dma((n_sp,)), dma((n_tp,)), dma((n_tp,)),
        dma((n_y, COLS)), dma((n_y, COLS)), dma((n_y, COLS)), dma((n_y, COLS)),
    ]
    return pl.pallas_call(
        functools.partial(fused_kernel, n_sp, n_tp, heads),
        out_shape=jax.ShapeDtypeStruct((rd, width), BF16),
        in_specs=[pl.BlockSpec(memory_space=pl.ANY)] * len(args),
        out_specs=pl.BlockSpec(memory_space=pltpu.VMEM),
        scratch_shapes=scratch,
        compiler_params=pltpu.CompilerParams(
            collective_id=0, has_side_effects=True, vmem_limit_bytes=67043328
        ),
        name="layer",
    )(*args)


def solution(mesh):
    placed = (
        P("sp", "tp"),
        P(),
        P("sp"),
        P(None, "tp"),
        P(None, "tp"),
        P(None, "tp"),
        P("tp", None, None),
        P("tp", None, None),
        P("tp"),
        P(None, "tp"),
        P(),
        P(),
        P(),
        P(None, "tp"),
        P("tp"),
        P("tp"),
        P("tp", None),
        P("tp", None),
        P(),
    )
    return jax.shard_map(
        shards, mesh=mesh, in_specs=placed, out_specs=P(("sp", "tp"), None), check_vma=False
    )
```

```python
import functools
import math

import jax
import jax.numpy as jnp
import numpy as np
from jax import lax
from jax.experimental import pallas as pl
from jax.experimental.pallas import tpu as pltpu
from jax.sharding import PartitionSpec as P

NOPE = 128
ROPE = 64
VDIM = 128
LANES = 128

EPS = 1e-06
RATE_C = 8.0
THETA = 10000.0
CHUNKS = 4
BATCH = 4
COLS = 4

MESH = pl.DeviceIdType.MESH
F32 = jnp.float32
BF16 = jnp.bfloat16


def one_minus_exp(y):
    series = 1.0 + y * (1.0 / 8.0)
    for order in (7, 6, 5, 4, 3, 2):
        series = 1.0 + y * (1.0 / order) * series
    return jnp.where(y > -0.5, -y * series, 1.0 - jnp.exp(y))


def gelu_tanh(x):
    inner = math.sqrt(2.0 / math.pi) * (x + 0.044715 * (x * x * x))
    return 0.5 * x * (1.0 + jnp.tanh(inner))


def softplus(x):
    z = jnp.exp(-jnp.abs(x))
    w = z / (2.0 + z)
    w2 = w * w
    series = jnp.full_like(w, 1.0 / 17.0)
    for order in (15, 13, 11, 9, 7, 5, 3):
        series = 1.0 / order + w2 * series
    return jnp.maximum(x, 0.0) + 2.0 * (w + w * w2 * series)


def rotate(tile, cosine, sine):
    lane = lax.broadcasted_iota(jnp.int32, tile.shape, 1)
    half = ROPE // 2
    other = jnp.where(
        lane < half, pltpu.roll(tile, tile.shape[1] - half, 1), pltpu.roll(tile, half, 1)
    )
    return tile * cosine + other * sine


def fused_kernel(
    n_sp, n_tp, heads,
    tokens, pre_gain, rate_factor, w_rec, w_gate, taps_in, rmap_in, imap_in, decay_in, w_query,
    w_latent, w_rope, lat_gain_in, w_expand, rec_gain_in, att_gain_in, w_or, w_oa, post_gain_in,
    turns_in, starts_in,
    out_ref,
    tok, scaled, gain, rate, wrec, wgate, taps, rmap, imap, decay, wq, wlat, wrope, lgain, wexp,
    rgain, again, wor, woa, pgain, turns, starts,
    acc_lat, acc_rope, acc_rec, acc_gate, acc_q, sq, kv, qcat, padded, gated,
    m_ref, l_ref, o_ref, a_ref, b_ref, rb, ab,
    tail_tx, tail_rx, carry_tx, carry_rx, sq_tx, sq_rx, inv,
    prod, d2d_tx, d2d_rx, y_tx, y_rx, mixed,
    load_sem, weight_sem, own_tx, own_rx, tok_tx, tok_rx, fwd_tx, fwd_rx,
    kvz_tx, kvx_tx, kv_rx, kvd_tx, kvd_rx,
    tail_s, carry_s, carry_r, sq_s, sq_r, d2d_s, d2d_r, y_s, y_r,
):
    me = lax.axis_index("sp")
    tp = lax.axis_index("tp")
    n_y = n_tp // 2
    levels = n_sp // 2
    core = lax.rem(tp, 2)
    yy = lax.div(tp, 2)
    partner = tp + 1 - 2 * core
    column = lax.rem(me, 2)
    level = lax.div(me, 2)
    neighbour = me + 1 - 2 * column
    rows, feats = tokens.shape
    width = feats * n_tp
    latent = w_latent.shape[1]
    channels = w_rec.shape[1]
    rc = rows // CHUNKS
    hc = rc // 2
    rd = rows // n_tp
    cb = width // COLS

    small = (
        (tokens, tok.at[tp]), (pre_gain, gain), (lat_gain_in, lgain), (turns_in, turns),
        (starts_in, starts),
    )
    later = (
        (w_expand, wexp), (rate_factor, rate), (taps_in, taps), (rmap_in, rmap), (imap_in, imap),
        (decay_in, decay), (rec_gain_in, rgain), (att_gain_in, again), (w_or, wor), (w_oa, woa),
        (post_gain_in, pgain),
    )
    projections = ((w_latent, wlat), (w_rec, wrec), (w_gate, wgate), (w_query, wq))

    def loads_of(group, first):
        return [
            pltpu.make_async_copy(s, d, load_sem.at[first + i]) for i, (s, d) in enumerate(group)
        ]

    def features(blk):
        return pl.ds(pl.multiple_of(blk * feats, feats), feats)

    def weight_loads(blk):
        at = features(blk)
        copies = [pltpu.make_async_copy(w_rope.at[:, at], wrope.at[:, at], weight_sem.at[0, blk])]
        for i, (s, d) in enumerate(projections):
            copies.append(pltpu.make_async_copy(s.at[at], d.at[at], weight_sem.at[1 + i, blk]))
        return copies

    first_loads = loads_of(small, 0)
    last_loads = loads_of(later, len(small))
    for copy in first_loads:
        copy.start()
    for dy in range(n_y):
        for b in range(2):
            for copy in weight_loads(2 * lax.rem(yy + dy, n_y) + lax.rem(core + b, 2)):
                copy.start()

    barrier = pltpu.get_barrier_semaphore()
    for d in range(1, n_sp):
        pl.semaphore_signal(
            barrier, inc=1, device_id={"sp": lax.rem(me + d, n_sp)}, device_id_type=MESH
        )
    for d in range(1, n_tp):
        pl.semaphore_signal(
            barrier, inc=1, device_id={"tp": lax.rem(tp + d, n_tp)}, device_id_type=MESH
        )
    with jax.named_scope("entry"):
        for ref in (acc_lat, acc_rope, acc_rec, acc_gate, acc_q, sq):
            ref[...] = jnp.zeros_like(ref)

        def blank(s, _):
            kv[s] = jnp.zeros(kv.shape[1:], BF16)
            return 0

        lax.fori_loop(me + 1, lax.div(me + BATCH - 1, BATCH) * BATCH, blank, 0)
        pl.semaphore_wait(barrier, n_sp + n_tp - 2)
        first_loads[0].wait()

    def remote(src, dst, send, recv, **where):
        return pltpu.make_async_remote_copy(
            src_ref=src, dst_ref=dst, send_sem=send, recv_sem=recv, device_id=where,
            device_id_type=MESH,
        )

    def chunk(r):
        return pl.ds(pl.multiple_of(r * rc, rc), rc)

    def half(r):
        return pl.ds(pl.multiple_of(r * rc + core * hc, hc), hc)

    def own_copy():
        return remote(tok.at[tp], tok.at[tp], own_tx, own_rx, tp=partner)

    def tok_copy(dy, r):
        to = 2 * lax.rem(yy + dy, n_y) + core
        part = tok.at[tp, chunk(r)]
        return remote(part, part, tok_tx.at[dy, r], tok_rx.at[dy, r], tp=to)

    def fwd_copy(dy, r):
        part = tok.at[2 * lax.rem(yy + n_y - dy, n_y) + core, chunk(r)]
        return remote(part, part, fwd_tx.at[dy, r], fwd_rx.at[dy, r], tp=partner)

    for step in range(CHUNKS):
        for dy in range(1, n_y):
            tok_copy(dy, CHUNKS - 1 - step).start()
    own_copy().start()

    def dot(a, b):
        return jnp.dot(a, b, preferred_element_type=F32)

    def dot_t(a, b):
        return lax.dot_general(a, b, (((1,), (1,)), ((), ())), preferred_element_type=F32)

    def tiles(x):
        return [x[:, i : i + LANES] for i in range(0, x.shape[1], LANES)]

    def wide(x, count):
        return jnp.concatenate([x] * count, axis=1) if count > 1 else x

    @jax.named_scope("scale")
    def scale_rows(blk, first, count):
        span = min(count, 32)

        def body(i, _):
            at = pl.ds(pl.multiple_of(first + i * span, span), span)
            x = tok[blk, at, :].astype(F32)
            scaled[at, :] = (x * gain[blk]).astype(BF16)
            sq[at, :] += functools.reduce(jnp.add, tiles(x * x))
            return 0

        lax.fori_loop(0, count // span, body, 0)

    @jax.named_scope("early")
    def project_early(blk, at):
        k = features(blk)
        x = scaled[at, :]
        acc_rope[at, : wrope.shape[0]] += dot_t(x, wrope[:, k])
        acc_lat[at, :] += dot(x, wlat[k, :])

    @jax.named_scope("late")
    def project_late(blk, at):
        k = features(blk)
        x = scaled[at, :]
        for w, acc in ((wrec, acc_rec), (wgate, acc_gate), (wq, acc_q)):
            acc[at, : w.shape[1]] += dot(x, w[k, :])

    for copy in first_loads[1:]:
        copy.wait()
    everything = pl.ds(0, rows)

    def own_chip(i, _):
        blk = 2 * yy + lax.rem(core + i, 2)

        @pl.when(i == 1)
        def _():
            own_copy().wait()

        scale_rows(blk, 0, rows)
        with jax.named_scope("weights"):
            for copy in weight_loads(blk):
                copy.wait()
        project_early(blk, everything)
        project_late(blk, everything)
        return 0

    lax.fori_loop(0, 2, own_chip, 0)
    for copy in last_loads:
        copy.start()

    def kvz_copy(dz, r):
        part = kv.at[me, half(r)]
        return remote(part, part, kvz_tx.at[dz, r], kv_rx.at[me, r], sp=me + 2 * dz)

    def kvx_copy(s, r):
        part = kv.at[s, half(r)]
        return remote(part, part, kvx_tx.at[s, r], kv_rx.at[s, r], sp=neighbour)

    def kvd_copy(s, r):
        part = kv.at[s, half(r)]
        return remote(part, part, kvd_tx.at[s, r], kvd_rx.at[s, r], tp=partner)

    @jax.named_scope("fwdz")
    def forward_z(r, near, far):
        def body(dz, _):
            s = me - 2 * dz
            kvx_copy(s, r).wait_recv()
            kvx_copy(s, r).start()
            kvd_copy(s, r).start()
            return 0

        lax.fori_loop(near, jnp.minimum(far, level + 1), body, 0)

    @jax.named_scope("fwdx")
    def forward_x(r):
        def body(dz, _):
            s = neighbour - 2 * dz
            kvx_copy(s, r).wait_recv()
            kvd_copy(s, r).start()
            return 0

        lax.fori_loop(1 - column, level + 1, body, 0)

    def angles(at):
        lane = lax.broadcasted_iota(jnp.int32, (1, LANES), 1)
        kept = jnp.where(lane < ROPE, 1.0, 0.0)
        sign = jnp.where(lane < ROPE // 2, -1.0, kept)
        c, s = turns[0, at, :], turns[1, at, :]
        c0, s0 = starts[0, me], starts[1, me]
        return (c * c0 - s * s0) * kept, (s * c0 + c * s0) * sign

    def inverse_of(at):
        total = jnp.sum(sq[at, :], axis=1, keepdims=True)
        return lax.rsqrt(total * (1.0 / width) + EPS)

    @jax.named_scope("latent")
    def finish_latent(r, at):
        inverse = inverse_of(at)
        cosine, sine = angles(at)
        raw = acc_lat[at, :] * inverse
        norm = raw * lax.rsqrt(jnp.mean(raw * raw, axis=1, keepdims=True) + EPS) * lgain[...]
        kv[me, at, :latent] = norm.astype(BF16)
        kv[me, at, latent:] = rotate(acc_rope[at, :] * inverse, cosine, sine).astype(BF16)
        for dz in range(1, levels):
            @pl.when(level + dz < levels)
            def _():
                kvz_copy(dz, r).start()

        @pl.when(column == 0)
        def _():
            kvx_copy(me, r).start()

    def tok_step(step, _):
        r = CHUNKS - 1 - step
        at = chunk(r)
        with jax.named_scope("tokwait"):
            for dy in range(1, n_y):
                tok_copy(dy, r).wait_recv()
                fwd_copy(dy, r).start()

        for b in range(2):
            for dy in range(1, n_y):
                blk = 2 * lax.rem(yy + n_y - dy, n_y) + lax.rem(core + b, 2)
                if b == 1:
                    with jax.named_scope("fwdwait"):
                        fwd_copy(dy, r).wait_recv()
                scale_rows(blk, r * rc, rc)

                @pl.when(step == 0)
                def _():
                    for copy in weight_loads(blk):
                        copy.wait()

                project_early(blk, at)
                if b == 1 and dy == n_y - 1:
                    finish_latent(r, at)
                project_late(blk, at)

        with jax.named_scope("finish"):
            inverse = inverse_of(at)
            cosine, sine = angles(at)
            low = (acc_rec[at, :] * inverse).astype(BF16)
            padded[pl.ds(pl.multiple_of(r * rc + 8, 8), rc), :] = low.astype(F32)
            gated[at, :] = gelu_tanh(acc_gate[at, :] * inverse)
            query = acc_q[at, :] * inverse
            total = query.shape[1]
            for h in range(heads):
                start = h * (NOPE + ROPE)
                turned = query if start == 0 else pltpu.roll(query, total - start, 1)
                qcat[h, at, :NOPE] = turned[:, :NOPE].astype(BF16)
                qcat[h, at, NOPE:] = rotate(turned[:, NOPE : NOPE + LANES], cosine, sine).astype(BF16)

        @pl.when(step == 0)
        def _():
            tail_tx[...] = padded[rows : rows + 8, :]

            @pl.when(me + 1 < n_sp)
            def _():
                tail_copy().start()

        @pl.when(step > 0)
        def _():
            forward_z(r + 1, 1, 2)

        @pl.when(step > 1)
        def _():
            forward_z(r + 2, 2, levels)

        return 0

    def tail_copy():
        return remote(tail_tx, tail_rx, tail_s.at[0], tail_s.at[1], sp=me + 1)

    lax.fori_loop(0, CHUNKS, tok_step, 0)

    for copy in last_loads:
        copy.wait()

    @pl.when(me > 0)
    def _():
        tail_copy().wait_recv()
        padded[0:8, :] = tail_rx[...]

    @pl.when(me == 0)
    def _():
        padded[0:8, :] = jnp.zeros((8, channels), F32)

    mark = jax.named_scope("rec")
    mark.__enter__()
    count = taps.shape[0]
    conv = taps[0:1, :] * padded[9 - count : 9 - count + rows, :]
    for k in range(1, count):
        conv = conv + taps[k : k + 1, :] * padded[9 - count + k : 9 - count + k + rows, :]
    low = conv.astype(BF16)
    bw = rmap.shape[1]
    rates, entries = [], []
    for b in range(rmap.shape[0]):
        part = low[:, b * bw : (b + 1) * bw]
        rates.append(dot(part, rmap[b]))
        entries.append(dot(part, imap[b]))
    rate_gate = jax.nn.sigmoid(jnp.concatenate(rates, axis=1))
    entry = jax.nn.sigmoid(jnp.concatenate(entries, axis=1))
    eye = lax.broadcasted_iota(jnp.int32, (rows, rows), 0) == lax.broadcasted_iota(
        jnp.int32, (rows, rows), 1
    )

    def to_column(row):
        return jnp.sum(jnp.where(eye, row, 0.0), axis=1, keepdims=True)

    def to_row(col):
        return jnp.sum(jnp.where(eye, col, 0.0), axis=0, keepdims=True)

    log_keep = -RATE_C * to_column(rate[...]) * rate_gate * softplus(-decay[...])
    a = jnp.exp(log_keep)
    b = jnp.sqrt(one_minus_exp(2.0 * log_keep)) * entry * conv
    row = lax.broadcasted_iota(jnp.int32, (rows, channels), 0)
    d = 1
    while d < rows:
        inside = row >= d
        b = a * jnp.where(inside, pltpu.roll(b, d, 0), 0.0) + b
        a = a * jnp.where(inside, pltpu.roll(a, d, 0), 1.0)
        d *= 2
    a_ref[...] = a
    b_ref[...] = b
    carry_tx[...] = jnp.zeros_like(carry_tx)
    carry_tx[0:1, :] = a[rows - 1 :, :]
    carry_tx[1:2, :] = b[rows - 1 :, :]

    mark.__exit__(None, None, None)

    def carry_copy(d):
        return remote(
            carry_tx, carry_rx.at[me], carry_s.at[d], carry_r.at[me], sp=me + d
        )

    def carry_start(d, _):
        carry_copy(d).start()
        return 0

    lax.fori_loop(1, n_sp - me, carry_start, 0)

    forward_z(0, 1, 2)
    forward_z(1, 2, levels)

    root = 1.0 / math.sqrt(NOPE + ROPE)

    @jax.named_scope("attend")
    def attend(keys_latent, keys_rope, limit):
        expanded = dot(keys_latent, wexp[...]).astype(BF16)
        for h in range(heads):
            at = h * (NOPE + VDIM)
            keys = jnp.concatenate([expanded[:, at : at + NOPE], keys_rope], axis=1)
            values = expanded[:, at + NOPE : at + NOPE + VDIM]
            scores = dot_t(qcat[h], keys) * root
            k_at = lax.broadcasted_iota(jnp.int32, scores.shape, 1)
            if limit is None:
                limit_at = lax.broadcasted_iota(jnp.int32, scores.shape, 0) + 1
            else:
                limit_at = limit
            scores = tiles(jnp.where(k_at < limit_at, scores, -jnp.inf))
            top = jnp.max(functools.reduce(jnp.maximum, scores), axis=1, keepdims=True)
            if limit is not None:
                old = m_ref[h]
                top = jnp.maximum(old, top)
                shrink = jnp.exp(old - top)
            weights = [jnp.exp(x - top) for x in scores]
            total = functools.reduce(jnp.add, weights)
            found = dot(jnp.concatenate([x.astype(BF16) for x in weights], axis=1), values)
            if limit is not None:
                total = total + l_ref[h] * shrink
                found = found + o_ref[h] * shrink
            m_ref[h] = jnp.broadcast_to(top, m_ref.shape[1:])
            l_ref[h] = total
            o_ref[h] = found

    def attend_chunk(r):
        def ready(s, _):
            kvd_copy(s, r).wait_recv()
            return 0

        with jax.named_scope("kvwait"):
            lax.fori_loop(0, me, ready, 0)

        def group(g, _):
            several = pl.ds(g * BATCH, BATCH)
            count = BATCH * rc
            attend(
                kv[several, chunk(r), :latent].reshape(count, latent),
                kv[several, chunk(r), latent:].reshape(count, LANES),
                (me - g * BATCH) * rc,
            )
            return 0

        lax.fori_loop(0, lax.div(me + BATCH - 1, BATCH), group, 0)

    attend(kv[me, :, :latent], kv[me, :, latent:], None)
    forward_z(0, 2, levels)

    def sq_copy(kind, d):
        return remote(
            sq_tx.at[kind], sq_rx.at[kind, d], sq_s.at[kind, d], sq_r.at[kind, d],
            tp=lax.rem(tp + d, n_tp),
        )

    def share_squares(kind, column):
        sq_tx[kind] = jnp.broadcast_to(to_row(column), sq_tx.shape[1:])
        for d in range(1, n_tp):
            sq_copy(kind, d).start()

    @jax.named_scope("sums")
    def join_squares(kind, count):
        total = sq_tx[kind]
        for d in range(1, n_tp):
            sq_copy(kind, d).wait_recv()
            total = total + sq_rx[kind, d]
        scale = lax.rsqrt(total * (1.0 / count) + EPS)
        inv[kind] = jnp.broadcast_to(to_column(scale[0:1, :]), inv.shape[1:])

    @jax.named_scope("join")
    def finish_recurrence():
        def join(s, carried):
            remote(
                carry_tx, carry_rx.at[s], carry_s.at[0], carry_r.at[s], sp=neighbour
            ).wait_recv()
            return carry_rx[s, 0:1, :] * carried + carry_rx[s, 1:2, :]

        carried = lax.fori_loop(0, me, join, jnp.zeros((1, channels), F32))
        rec_out = (b_ref[...] + a_ref[...] * carried) * gated[...]
        rb[...] = (rec_out * rgain[...]).astype(BF16)
        share_squares(0, jnp.sum(rec_out * rec_out, axis=1, keepdims=True))

    def block(dy):
        return pl.ds(pl.multiple_of(2 * rd * lax.rem(yy + dy, n_y), 2 * rd), 2 * rd)

    def cols(c):
        return pl.ds(pl.multiple_of(c * cb, cb), cb)

    @jax.named_scope("recprod")
    def multiply(dy, c, left, right, add):
        at = block(dy)
        value = dot(left[at, :], right[:, cols(c)])
        if add:
            count = cb // LANES
            value = value * wide(inv[1, at, :], count) + prod[dy, c] * wide(inv[0, at, :], count)
        prod[dy, c] = value

    forward_x(CHUNKS - 1)
    forward_x(CHUNKS - 2)
    attend_chunk(CHUNKS - 1)
    for r in range(CHUNKS - 3, 0, -1):
        forward_x(r)
        attend_chunk(r + 1)
    finish_recurrence()
    attend_chunk(1)
    forward_x(0)

    for dy in range(n_y):
        def rec_product(c, _):
            multiply(dy, c, rb, wor, False)
            return 0

        lax.fori_loop(0, COLS, rec_product, 0)
    join_squares(0, channels * n_tp)
    attend_chunk(0)

    att_sq = jnp.zeros((rows, 1), F32)
    for h in range(heads):
        att = o_ref[h] / jnp.sum(l_ref[h], axis=1, keepdims=True)
        att_sq = att_sq + jnp.sum(att * att, axis=1, keepdims=True)
        at = slice(h * VDIM, (h + 1) * VDIM)
        ab[:, at] = (att * again[:, at]).astype(BF16)
    share_squares(1, att_sq)
    join_squares(1, heads * VDIM * n_tp)

    def d2d_copy(dy, c):
        return remote(
            d2d_tx.at[dy, c], d2d_rx.at[dy, c], d2d_s.at[dy, c], d2d_r.at[dy, c], tp=partner
        )

    def y_copy(dy, c):
        to = 2 * lax.rem(yy + dy, n_y) + core
        return remote(y_tx.at[dy, c], y_rx.at[dy, c], y_s.at[dy, c], y_r.at[dy, c], tp=to)

    @jax.named_scope("produce")
    def produce(dy, c):
        multiply(dy, c, ab, woa, True)
        theirs = pl.ds(pl.multiple_of((1 - core) * rd, rd), rd)
        d2d_tx[dy, c] = prod[dy, c, theirs, :].astype(BF16)
        d2d_copy(dy, c).start()

    def mine(dy, c):
        return prod[dy, c, pl.ds(pl.multiple_of(core * rd, rd), rd), :]

    @jax.named_scope("pair")
    def send_pair(dy, c):
        d2d_copy(dy, c).wait_recv()
        y_tx[dy, c] = (mine(dy, c) + d2d_rx[dy, c].astype(F32)).astype(BF16)
        y_copy(dy, c).start()

    for dy in range(1, n_y):
        def away(c, _):
            @pl.when(c < COLS)
            def _():
                produce(dy, c)

            @pl.when(c > 0)
            def _():
                send_pair(dy, c - 1)

            return 0

        lax.fori_loop(0, COLS + 1, away, 0)

    def home(c, _):
        produce(0, c)
        return 0

    lax.fori_loop(0, COLS, home, 0)

    @jax.named_scope("gather")
    def gather(c, total):
        d2d_copy(0, c).wait_recv()
        value = mine(0, c) + d2d_rx[0, c].astype(F32)
        for dy in range(1, n_y):
            y_copy(dy, c).wait_recv()
            value = value + y_rx[dy, c].astype(F32)
        mixed[c] = value
        return total + jnp.sum(value * value, axis=1, keepdims=True)

    total = lax.fori_loop(0, COLS, gather, jnp.zeros((rd, 1), F32))
    last = lax.rsqrt(total * (1.0 / width) + EPS)

    for c in range(COLS):
        at = slice(c * cb, (c + 1) * cb)
        out_ref[:, at] = (mixed[c] * last * pgain[:, at]).astype(BF16)

    @jax.named_scope("drain")
    def drain(r, _):
        for dy in range(1, n_y):
            tok_copy(dy, r).wait_send()
            fwd_copy(dy, r).wait_send()
        for dz in range(1, levels):
            @pl.when(level + dz < levels)
            def _():
                kvz_copy(dz, r).wait_send()

        @pl.when(column == 0)
        def _():
            kvx_copy(me, r).wait_send()

        def sent_z(dz, _):
            kvx_copy(me - 2 * dz, r).wait_send()
            kvd_copy(me - 2 * dz, r).wait_send()
            return 0

        lax.fori_loop(1, level + 1, sent_z, 0)

        def sent_x(dz, _):
            kvd_copy(neighbour - 2 * dz, r).wait_send()
            return 0

        lax.fori_loop(1 - column, level + 1, sent_x, 0)
        return 0

    lax.fori_loop(0, CHUNKS, drain, 0)

    @pl.when(me + 1 < n_sp)
    def _():
        tail_copy().wait_send()

    def carry_done(d, _):
        carry_copy(d).wait_send()
        return 0

    lax.fori_loop(1, n_sp - me, carry_done, 0)
    for kind in range(2):
        for d in range(1, n_tp):
            sq_copy(kind, d).wait_send()

    def sums_done(c, _):
        for dy in range(n_y):
            d2d_copy(dy, c).wait_send()
            if dy > 0:
                y_copy(dy, c).wait_send()
        return 0

    lax.fori_loop(0, COLS, sums_done, 0)


def shards(
    tokens, pre_gain, rate_factor, w_rec_in, w_rec_gate, conv_taps, rate_maps, input_maps,
    decay_param, w_query, w_latent, w_rope_key, latent_gain, w_expand, rec_gain, att_gain,
    w_out_rec, w_out_att, post_gain,
):
    n_sp = lax.axis_size("sp")
    n_tp = lax.axis_size("tp")
    n_y = n_tp // 2
    rows, feats = tokens.shape
    width = feats * n_tp
    channels = w_rec_in.shape[1]
    latent = w_latent.shape[1]
    q_cols = w_query.shape[1]
    heads = q_cols // (NOPE + ROPE)
    q_pad = -(-q_cols // LANES) * LANES
    rd = rows // n_tp
    cb = width // COLS

    lane = np.arange(LANES)
    frequency = np.where(lane < ROPE, THETA ** (-2.0 * (lane % (ROPE // 2)) / ROPE), 0.0)
    within = np.arange(rows)[:, None] * frequency
    start = rows * np.arange(n_sp)[:, None, None] * frequency
    turns = np.stack([np.cos(within), np.sin(within)]).astype(np.float32)
    starts = np.stack([np.cos(start), np.sin(start)]).astype(np.float32)

    def row(v):
        return v.reshape(1, -1)

    args = (
        tokens, pre_gain.reshape(n_tp, 1, feats), row(rate_factor), w_rec_in, w_rec_gate,
        conv_taps, rate_maps, input_maps, row(decay_param), w_query, w_latent, w_rope_key.T,
        row(latent_gain), w_expand, row(rec_gain), row(att_gain), w_out_rec, w_out_att,
        row(post_gain), jnp.asarray(turns), jnp.asarray(starts),
    )
    vm = pltpu.VMEM
    dma = pltpu.SemaphoreType.DMA

    def like(x):
        return vm(x.shape, x.dtype)

    scratch = [
        vm((n_tp, rows, feats), BF16), vm((rows, feats), BF16), like(args[1]), like(args[2]),
        like(args[3]), like(args[4]), like(args[5]), like(args[6]), like(args[7]), like(args[8]),
        like(args[9]), like(args[10]), like(args[11]), like(args[12]), like(args[13]),
        like(args[14]), like(args[15]), like(args[16]), like(args[17]), like(args[18]),
        like(args[19]), like(args[20]),
        vm((rows, latent), F32), vm((rows, LANES), F32), vm((rows, channels), F32),
        vm((rows, channels), F32), vm((rows, q_pad), F32), vm((rows, LANES), F32),
        vm((n_sp, rows, latent + LANES), BF16), vm((heads, rows, NOPE + LANES), BF16),
        vm((rows + 8, channels), F32), vm((rows, channels), F32),
        vm((heads, rows, LANES), F32), vm((heads, rows, LANES), F32), vm((heads, rows, VDIM), F32),
        vm((rows, channels), F32), vm((rows, channels), F32),
        vm((rows, channels), BF16), vm((rows, heads * VDIM), BF16),
        vm((8, channels), F32), vm((8, channels), F32), vm((8, channels), F32),
        vm((n_sp, 8, channels), F32), vm((2, 8, rows), F32), vm((2, n_tp, 8, rows), F32),
        vm((2, rows, LANES), F32),
        vm((n_y, COLS, 2 * rd, cb), F32), vm((n_y, COLS, rd, cb), BF16),
        vm((n_y, COLS, rd, cb), BF16), vm((n_y, COLS, rd, cb), BF16),
        vm((n_y, COLS, rd, cb), BF16), vm((COLS, rd, cb), F32),
        dma((len(args),)), dma((5, n_tp)), dma, dma, dma((n_y, CHUNKS)), dma((n_y, CHUNKS)),
        dma((n_y, CHUNKS)), dma((n_y, CHUNKS)),
        dma((n_sp // 2, CHUNKS)), dma((n_sp, CHUNKS)), dma((n_sp, CHUNKS)),
        dma((n_sp, CHUNKS)), dma((n_sp, CHUNKS)),
        dma((2,)), dma((n_sp,)), dma((n_sp,)), dma((2, n_tp)), dma((2, n_tp)),
        dma((n_y, COLS)), dma((n_y, COLS)), dma((n_y, COLS)), dma((n_y, COLS)),
    ]
    return pl.pallas_call(
        functools.partial(fused_kernel, n_sp, n_tp, heads),
        out_shape=jax.ShapeDtypeStruct((rd, width), BF16),
        in_specs=[pl.BlockSpec(memory_space=pl.ANY)] * len(args),
        out_specs=pl.BlockSpec(memory_space=pltpu.VMEM),
        scratch_shapes=scratch,
        compiler_params=pltpu.CompilerParams(
            collective_id=0, has_side_effects=True, vmem_limit_bytes=67043328
        ),
        name="layer",
    )(*args)


def solution(mesh):
    placed = (
        P("sp", "tp"),
        P(),
        P("sp"),
        P(None, "tp"),
        P(None, "tp"),
        P(None, "tp"),
        P("tp", None, None),
        P("tp", None, None),
        P("tp"),
        P(None, "tp"),
        P(),
        P(),
        P(),
        P(None, "tp"),
        P("tp"),
        P("tp"),
        P("tp", None),
        P("tp", None),
        P(),
    )
    return jax.shard_map(
        shards, mesh=mesh, in_specs=placed, out_specs=P(("sp", "tp"), None), check_vma=False
    )
```

```python
import functools
import math

import jax
import jax.numpy as jnp
import numpy as np
from jax import lax
from jax.experimental import pallas as pl
from jax.experimental.pallas import tpu as pltpu
from jax.sharding import PartitionSpec as P

NOPE = 128
ROPE = 64
VDIM = 128
LANES = 128

EPS = 1e-06
RATE_C = 8.0
THETA = 10000.0
CHUNKS = 4
BATCH = 8
COLS = 4

MESH = pl.DeviceIdType.MESH
F32 = jnp.float32
BF16 = jnp.bfloat16


def one_minus_exp(y):
    series = 1.0 + y * (1.0 / 8.0)
    for order in (7, 6, 5, 4, 3, 2):
        series = 1.0 + y * (1.0 / order) * series
    return jnp.where(y > -0.5, -y * series, 1.0 - jnp.exp(y))


def gelu_tanh(x):
    inner = math.sqrt(2.0 / math.pi) * (x + 0.044715 * (x * x * x))
    return 0.5 * x * (1.0 + jnp.tanh(inner))


def softplus(x):
    z = jnp.exp(-jnp.abs(x))
    w = z / (2.0 + z)
    w2 = w * w
    series = jnp.full_like(w, 1.0 / 17.0)
    for order in (15, 13, 11, 9, 7, 5, 3):
        series = 1.0 / order + w2 * series
    return jnp.maximum(x, 0.0) + 2.0 * (w + w * w2 * series)


def rotate(tile, cosine, sine):
    lane = lax.broadcasted_iota(jnp.int32, tile.shape, 1)
    half = ROPE // 2
    other = jnp.where(
        lane < half, pltpu.roll(tile, tile.shape[1] - half, 1), pltpu.roll(tile, half, 1)
    )
    return tile * cosine + other * sine


def fused_kernel(
    n_sp, n_tp, heads,
    tokens, pre_gain, rate_factor, w_rec, w_gate, taps_in, rmap_in, imap_in, decay_in, w_query,
    w_latent, w_rope, lat_gain_in, w_expand, rec_gain_in, att_gain_in, w_or, w_oa, post_gain_in,
    turns_in, starts_in,
    out_ref,
    tok, scaled, gain, rate, wcat, taps, rmap, imap, decay, wrope, lgain, wexp,
    rgain, again, wor, woa, pgain, turns, starts,
    acc_lat, acc_rope, acc_rec, acc_gate, acc_q, sq, kv, qcat, padded, gated,
    m_ref, l_ref, o_ref, a_ref, b_ref, rb, ab,
    tail_tx, tail_rx, carry_tx, carry_rx, sq_tx, sq_rx, inv,
    prod, held, own, d2d_tx, d2d_rx, y_tx, y_rx, mixed, done, out_sem,
    load_sem, weight_sem, own_sem, tok_tx, tok_rx, fwd_tx, fwd_rx,
    kvz_tx, kvx_tx, kvd_tx, kvz_rx, kvx_rx, kvd_rx,
    tail_s, carry_s, carry_r, sq_s, sq_r, d2d_s, d2d_r, y_s, y_r,
):
    me = lax.axis_index("sp")
    tp = lax.axis_index("tp")
    n_y = n_tp // 2
    levels = n_sp // 2
    core = lax.rem(tp, 2)
    yy = lax.div(tp, 2)
    partner = tp + 1 - 2 * core
    column = lax.rem(me, 2)
    level = lax.div(me, 2)
    neighbour = me + 1 - 2 * column
    rows, feats = tokens.shape
    width = feats * n_tp
    latent = w_latent.shape[1]
    channels = w_rec.shape[1]
    rc = rows // CHUNKS
    hc = rc // 2
    rd = rows // n_tp
    cb = width // COLS

    small = (
        (tokens, tok.at[tp]), (pre_gain, gain), (lat_gain_in, lgain), (turns_in, turns),
        (starts_in, starts),
    )
    later = (
        (w_expand, wexp), (rate_factor, rate), (taps_in, taps), (rmap_in, rmap), (imap_in, imap),
        (decay_in, decay), (rec_gain_in, rgain), (att_gain_in, again), (w_or, wor), (w_oa, woa),
        (post_gain_in, pgain),
    )
    projections = []
    for s in (w_latent, w_rec, w_gate, w_query):
        first = projections[-1][2] if projections else 0
        projections.append((s, first, first + s.shape[1]))

    def loads_of(group, first):
        return [
            pltpu.make_async_copy(s, d, load_sem.at[first + i]) for i, (s, d) in enumerate(group)
        ]

    def features(blk):
        return pl.ds(pl.multiple_of(blk * feats, feats), feats)

    def weight_loads(blk):
        at = features(blk)
        copies = [pltpu.make_async_copy(w_rope.at[:, at], wrope.at[:, at], weight_sem.at[0, blk])]
        for s, first, last in projections:
            copies.append(
                pltpu.make_async_copy(s.at[at], wcat.at[at, first:last], weight_sem.at[1, blk])
            )
        return copies

    def weights_ready(blk):
        at = features(blk)
        weight_loads(blk)[0].wait()
        pltpu.make_async_copy(wcat.at[at], wcat.at[at], weight_sem.at[1, blk]).wait()

    first_loads = loads_of(small, 0)
    last_loads = loads_of(later, len(small))
    for copy in first_loads:
        copy.start()
    for dy in range(n_y):
        for b in range(2):
            for copy in weight_loads(2 * lax.rem(yy + dy, n_y) + lax.rem(core + b, 2)):
                copy.start()

    barrier = pltpu.get_barrier_semaphore()
    for d in range(1, n_sp):
        pl.semaphore_signal(
            barrier, inc=1, device_id={"sp": lax.rem(me + d, n_sp)}, device_id_type=MESH
        )
    for d in range(1, n_tp):
        pl.semaphore_signal(
            barrier, inc=1, device_id={"tp": lax.rem(tp + d, n_tp)}, device_id_type=MESH
        )
    with jax.named_scope("entry"):
        for ref in (acc_lat, acc_rope, acc_rec, acc_gate, acc_q, sq):
            ref[...] = jnp.zeros_like(ref)

        def blank(s, _):
            kv[s] = jnp.zeros(kv.shape[1:], BF16)
            return 0

        lax.fori_loop(me + 1, lax.div(me + BATCH - 1, BATCH) * BATCH, blank, 0)
        pl.semaphore_wait(barrier, n_sp + n_tp - 2)
        first_loads[0].wait()

    def remote(src, dst, send, recv, **where):
        return pltpu.make_async_remote_copy(
            src_ref=src, dst_ref=dst, send_sem=send, recv_sem=recv, device_id=where,
            device_id_type=MESH,
        )

    def chunk(r):
        return pl.ds(pl.multiple_of(r * rc, rc), rc)

    def half(r):
        return pl.ds(pl.multiple_of(r * rc + core * hc, hc), hc)

    def own_copy():
        return remote(tok.at[tp], tok.at[tp], own_sem.at[0], own_sem.at[1], tp=partner)

    def tok_copy(dy, r):
        to = 2 * lax.rem(yy + dy, n_y) + core
        part = tok.at[tp, chunk(r)]
        return remote(part, part, tok_tx, tok_rx.at[dy - 1, r], tp=to)

    def fwd_copy(dy, r):
        part = tok.at[2 * lax.rem(yy + n_y - dy, n_y) + core, chunk(r)]
        return remote(part, part, fwd_tx, fwd_rx.at[dy - 1, r], tp=partner)

    for step in range(CHUNKS):
        for dy in range(1, n_y):
            tok_copy(dy, CHUNKS - 1 - step).start()
    own_copy().start()

    def dot(a, b):
        return jnp.dot(a, b, preferred_element_type=F32)

    def dot_t(a, b):
        return lax.dot_general(a, b, (((1,), (1,)), ((), ())), preferred_element_type=F32)

    def tiles(x):
        return [x[:, i : i + LANES] for i in range(0, x.shape[1], LANES)]

    def wide(x, count):
        return jnp.concatenate([x] * count, axis=1) if count > 1 else x

    @jax.named_scope("scale")
    def scale_rows(blk, first, count):
        span = min(count, 32)

        def body(i, _):
            at = pl.ds(pl.multiple_of(first + i * span, span), span)
            x = tok[blk, at, :].astype(F32)
            scaled[at, :] = (x * gain[blk]).astype(BF16)
            sq[at, :] += functools.reduce(jnp.add, tiles(x * x))
            return 0

        lax.fori_loop(0, count // span, body, 0)

    @jax.named_scope("early")
    def project_early(blk, at):
        k = features(blk)
        x = scaled[at, :]
        acc_rope[at, : wrope.shape[0]] += dot_t(x, wrope[:, k])
        acc_lat[at, :] += dot(x, wcat[k, :latent])

    @jax.named_scope("late")
    def project_late(blk, at):
        k = features(blk)
        x = scaled[at, :]
        for (_, first, last), acc in zip(projections[1:], (acc_rec, acc_gate, acc_q)):
            acc[at, : last - first] += dot(x, wcat[k, first:last])

    for copy in first_loads[1:]:
        copy.wait()
    everything = pl.ds(0, rows)

    def own_chip(i, _):
        blk = 2 * yy + lax.rem(core + i, 2)

        @pl.when(i == 1)
        def _():
            own_copy().wait_recv()

        scale_rows(blk, 0, rows)
        with jax.named_scope("weights"):
            weights_ready(blk)
        project_early(blk, everything)
        project_late(blk, everything)
        return 0

    lax.fori_loop(0, 2, own_chip, 0)
    for copy in last_loads:
        copy.start()

    def settle(count, most, wait):
        for k in range(1, most + 1):
            @pl.when(count == k)
            def _():
                wait(k)

    def upwards(s, r):
        part = kv.at[s, half(r)]
        for dz in range(1, min(3, levels)):
            @pl.when(level + dz < levels)
            def _():
                (
                    remote(part, part, kvz_tx, kvz_rx.at[level + dz - lax.div(s, 2), r], sp=me + 2 * dz)
                ).start()

    def kvx_copy(s, r):
        part = kv.at[s, half(r)]
        return remote(part, part, kvx_tx, kvx_rx.at[r], sp=neighbour)

    def kvd_copy(s, r):
        part = kv.at[s, half(r)]
        return remote(part, part, kvd_tx, kvd_rx.at[r], tp=partner)

    @jax.named_scope("fwdz")
    def forward_z(r, near, far):
        def body(dz, _):
            s = me - 2 * dz
            part = kv.at[s, half(r)]
            remote(part, part, kvz_tx, kvz_rx.at[dz, r], sp=neighbour).wait_recv()

            @pl.when(lax.rem(dz, 2) == 0)
            def _():
                upwards(s, r)

            kvx_copy(s, r).start()
            kvd_copy(s, r).start()
            return 0

        lax.fori_loop(near, jnp.minimum(far, level + 1), body, 0)

    @jax.named_scope("fwdx")
    def forward_x(r):
        def body(dz, _):
            kvd_copy(neighbour - 2 * dz, r).start()
            return 0

        def arrived(k):
            part = kv.at[0:k, 0:hc]
            remote(part, part, kvx_tx, kvx_rx.at[r], sp=neighbour).wait_recv()

        settle(level + column, levels, arrived)

        lax.fori_loop(1 - column, level + 1, body, 0)

    def angles(at):
        lane = lax.broadcasted_iota(jnp.int32, (1, LANES), 1)
        kept = jnp.where(lane < ROPE, 1.0, 0.0)
        sign = jnp.where(lane < ROPE // 2, -1.0, kept)
        c, s = turns[0, at, :], turns[1, at, :]
        c0, s0 = starts[0, me], starts[1, me]
        return (c * c0 - s * s0) * kept, (s * c0 + c * s0) * sign

    def inverse_of(at):
        total = jnp.sum(sq[at, :], axis=1, keepdims=True)
        return lax.rsqrt(total * (1.0 / width) + EPS)

    @jax.named_scope("latent")
    def finish_latent(r, at):
        inverse = inverse_of(at)
        cosine, sine = angles(at)
        raw = acc_lat[at, :] * inverse
        norm = raw * lax.rsqrt(jnp.mean(raw * raw, axis=1, keepdims=True) + EPS) * lgain[...]
        kv[me, at, :latent] = norm.astype(BF16)
        kv[me, at, latent:] = rotate(acc_rope[at, :] * inverse, cosine, sine).astype(BF16)
        upwards(me, r)

        @pl.when(column == 0)
        def _():
            kvx_copy(me, r).start()

    def tok_step(step, _):
        r = CHUNKS - 1 - step
        at = chunk(r)
        with jax.named_scope("tokwait"):
            for dy in range(1, n_y):
                tok_copy(dy, r).wait_recv()
                fwd_copy(dy, r).start()

        for b in range(2):
            for dy in range(1, n_y):
                blk = 2 * lax.rem(yy + n_y - dy, n_y) + lax.rem(core + b, 2)
                if b == 1:
                    with jax.named_scope("fwdwait"):
                        fwd_copy(dy, r).wait_recv()
                    if dy == 1:
                        @pl.when(step > 1)
                        def _():
                            forward_z(r + 2, 2, 3)

                        @pl.when(step > 2)
                        def _():
                            forward_z(r + 3, 3, levels)

                scale_rows(blk, r * rc, rc)

                @pl.when(step == 0)
                def _():
                    weights_ready(blk)

                project_early(blk, at)
                if b == 1 and dy == n_y - 1:
                    finish_latent(r, at)
                project_late(blk, at)

        with jax.named_scope("finish"):
            inverse = inverse_of(at)
            cosine, sine = angles(at)
            low = (acc_rec[at, :] * inverse).astype(BF16)
            padded[pl.ds(pl.multiple_of(r * rc + 8, 8), rc), :] = low.astype(F32)
            gated[at, :] = gelu_tanh(acc_gate[at, :] * inverse)
            query = acc_q[at, :] * inverse
            total = query.shape[1]
            for h in range(heads):
                start = h * (NOPE + ROPE)
                turned = query if start == 0 else pltpu.roll(query, total - start, 1)
                qcat[h, at, :NOPE] = turned[:, :NOPE].astype(BF16)
                qcat[h, at, NOPE:] = rotate(turned[:, NOPE : NOPE + LANES], cosine, sine).astype(BF16)

        @pl.when(step == 0)
        def _():
            tail_tx[...] = padded[rows : rows + 8, :]

            @pl.when(me + 1 < n_sp)
            def _():
                tail_copy().start()

        @pl.when(step > 0)
        def _():
            forward_z(r + 1, 1, 2)

        return 0

    def tail_copy():
        return remote(tail_tx, tail_rx, tail_s.at[0], tail_s.at[1], sp=me + 1)

    lax.fori_loop(0, CHUNKS, tok_step, 0)

    forward_z(1, 2, 3)

    for copy in last_loads:
        copy.wait()

    @pl.when(me > 0)
    def _():
        tail_copy().wait_recv()
        padded[0:8, :] = tail_rx[...]

    @pl.when(me == 0)
    def _():
        padded[0:8, :] = jnp.zeros((8, channels), F32)

    mark = jax.named_scope("rec")
    mark.__enter__()
    count = taps.shape[0]
    conv = taps[0:1, :] * padded[9 - count : 9 - count + rows, :]
    for k in range(1, count):
        conv = conv + taps[k : k + 1, :] * padded[9 - count + k : 9 - count + k + rows, :]
    low = conv.astype(BF16)
    bw = rmap.shape[1]
    rates, entries = [], []
    for b in range(rmap.shape[0]):
        part = low[:, b * bw : (b + 1) * bw]
        rates.append(dot(part, rmap[b]))
        entries.append(dot(part, imap[b]))
    rate_gate = jax.nn.sigmoid(jnp.concatenate(rates, axis=1))
    entry = jax.nn.sigmoid(jnp.concatenate(entries, axis=1))
    eye = lax.broadcasted_iota(jnp.int32, (rows, rows), 0) == lax.broadcasted_iota(
        jnp.int32, (rows, rows), 1
    )

    def to_column(row):
        return jnp.sum(jnp.where(eye, row, 0.0), axis=1, keepdims=True)

    def to_row(col):
        return jnp.sum(jnp.where(eye, col, 0.0), axis=0, keepdims=True)

    log_keep = -RATE_C * to_column(rate[...]) * rate_gate * softplus(-decay[...])
    a = jnp.exp(log_keep)
    b = jnp.sqrt(one_minus_exp(2.0 * log_keep)) * entry * conv
    row = lax.broadcasted_iota(jnp.int32, (rows, channels), 0)
    d = 1
    while d < rows:
        inside = row >= d
        b = a * jnp.where(inside, pltpu.roll(b, d, 0), 0.0) + b
        a = a * jnp.where(inside, pltpu.roll(a, d, 0), 1.0)
        d *= 2
    a_ref[...] = a
    b_ref[...] = b
    carry_tx[...] = jnp.zeros_like(carry_tx)
    carry_tx[0:1, :] = a[rows - 1 :, :]
    carry_tx[1:2, :] = b[rows - 1 :, :]

    mark.__exit__(None, None, None)

    def carry_copy(d):
        return remote(
            carry_tx, carry_rx.at[me], carry_s, carry_r, sp=me + d
        )

    def carry_start(d, _):
        carry_copy(d).start()
        return 0

    lax.fori_loop(1, n_sp - me, carry_start, 0)
    forward_z(2, 3, levels)

    root = 1.0 / math.sqrt(NOPE + ROPE)

    @jax.named_scope("attend")
    def attend(keys_latent, keys_rope, limit):
        expanded = dot(keys_latent, wexp[...]).astype(BF16)
        for h in range(heads):
            at = h * (NOPE + VDIM)
            keys = jnp.concatenate([expanded[:, at : at + NOPE], keys_rope], axis=1)
            values = expanded[:, at + NOPE : at + NOPE + VDIM]
            scores = dot_t(qcat[h], keys) * root
            k_at = lax.broadcasted_iota(jnp.int32, scores.shape, 1)
            if limit is None:
                limit_at = lax.broadcasted_iota(jnp.int32, scores.shape, 0) + 1
            else:
                limit_at = limit
            scores = tiles(jnp.where(k_at < limit_at, scores, -jnp.inf))
            top = jnp.max(functools.reduce(jnp.maximum, scores), axis=1, keepdims=True)
            if limit is not None:
                old = m_ref[h]
                top = jnp.maximum(old, top)
                shrink = jnp.exp(old - top)
            weights = [jnp.exp(x - top) for x in scores]
            total = functools.reduce(jnp.add, weights)
            found = dot(jnp.concatenate([x.astype(BF16) for x in weights], axis=1), values)
            if limit is not None:
                total = total + l_ref[h] * shrink
                found = found + o_ref[h] * shrink
            m_ref[h] = jnp.broadcast_to(top, m_ref.shape[1:])
            l_ref[h] = total
            o_ref[h] = found

    def attend_chunk(r):
        def ready(k):
            part = kv.at[0:k, 0:hc]
            remote(part, part, kvd_tx, kvd_rx.at[r], tp=partner).wait_recv()

        with jax.named_scope("kvwait"):
            settle(me, n_sp - 1, ready)

        def group(g, _):
            several = pl.ds(g * BATCH, BATCH)
            count = BATCH * rc
            attend(
                kv[several, chunk(r), :latent].reshape(count, latent),
                kv[several, chunk(r), latent:].reshape(count, LANES),
                (me - g * BATCH) * rc,
            )
            return 0

        lax.fori_loop(0, lax.div(me + BATCH - 1, BATCH), group, 0)

    attend(kv[me, :, :latent], kv[me, :, latent:], None)
    forward_z(0, 1, 2)
    forward_z(0, 2, 3)
    forward_z(1, 3, levels)

    def sq_copy(kind, d):
        return remote(
            sq_tx.at[kind], sq_rx.at[kind, d], sq_s, sq_r.at[kind], tp=lax.rem(tp + d, n_tp)
        )

    def share_squares(kind, column):
        sq_tx[kind] = jnp.broadcast_to(to_row(column), sq_tx.shape[1:])
        for d in range(1, n_tp):
            sq_copy(kind, d).start()

    @jax.named_scope("sums")
    def join_squares(kind, count):
        total = sq_tx[kind]
        part = sq_rx.at[kind, 1:n_tp]
        remote(part, part, sq_s, sq_r.at[kind], tp=partner).wait_recv()
        for d in range(1, n_tp):
            total = total + sq_rx[kind, d]
        scale = lax.rsqrt(total * (1.0 / count) + EPS)
        inv[kind] = jnp.broadcast_to(to_column(scale[0:1, :]), inv.shape[1:])

    @jax.named_scope("join")
    def finish_recurrence():
        def join(s, carried):
            return carry_rx[s, 0:1, :] * carried + carry_rx[s, 1:2, :]

        def arrived(k):
            part = carry_rx.at[0:k]
            remote(part, part, carry_s, carry_r, sp=neighbour).wait_recv()

        settle(me, n_sp - 1, arrived)
        carried = lax.fori_loop(0, me, join, jnp.zeros((1, channels), F32))
        rec_out = (b_ref[...] + a_ref[...] * carried) * gated[...]
        rb[...] = (rec_out * rgain[...]).astype(BF16)
        share_squares(0, jnp.sum(rec_out * rec_out, axis=1, keepdims=True))

    def block(dy):
        return pl.ds(pl.multiple_of(2 * rd * lax.rem(yy + dy, n_y), 2 * rd), 2 * rd)

    def cols(c):
        return pl.ds(pl.multiple_of(c * cb, cb), cb)

    @jax.named_scope("multiply")
    def multiply(dy, c, left, right, store):
        store[dy, c] = dot(left[block(dy), :], right[:, cols(c)])

    def d2d_copy(dy, c):
        return remote(
            d2d_tx.at[dy, c], d2d_rx.at[dy, c], d2d_s, d2d_r.at[dy, c], tp=partner
        )

    def y_copy(dy, c):
        to = 2 * lax.rem(yy + dy, n_y) + core
        return remote(y_tx.at[dy, c], y_rx.at[dy, c], y_s, y_r.at[dy - 1, c], tp=to)

    def hand_over(dy, c, value):
        held[...] = value
        theirs = pl.ds(pl.multiple_of((1 - core) * rd, rd), rd)
        mine = pl.ds(pl.multiple_of(core * rd, rd), rd)
        d2d_tx[dy, c] = held[theirs, :].astype(BF16)
        d2d_copy(dy, c).start()
        own[dy, c] = held[mine, :]

    def product(dy, c, left, right):
        return dot(left[block(dy), :], right[:, cols(c)])

    @jax.named_scope("produce")
    def produce(dy, c):
        at, count = block(dy), cb // LANES
        hand_over(
            dy, c,
            prod[dy, c] * wide(inv[0, at, :], count)
            + product(dy, c, ab, woa) * wide(inv[1, at, :], count),
        )

    @jax.named_scope("pair")
    def send_pair(dy, c):
        d2d_copy(dy, c).wait_recv()
        y_tx[dy, c] = (own[dy, c] + d2d_rx[dy, c].astype(F32)).astype(BF16)
        y_copy(dy, c).start()

    @jax.named_scope("multiply")
    def rec_products(dy):
        def body(c, _):
            prod[dy, c] = product(dy, c, rb, wor)
            return 0

        lax.fori_loop(1, COLS, body, 0)

    forward_x(3)
    finish_recurrence()
    for dy in range(1, n_y):
        hand_over(dy, COLS, product(dy, 0, rb, wor))
    forward_z(0, 3, levels)
    attend_chunk(3)
    for dy in range(1, n_y):
        send_pair(dy, COLS)
    forward_x(2)
    for dy in range(1, n_y):
        rec_products(dy)
    attend_chunk(2)
    forward_x(1)
    hand_over(0, COLS, product(0, 0, rb, wor))
    rec_products(0)
    join_squares(0, channels * n_tp)
    attend_chunk(1)
    forward_x(0)
    attend_chunk(0)

    att_sq = jnp.zeros((rows, 1), F32)
    for h in range(heads):
        att = o_ref[h] / jnp.sum(l_ref[h], axis=1, keepdims=True)
        att_sq = att_sq + jnp.sum(att * att, axis=1, keepdims=True)
        at = slice(h * VDIM, (h + 1) * VDIM)
        ab[:, at] = (att * again[:, at]).astype(BF16)
    share_squares(1, att_sq)
    for dy in range(1, n_y):
        hand_over(dy, 0, product(dy, 0, ab, woa))
    for dy in range(1, n_y):
        send_pair(dy, 0)
    join_squares(1, heads * VDIM * n_tp)

    for dy in range(1, n_y):
        def away(c, _):
            @pl.when(c < COLS)
            def _():
                produce(dy, c)

            @pl.when(c > 1)
            def _():
                send_pair(dy, c - 1)

            return 0

        lax.fori_loop(1, COLS + 1, away, 0)

    hand_over(0, 0, product(0, 0, ab, woa))

    def home(c, _):
        produce(0, c)
        return 0

    lax.fori_loop(1, COLS, home, 0)

    def gone(part, sem):
        remote(part, part, sem, own_sem.at[1], tp=partner).wait_send()

    with jax.named_scope("drain"):
        gone(tok.at[tp], own_sem.at[0])
        gone(tok.at[0 : n_y - 1], tok_tx)
        gone(tok.at[0 : n_y - 1], fwd_tx)
        for at in range(levels - 1):
            @pl.when(level == at)
            def _():
                count = (1 + at // 2) * min(2, levels - 1 - at)
                gone(kv.at[0:count, 0 : CHUNKS * hc], kvz_tx)

        settle(level + 1 - column, levels, lambda k: gone(kv.at[0:k, 0 : CHUNKS * hc], kvx_tx))
        settle(me, n_sp - 1, lambda k: gone(kv.at[0:k, 0 : CHUNKS * hc], kvd_tx))
        settle(n_sp - 1 - me, n_sp - 1, lambda k: gone(carry_rx.at[0:k], carry_s))
        gone(sq_rx.at[:, 1:n_tp], sq_s)

        @pl.when(me + 1 < n_sp)
        def _():
            tail_copy().wait_send()

    my_rows = pl.ds(pl.multiple_of(tp * rd, rd), rd)

    def summed(c):
        d2d_copy(0, c).wait_recv()
        value = own[0, c] + d2d_rx[0, c].astype(F32)
        for dy in range(1, n_y):
            y_copy(dy, c).wait_recv()
            value = value + y_rx[dy, c].astype(F32)
        return value

    @jax.named_scope("gather")
    def first_columns():
        count = cb // LANES
        value = summed(COLS) * wide(inv[0, my_rows, :], count)
        value = value + summed(0) * wide(inv[1, my_rows, :], count)
        mixed[0] = value
        return jnp.sum(value * value, axis=1, keepdims=True)

    @jax.named_scope("gather")
    def gather(c, total):
        value = summed(c)
        mixed[c] = value
        return total + jnp.sum(value * value, axis=1, keepdims=True)

    total = lax.fori_loop(1, COLS, gather, first_columns())

    def out_copy(at):
        return pltpu.make_async_copy(done.at[:, at], out_ref.at[:, at], out_sem)

    mark = jax.named_scope("final")
    mark.__enter__()
    last = lax.rsqrt(total * (1.0 / width) + EPS)

    for c in range(COLS):
        at = slice(c * cb, (c + 1) * cb)
        done[:, at] = (mixed[c] * last * pgain[:, at]).astype(BF16)
        out_copy(at).start()

    mark.__exit__(None, None, None)
    with jax.named_scope("outwait"):
        out_copy(slice(0, width)).wait()

    mark = jax.named_scope("sumsdone")
    mark.__enter__()

    gone(d2d_tx, d2d_s)
    gone(y_tx.at[1:n_y], y_s)
    mark.__exit__(None, None, None)


def shards(
    tokens, pre_gain, rate_factor, w_rec_in, w_rec_gate, conv_taps, rate_maps, input_maps,
    decay_param, w_query, w_latent, w_rope_key, latent_gain, w_expand, rec_gain, att_gain,
    w_out_rec, w_out_att, post_gain,
):
    n_sp = lax.axis_size("sp")
    n_tp = lax.axis_size("tp")
    n_y = n_tp // 2
    rows, feats = tokens.shape
    width = feats * n_tp
    channels = w_rec_in.shape[1]
    latent = w_latent.shape[1]
    q_cols = w_query.shape[1]
    heads = q_cols // (NOPE + ROPE)
    q_pad = -(-q_cols // LANES) * LANES
    rd = rows // n_tp
    cb = width // COLS

    lane = np.arange(LANES)
    frequency = np.where(lane < ROPE, THETA ** (-2.0 * (lane % (ROPE // 2)) / ROPE), 0.0)
    within = np.arange(rows)[:, None] * frequency
    start = rows * np.arange(n_sp)[:, None, None] * frequency
    turns = np.stack([np.cos(within), np.sin(within)]).astype(np.float32)
    starts = np.stack([np.cos(start), np.sin(start)]).astype(np.float32)

    def row(v):
        return v.reshape(1, -1)

    args = (
        tokens, pre_gain.reshape(n_tp, 1, feats), row(rate_factor), w_rec_in, w_rec_gate,
        conv_taps, rate_maps, input_maps, row(decay_param), w_query, w_latent, w_rope_key.T,
        row(latent_gain), w_expand, row(rec_gain), row(att_gain), w_out_rec, w_out_att,
        row(post_gain), jnp.asarray(turns), jnp.asarray(starts),
    )
    vm = pltpu.VMEM
    dma = pltpu.SemaphoreType.DMA

    def like(x):
        return vm(x.shape, x.dtype)

    scratch = [
        vm((n_tp, rows, feats), BF16), vm((rows, feats), BF16), like(args[1]), like(args[2]),
        vm((width, latent + 2 * channels + q_cols), BF16),
        like(args[5]), like(args[6]), like(args[7]), like(args[8]),
        like(args[11]), like(args[12]), like(args[13]),
        like(args[14]), like(args[15]), like(args[16]), like(args[17]), like(args[18]),
        like(args[19]), like(args[20]),
        vm((rows, latent), F32), vm((rows, LANES), F32), vm((rows, channels), F32),
        vm((rows, channels), F32), vm((rows, q_pad), F32), vm((rows, LANES), F32),
        vm((n_sp, rows, latent + LANES), BF16), vm((heads, rows, NOPE + LANES), BF16),
        vm((rows + 8, channels), F32), vm((rows, channels), F32),
        vm((heads, rows, LANES), F32), vm((heads, rows, LANES), F32), vm((heads, rows, VDIM), F32),
        vm((rows, channels), F32), vm((rows, channels), F32),
        vm((rows, channels), BF16), vm((rows, heads * VDIM), BF16),
        vm((8, channels), F32), vm((8, channels), F32), vm((8, channels), F32),
        vm((n_sp, 8, channels), F32), vm((2, 8, rows), F32), vm((2, n_tp, 8, rows), F32),
        vm((2, rows, LANES), F32),
        vm((n_y, COLS, 2 * rd, cb), F32), vm((2 * rd, cb), F32),
        vm((n_y, COLS + 1, rd, cb), F32), vm((n_y, COLS + 1, rd, cb), BF16),
        vm((n_y, COLS + 1, rd, cb), BF16), vm((n_y, COLS + 1, rd, cb), BF16),
        vm((n_y, COLS + 1, rd, cb), BF16), vm((COLS, rd, cb), F32), vm((rd, width), BF16),
        dma,
        dma((16,)), dma((2, n_tp)), dma((2,)), dma, dma((n_y - 1, CHUNKS)),
        dma, dma((n_y - 1, CHUNKS)),
        dma, dma, dma, dma((n_sp // 2, CHUNKS)), dma((CHUNKS,)), dma((CHUNKS,)),
        dma((2,)), dma, dma, dma, dma((2,)),
        dma, dma((n_y, COLS + 1)), dma, dma((n_y - 1, COLS + 1)),
    ]
    return pl.pallas_call(
        functools.partial(fused_kernel, n_sp, n_tp, heads),
        out_shape=jax.ShapeDtypeStruct((rd, width), BF16),
        in_specs=[pl.BlockSpec(memory_space=pl.ANY)] * len(args),
        out_specs=pl.BlockSpec(memory_space=pl.ANY),
        scratch_shapes=scratch,
        compiler_params=pltpu.CompilerParams(
            collective_id=0, has_side_effects=True, vmem_limit_bytes=67043328
        ),
        name="layer",
    )(*args)


def solution(mesh):
    placed = (
        P("sp", "tp"),
        P(),
        P("sp"),
        P(None, "tp"),
        P(None, "tp"),
        P(None, "tp"),
        P("tp", None, None),
        P("tp", None, None),
        P("tp"),
        P(None, "tp"),
        P(),
        P(),
        P(),
        P(None, "tp"),
        P("tp"),
        P("tp"),
        P("tp", None),
        P("tp", None),
        P(),
    )
    return jax.shard_map(
        shards, mesh=mesh, in_specs=placed, out_specs=P(("sp", "tp"), None), check_vma=False
    )
```

```python
import functools
import math

import jax
import jax.numpy as jnp
import numpy as np
from jax import lax
from jax.experimental import pallas as pl
from jax.experimental.pallas import tpu as pltpu
from jax.sharding import PartitionSpec as P

NOPE = 128
ROPE = 64
VDIM = 128
LANES = 128

EPS = 1e-06
RATE_C = 8.0
THETA = 10000.0
CHUNKS = 4
BATCH = 8
SPLIT = 2
COLS = 4

MESH = pl.DeviceIdType.MESH
F32 = jnp.float32
BF16 = jnp.bfloat16


def one_minus_exp(y):
    series = 1.0 + y * (1.0 / 8.0)
    for order in (7, 6, 5, 4, 3, 2):
        series = 1.0 + y * (1.0 / order) * series
    return jnp.where(y > -0.5, -y * series, 1.0 - jnp.exp(y))


def gelu_tanh(x):
    inner = math.sqrt(2.0 / math.pi) * (x + 0.044715 * (x * x * x))
    return 0.5 * x * (1.0 + jnp.tanh(inner))


def softplus(x):
    z = jnp.exp(-jnp.abs(x))
    w = z / (2.0 + z)
    w2 = w * w
    series = jnp.full_like(w, 1.0 / 17.0)
    for order in (15, 13, 11, 9, 7, 5, 3):
        series = 1.0 / order + w2 * series
    return jnp.maximum(x, 0.0) + 2.0 * (w + w * w2 * series)


def rotate(tile, cosine, sine):
    lane = lax.broadcasted_iota(jnp.int32, tile.shape, 1)
    half = ROPE // 2
    other = jnp.where(
        lane < half, pltpu.roll(tile, tile.shape[1] - half, 1), pltpu.roll(tile, half, 1)
    )
    return tile * cosine + other * sine


def fused_kernel(
    n_sp, n_tp, heads,
    tokens, pre_gain, rate_factor, w_rec, w_gate, taps_in, rmap_in, imap_in, decay_in, w_query,
    w_latent, w_rope, lat_gain_in, w_expand, rec_gain_in, att_gain_in, w_or, w_oa, post_gain_in,
    turns_in, starts_in,
    out_ref,
    tok, scaled, gain, rate, wcat, taps, rmap, imap, decay, wrope, lgain, wexp,
    rgain, again, wor, woa, pgain, turns, starts,
    acc_lat, acc_rope, acc_rec, acc_gate, acc_q, sq, kv, qcat, padded, gated,
    m_ref, l_ref, o_ref, a_ref, b_ref, rb, ab,
    tail_tx, tail_rx, carry_tx, carry_rx, sq_tx, sq_rx, inv,
    prod, held, own, d2d_tx, d2d_rx, y_tx, y_rx, mixed, done, out_sem, known,
    load_sem, weight_sem, own_sem, tok_tx, tok_rx, fwd_tx, fwd_rx,
    kvz_tx, kvx_tx, kvd_tx, kvz_rx, kvx_rx, kvd_rx,
    tail_s, carry_s, carry_r, sq_s, sq_r, d2d_s, d2d_r, y_s, y_r,
):
    me = lax.axis_index("sp")
    tp = lax.axis_index("tp")
    n_y = n_tp // 2
    levels = n_sp // 2
    core = lax.rem(tp, 2)
    yy = lax.div(tp, 2)
    partner = tp + 1 - 2 * core
    column = lax.rem(me, 2)
    level = lax.div(me, 2)
    neighbour = me + 1 - 2 * column
    rows, feats = tokens.shape
    width = feats * n_tp
    latent = w_latent.shape[1]
    channels = w_rec.shape[1]
    rc = rows // CHUNKS
    hc = rc // 2
    rd = rows // n_tp
    cb = width // COLS

    small = (
        (tokens, tok.at[tp]), (pre_gain, gain), (lat_gain_in, lgain), (turns_in, turns),
        (starts_in, starts),
    )
    later = (
        (w_expand, wexp), (rate_factor, rate), (taps_in, taps), (rmap_in, rmap), (imap_in, imap),
        (decay_in, decay), (rec_gain_in, rgain), (att_gain_in, again), (w_or, wor), (w_oa, woa),
        (post_gain_in, pgain),
    )
    projections = []
    for s in (w_latent, w_rec, w_gate, w_query):
        first = projections[-1][2] if projections else 0
        projections.append((s, first, first + s.shape[1]))

    def loads_of(group, first):
        return [
            pltpu.make_async_copy(s, d, load_sem.at[first + i]) for i, (s, d) in enumerate(group)
        ]

    def features(blk):
        return pl.ds(pl.multiple_of(blk * feats, feats), feats)

    def rope_load(blk):
        at = features(blk)
        return pltpu.make_async_copy(w_rope.at[:, at], wrope.at[:, at], weight_sem.at[0, blk])

    def weight_loads(blk):
        at = features(blk)
        return [rope_load(blk)] + [
            pltpu.make_async_copy(s.at[at], wcat.at[at, first:last], weight_sem.at[1, blk])
            for s, first, last in projections
        ]

    def weights_ready(blk):
        at = features(blk)
        rope_load(blk).wait()
        pltpu.make_async_copy(wcat.at[at], wcat.at[at], weight_sem.at[1, blk]).wait()

    first_loads = loads_of(small, 0)
    last_loads = loads_of(later, len(small))
    for copy in first_loads:
        copy.start()

    def start_weights(dy):
        for b in range(2):
            for copy in weight_loads(2 * lax.rem(yy + dy, n_y) + lax.rem(core + b, 2)):
                copy.start()

    barrier = pltpu.get_barrier_semaphore()
    near = [o for step in (1, 2, 4) for o in (step, -step)]
    inside = [(me + o >= 0) & (me + o < n_sp) for o in near]
    near_count = functools.reduce(jnp.add, [x.astype(jnp.int32) for x in inside])

    def tell_near(sem):
        for o, x in zip(near, inside):
            @pl.when(x)
            def _():
                pl.semaphore_signal(
                    sem, inc=1, device_id={"sp": me + o}, device_id_type=MESH
                )

    rounds = known.shape[0]
    tell_near(barrier)
    for d in range(1, n_tp):
        pl.semaphore_signal(
            barrier, inc=1, device_id={"tp": lax.rem(tp + d, n_tp)}, device_id_type=MESH
        )
    with jax.named_scope("entry"):
        for ref in (acc_lat, acc_rope, acc_rec, acc_gate, acc_q, sq):
            ref[...] = jnp.zeros_like(ref)

        def blank(s, _):
            kv[s] = jnp.zeros(kv.shape[1:], BF16)
            return 0

        lax.fori_loop(me + 1, lax.div(me + BATCH - 1, BATCH) * BATCH, blank, 0)
        first_loads[0].wait()
        start_weights(0)
        pl.semaphore_wait(barrier, near_count + n_tp - 1)
        tell_near(known.at[0])

    def remote(src, dst, send, recv, **where):
        return pltpu.make_async_remote_copy(
            src_ref=src, dst_ref=dst, send_sem=send, recv_sem=recv, device_id=where,
            device_id_type=MESH,
        )

    def chunk(r):
        return pl.ds(pl.multiple_of(r * rc, rc), rc)

    def half(r):
        return pl.ds(pl.multiple_of(r * rc + core * hc, hc), hc)

    def own_copy():
        return remote(tok.at[tp], tok.at[tp], own_sem.at[0], own_sem.at[1], tp=partner)

    def tok_copy(dy, r):
        to = 2 * lax.rem(yy + dy, n_y) + core
        part = tok.at[tp, chunk(r)]
        return remote(part, part, tok_tx, tok_rx.at[dy - 1, r], tp=to)

    def fwd_copy(dy, r):
        part = tok.at[2 * lax.rem(yy + n_y - dy, n_y) + core, chunk(r)]
        return remote(part, part, fwd_tx, fwd_rx.at[dy - 1, r], tp=partner)

    for step in range(CHUNKS):
        for dy in range(1, n_y):
            tok_copy(dy, CHUNKS - 1 - step).start()
    own_copy().start()

    @jax.named_scope("tokwait")
    def pass_on(r):
        for dy in range(1, n_y):
            tok_copy(dy, r).wait_recv()
            fwd_copy(dy, r).start()

    def dot(a, b):
        return jnp.dot(a, b, preferred_element_type=F32)

    def dot_t(a, b):
        return lax.dot_general(a, b, (((1,), (1,)), ((), ())), preferred_element_type=F32)

    def tiles(x):
        return [x[:, i : i + LANES] for i in range(0, x.shape[1], LANES)]

    def wide(x, count):
        return jnp.concatenate([x] * count, axis=1) if count > 1 else x

    @jax.named_scope("scale")
    def scale_rows(blk, first, count):
        span = min(count, 32)

        def body(i, _):
            at = pl.ds(pl.multiple_of(first + i * span, span), span)
            x = tok[blk, at, :].astype(F32)
            scaled[at, :] = (x * gain[blk]).astype(BF16)
            sq[at, :] += functools.reduce(jnp.add, tiles(x * x))
            return 0

        lax.fori_loop(0, count // span, body, 0)

    @jax.named_scope("early")
    def project_early(blk, at):
        k = features(blk)
        x = scaled[at, :]
        acc_rope[at, : wrope.shape[0]] += dot_t(x, wrope[:, k])
        acc_lat[at, :] += dot(x, wcat[k, :latent])

    @jax.named_scope("late")
    def project_late(blk, at):
        k = features(blk)
        x = scaled[at, :]
        for (_, first, last), acc in zip(projections[1:], (acc_rec, acc_gate, acc_q)):
            acc[at, : last - first] += dot(x, wcat[k, first:last])

    for copy in first_loads[1:]:
        copy.wait()
    everything = pl.ds(0, rows)

    def own_chip(i, _):
        blk = 2 * yy + lax.rem(core + i, 2)

        @pl.when(i == 1)
        def _():
            own_copy().wait_recv()

        scale_rows(blk, 0, rows)
        with jax.named_scope("weights"):
            weights_ready(blk)

        @pl.when(i == 0)
        def _():
            for dy in range(1, n_y):
                start_weights(dy)

        project_early(blk, everything)
        project_late(blk, everything)
        return 0

    lax.fori_loop(0, 2, own_chip, 0)
    for copy in last_loads:
        copy.start()
    for k in range(rounds - 1):
        pl.semaphore_wait(known.at[k], near_count)
        tell_near(known.at[k + 1])

    def settle(count, most, wait):
        for k in range(1, most + 1):
            @pl.when(count == k)
            def _():
                wait(k)

    def upwards(s, r):
        part = kv.at[s, half(r)]
        for dz in range(1, min(3, levels)):
            @pl.when(level + dz < levels)
            def _():
                (
                    remote(part, part, kvz_tx, kvz_rx.at[level + dz - lax.div(s, 2), r], sp=me + 2 * dz)
                ).start()

    def kvx_copy(s, r):
        part = kv.at[s, half(r)]
        return remote(part, part, kvx_tx, kvx_rx.at[r], sp=neighbour)

    def kvd_copy(s, r):
        part = kv.at[s, half(r)]
        return remote(part, part, kvd_tx, kvd_rx.at[r], tp=partner)

    @jax.named_scope("fwdz")
    def forward_z(r, near, far):
        def body(dz, _):
            s = me - 2 * dz
            part = kv.at[s, half(r)]
            remote(part, part, kvz_tx, kvz_rx.at[dz, r], sp=neighbour).wait_recv()

            @pl.when(lax.rem(dz, 2) == 0)
            def _():
                upwards(s, r)

            kvx_copy(s, r).start()
            kvd_copy(s, r).start()
            return 0

        lax.fori_loop(near, jnp.minimum(far, level + 1), body, 0)

    @jax.named_scope("fwdx")
    def forward_x(r):
        def body(dz, _):
            kvd_copy(neighbour - 2 * dz, r).start()
            return 0

        def arrived(k):
            part = kv.at[0:k, 0:hc]
            remote(part, part, kvx_tx, kvx_rx.at[r], sp=neighbour).wait_recv()

        settle(level + column, levels, arrived)

        lax.fori_loop(1 - column, level + 1, body, 0)

    def angles(at):
        lane = lax.broadcasted_iota(jnp.int32, (1, LANES), 1)
        kept = jnp.where(lane < ROPE, 1.0, 0.0)
        sign = jnp.where(lane < ROPE // 2, -1.0, kept)
        c, s = turns[0, at, :], turns[1, at, :]
        c0, s0 = starts[0, me], starts[1, me]
        return (c * c0 - s * s0) * kept, (s * c0 + c * s0) * sign

    def inverse_of(at):
        total = jnp.sum(sq[at, :], axis=1, keepdims=True)
        return lax.rsqrt(total * (1.0 / width) + EPS)

    @jax.named_scope("latent")
    def finish_latent(r, at):
        inverse = inverse_of(at)
        cosine, sine = angles(at)
        raw = acc_lat[at, :] * inverse
        norm = raw * lax.rsqrt(jnp.mean(raw * raw, axis=1, keepdims=True) + EPS) * lgain[...]
        kv[me, at, :latent] = norm.astype(BF16)
        kv[me, at, latent:] = rotate(acc_rope[at, :] * inverse, cosine, sine).astype(BF16)
        upwards(me, r)

        @pl.when(column == 0)
        def _():
            kvx_copy(me, r).start()

    def tok_step(step, _):
        r = CHUNKS - 1 - step
        at = chunk(r)
        pass_on(r)

        for b in range(2):
            for dy in range(1, n_y):
                blk = 2 * lax.rem(yy + n_y - dy, n_y) + lax.rem(core + b, 2)
                if b == 1:
                    with jax.named_scope("fwdwait"):
                        fwd_copy(dy, r).wait_recv()
                    if dy == 1:
                        @pl.when(step > 1)
                        def _():
                            forward_z(r + 2, 2, 3)

                        @pl.when(step > 2)
                        def _():
                            forward_z(r + 3, 3, levels)

                scale_rows(blk, r * rc, rc)

                @pl.when(step == 0)
                def _():
                    weights_ready(blk)

                project_early(blk, at)
                if b == 1 and dy == n_y - 1:
                    finish_latent(r, at)
                project_late(blk, at)

        with jax.named_scope("finish"):
            inverse = inverse_of(at)
            cosine, sine = angles(at)
            low = (acc_rec[at, :] * inverse).astype(BF16)
            padded[pl.ds(pl.multiple_of(r * rc + 8, 8), rc), :] = low.astype(F32)
            gated[at, :] = gelu_tanh(acc_gate[at, :] * inverse)
            query = acc_q[at, :] * inverse
            total = query.shape[1]
            for h in range(heads):
                start = h * (NOPE + ROPE)
                turned = query if start == 0 else pltpu.roll(query, total - start, 1)
                qcat[h, at, :NOPE] = turned[:, :NOPE].astype(BF16)
                qcat[h, at, NOPE:] = rotate(turned[:, NOPE : NOPE + LANES], cosine, sine).astype(BF16)

        @pl.when(step == 0)
        def _():
            tail_tx[...] = padded[rows : rows + 8, :]

            @pl.when(me + 1 < n_sp)
            def _():
                tail_copy().start()

        @pl.when(step > 0)
        def _():
            forward_z(r + 1, 1, 2)

        return 0

    def tail_copy():
        return remote(tail_tx, tail_rx, tail_s.at[0], tail_s.at[1], sp=me + 1)

    lax.fori_loop(0, CHUNKS, tok_step, 0)

    forward_z(1, 2, 3)

    for copy in last_loads:
        copy.wait()

    @pl.when(me > 0)
    def _():
        tail_copy().wait_recv()
        padded[0:8, :] = tail_rx[...]

    @pl.when(me == 0)
    def _():
        padded[0:8, :] = jnp.zeros((8, channels), F32)

    mark = jax.named_scope("rec")
    mark.__enter__()
    count = taps.shape[0]
    conv = taps[0:1, :] * padded[9 - count : 9 - count + rows, :]
    for k in range(1, count):
        conv = conv + taps[k : k + 1, :] * padded[9 - count + k : 9 - count + k + rows, :]
    low = conv.astype(BF16)
    bw = rmap.shape[1]
    rates, entries = [], []
    for b in range(rmap.shape[0]):
        part = low[:, b * bw : (b + 1) * bw]
        rates.append(dot(part, rmap[b]))
        entries.append(dot(part, imap[b]))
    rate_gate = jax.nn.sigmoid(jnp.concatenate(rates, axis=1))
    entry = jax.nn.sigmoid(jnp.concatenate(entries, axis=1))
    eye = lax.broadcasted_iota(jnp.int32, (rows, rows), 0) == lax.broadcasted_iota(
        jnp.int32, (rows, rows), 1
    )

    def to_column(row):
        return jnp.sum(jnp.where(eye, row, 0.0), axis=1, keepdims=True)

    def to_row(col):
        return jnp.sum(jnp.where(eye, col, 0.0), axis=0, keepdims=True)

    log_keep = -RATE_C * to_column(rate[...]) * rate_gate * softplus(-decay[...])
    a = jnp.exp(log_keep)
    b = jnp.sqrt(one_minus_exp(2.0 * log_keep)) * entry * conv
    row = lax.broadcasted_iota(jnp.int32, (rows, channels), 0)
    d = 1
    while d < rows:
        inside = row >= d
        b = a * jnp.where(inside, pltpu.roll(b, d, 0), 0.0) + b
        a = a * jnp.where(inside, pltpu.roll(a, d, 0), 1.0)
        d *= 2
    a_ref[...] = a
    b_ref[...] = b
    carry_tx[...] = jnp.zeros_like(carry_tx)
    carry_tx[0:1, :] = a[rows - 1 :, :]
    carry_tx[1:2, :] = b[rows - 1 :, :]

    mark.__exit__(None, None, None)

    def carry_copy(d):
        return remote(
            carry_tx, carry_rx.at[me], carry_s, carry_r, sp=me + d
        )

    def carry_start(d, _):
        carry_copy(d).start()
        return 0

    pl.semaphore_wait(known.at[rounds - 1], near_count)
    lax.fori_loop(1, n_sp - me, carry_start, 0)

    root = 1.0 / math.sqrt(NOPE + ROPE)

    @jax.named_scope("attend")
    def attend(keys_latent, keys_rope, limit):
        expanded = dot(keys_latent, wexp[...]).astype(BF16)
        for h in range(heads):
            at = h * (NOPE + VDIM)
            keys = jnp.concatenate([expanded[:, at : at + NOPE], keys_rope], axis=1)
            values = expanded[:, at + NOPE : at + NOPE + VDIM]
            scores = dot_t(qcat[h], keys) * root
            k_at = lax.broadcasted_iota(jnp.int32, scores.shape, 1)
            if limit is None:
                limit_at = lax.broadcasted_iota(jnp.int32, scores.shape, 0) + 1
            else:
                limit_at = limit
            scores = tiles(jnp.where(k_at < limit_at, scores, -jnp.inf))
            top = jnp.max(functools.reduce(jnp.maximum, scores), axis=1, keepdims=True)
            if limit is not None:
                old = m_ref[h]
                top = jnp.maximum(old, top)
                shrink = jnp.exp(old - top)
            weights = [jnp.exp(x - top) for x in scores]
            total = functools.reduce(jnp.add, weights)
            found = dot(jnp.concatenate([x.astype(BF16) for x in weights], axis=1), values)
            if limit is not None:
                total = total + l_ref[h] * shrink
                found = found + o_ref[h] * shrink
            m_ref[h] = jnp.broadcast_to(top, m_ref.shape[1:])
            l_ref[h] = total
            o_ref[h] = found

    def attend_chunk(r):
        def ready(k):
            part = kv.at[0:k, 0:hc]
            remote(part, part, kvd_tx, kvd_rx.at[r], tp=partner).wait_recv()

        with jax.named_scope("kvwait"):
            settle(me, n_sp - 1, ready)

        def several(first, blocks):
            these = pl.ds(first, blocks)
            count = blocks * rc
            attend(
                kv[these, chunk(r), :latent].reshape(count, latent),
                kv[these, chunk(r), latent:].reshape(count, LANES),
                (me - first) * rc,
            )

        @pl.when((me > 0) & (me <= BATCH // 2))
        def _():
            several(0, BATCH // 2)

        @pl.when(me > BATCH // 2)
        def _():
            def group(g, _):
                several(g * BATCH, BATCH)
                return 0

            lax.fori_loop(0, lax.div(me + BATCH - 1, BATCH), group, 0)

    def sq_copy(kind, d):
        return remote(
            sq_tx.at[kind], sq_rx.at[kind, d], sq_s, sq_r.at[kind], tp=lax.rem(tp + d, n_tp)
        )

    def share_squares(kind, column):
        sq_tx[kind] = jnp.broadcast_to(to_row(column), sq_tx.shape[1:])
        for d in range(1, n_tp):
            sq_copy(kind, d).start()

    @jax.named_scope("sums")
    def join_squares(kind, count):
        total = sq_tx[kind]
        part = sq_rx.at[kind, 1:n_tp]
        remote(part, part, sq_s, sq_r.at[kind], tp=partner).wait_recv()
        for d in range(1, n_tp):
            total = total + sq_rx[kind, d]
        scale = lax.rsqrt(total * (1.0 / count) + EPS)
        inv[kind] = jnp.broadcast_to(to_column(scale[0:1, :]), inv.shape[1:])

    @jax.named_scope("join")
    def finish_recurrence():
        def join(s, carried):
            return carry_rx[s, 0:1, :] * carried + carry_rx[s, 1:2, :]

        def arrived(k):
            part = carry_rx.at[0:k]
            remote(part, part, carry_s, carry_r, sp=neighbour).wait_recv()

        settle(me, n_sp - 1, arrived)
        carried = lax.fori_loop(0, me, join, jnp.zeros((1, channels), F32))
        rec_out = (b_ref[...] + a_ref[...] * carried) * gated[...]
        rb[...] = (rec_out * rgain[...]).astype(BF16)
        share_squares(0, jnp.sum(rec_out * rec_out, axis=1, keepdims=True))

    def block(dy):
        return pl.ds(pl.multiple_of(2 * rd * lax.rem(yy + dy, n_y), 2 * rd), 2 * rd)

    def cols(c):
        return pl.ds(pl.multiple_of(c * cb, cb), cb)

    @jax.named_scope("multiply")
    def multiply(dy, c, left, right, store):
        store[dy, c] = dot(left[block(dy), :], right[:, cols(c)])

    def d2d_copy(dy, c):
        return remote(
            d2d_tx.at[dy, c], d2d_rx.at[dy, c], d2d_s, d2d_r.at[dy, c], tp=partner
        )

    def y_copy(dy, c):
        to = 2 * lax.rem(yy + dy, n_y) + core
        return remote(y_tx.at[dy, c], y_rx.at[dy, c], y_s, y_r.at[dy - 1, c], tp=to)

    def hand_over(dy, c, value):
        held[...] = value
        theirs = pl.ds(pl.multiple_of((1 - core) * rd, rd), rd)
        mine = pl.ds(pl.multiple_of(core * rd, rd), rd)
        d2d_tx[dy, c] = held[theirs, :].astype(BF16)
        d2d_copy(dy, c).start()
        own[dy, c] = held[mine, :]

    def product(dy, c, left, right):
        return dot(left[block(dy), :], right[:, cols(c)])

    @jax.named_scope("produce")
    def produce(dy, c):
        at, count = block(dy), cb // LANES
        hand_over(
            dy, c,
            prod[dy, c] * wide(inv[0, at, :], count)
            + product(dy, c, ab, woa) * wide(inv[1, at, :], count),
        )

    @jax.named_scope("pair")
    def send_pair(dy, c):
        d2d_copy(dy, c).wait_recv()
        y_tx[dy, c] = (own[dy, c] + d2d_rx[dy, c].astype(F32)).astype(BF16)
        y_copy(dy, c).start()

    @jax.named_scope("multiply")
    def rec_products(dy):
        def body(c, _):
            prod[dy, c] = product(dy, c, rb, wor)
            return 0

        lax.fori_loop(SPLIT, COLS, body, 0)

    forward_z(2, 3, levels)
    forward_x(3)
    attend(kv[me, :, :latent], kv[me, :, latent:], None)
    forward_z(0, 1, 2)
    attend_chunk(3)
    forward_z(0, 2, 3)
    forward_z(1, 3, levels)
    forward_x(2)
    finish_recurrence()
    for dy in range(1, n_y):
        for c in range(SPLIT):
            hand_over(dy, COLS + c, product(dy, c, rb, wor))
    forward_z(0, 3, levels)
    attend_chunk(2)
    for dy in range(1, n_y):
        for c in range(SPLIT):
            send_pair(dy, COLS + c)
    forward_x(1)
    for dy in range(1, n_y):
        rec_products(dy)
    attend_chunk(1)
    forward_x(0)
    for c in range(SPLIT):
        hand_over(0, COLS + c, product(0, c, rb, wor))
    rec_products(0)
    join_squares(0, channels * n_tp)
    attend_chunk(0)

    att_sq = jnp.zeros((rows, 1), F32)
    for h in range(heads):
        att = o_ref[h] / jnp.sum(l_ref[h], axis=1, keepdims=True)
        att_sq = att_sq + jnp.sum(att * att, axis=1, keepdims=True)
        at = slice(h * VDIM, (h + 1) * VDIM)
        ab[:, at] = (att * again[:, at]).astype(BF16)
    share_squares(1, att_sq)
    for c in range(SPLIT):
        for dy in range(1, n_y):
            hand_over(dy, c, product(dy, c, ab, woa))
    for c in range(SPLIT):
        for dy in range(1, n_y):
            send_pair(dy, c)
    join_squares(1, heads * VDIM * n_tp)

    for dy in range(1, n_y):
        def away(c, _):
            @pl.when(c < COLS)
            def _():
                produce(dy, c)

            @pl.when(c > SPLIT)
            def _():
                send_pair(dy, c - 1)

            return 0

        lax.fori_loop(SPLIT, COLS + 1, away, 0)

    for c in range(SPLIT):
        hand_over(0, c, product(0, c, ab, woa))

    def home(c, _):
        produce(0, c)
        return 0

    lax.fori_loop(SPLIT, COLS, home, 0)

    def gone(part, sem):
        remote(part, part, sem, own_sem.at[1], tp=partner).wait_send()

    with jax.named_scope("drain"):
        gone(tok.at[tp], own_sem.at[0])
        gone(tok.at[0 : n_y - 1], tok_tx)
        gone(tok.at[0 : n_y - 1], fwd_tx)
        for at in range(levels - 1):
            @pl.when(level == at)
            def _():
                count = (1 + at // 2) * min(2, levels - 1 - at)
                gone(kv.at[0:count, 0 : CHUNKS * hc], kvz_tx)

        settle(level + 1 - column, levels, lambda k: gone(kv.at[0:k, 0 : CHUNKS * hc], kvx_tx))
        settle(me, n_sp - 1, lambda k: gone(kv.at[0:k, 0 : CHUNKS * hc], kvd_tx))
        settle(n_sp - 1 - me, n_sp - 1, lambda k: gone(carry_rx.at[0:k], carry_s))
        gone(sq_rx.at[:, 1:n_tp], sq_s)

        @pl.when(me + 1 < n_sp)
        def _():
            tail_copy().wait_send()

    my_rows = pl.ds(pl.multiple_of(tp * rd, rd), rd)

    def summed(c):
        d2d_copy(0, c).wait_recv()
        value = own[0, c] + d2d_rx[0, c].astype(F32)
        for dy in range(1, n_y):
            y_copy(dy, c).wait_recv()
            value = value + y_rx[dy, c].astype(F32)
        return value

    @jax.named_scope("gather")
    def first_columns(c, total):
        count = cb // LANES
        value = summed(COLS + c) * wide(inv[0, my_rows, :], count)
        value = value + summed(c) * wide(inv[1, my_rows, :], count)
        mixed[c] = value
        return total + jnp.sum(value * value, axis=1, keepdims=True)

    @jax.named_scope("gather")
    def gather(c, total):
        value = summed(c)
        mixed[c] = value
        return total + jnp.sum(value * value, axis=1, keepdims=True)

    total = lax.fori_loop(0, SPLIT, first_columns, jnp.zeros((rd, 1), F32))
    total = lax.fori_loop(SPLIT, COLS, gather, total)

    def out_copy(at):
        return pltpu.make_async_copy(done.at[:, at], out_ref.at[:, at], out_sem)

    mark = jax.named_scope("final")
    mark.__enter__()
    last = lax.rsqrt(total * (1.0 / width) + EPS)

    for c in range(COLS):
        at = slice(c * cb, (c + 1) * cb)
        done[:, at] = (mixed[c] * last * pgain[:, at]).astype(BF16)
        out_copy(at).start()

    mark.__exit__(None, None, None)
    with jax.named_scope("outwait"):
        out_copy(slice(0, width)).wait()

    mark = jax.named_scope("sumsdone")
    mark.__enter__()

    gone(d2d_tx, d2d_s)
    gone(y_tx.at[1:n_y], y_s)
    mark.__exit__(None, None, None)


def shards(
    tokens, pre_gain, rate_factor, w_rec_in, w_rec_gate, conv_taps, rate_maps, input_maps,
    decay_param, w_query, w_latent, w_rope_key, latent_gain, w_expand, rec_gain, att_gain,
    w_out_rec, w_out_att, post_gain,
):
    n_sp = lax.axis_size("sp")
    n_tp = lax.axis_size("tp")
    n_y = n_tp // 2
    rows, feats = tokens.shape
    width = feats * n_tp
    channels = w_rec_in.shape[1]
    latent = w_latent.shape[1]
    q_cols = w_query.shape[1]
    heads = q_cols // (NOPE + ROPE)
    q_pad = -(-q_cols // LANES) * LANES
    rd = rows // n_tp
    cb = width // COLS

    lane = np.arange(LANES)
    frequency = np.where(lane < ROPE, THETA ** (-2.0 * (lane % (ROPE // 2)) / ROPE), 0.0)
    within = np.arange(rows)[:, None] * frequency
    start = rows * np.arange(n_sp)[:, None, None] * frequency
    turns = np.stack([np.cos(within), np.sin(within)]).astype(np.float32)
    starts = np.stack([np.cos(start), np.sin(start)]).astype(np.float32)

    def row(v):
        return v.reshape(1, -1)

    args = (
        tokens, pre_gain.reshape(n_tp, 1, feats), row(rate_factor), w_rec_in, w_rec_gate,
        conv_taps, rate_maps, input_maps, row(decay_param), w_query, w_latent, w_rope_key.T,
        row(latent_gain), w_expand, row(rec_gain), row(att_gain), w_out_rec, w_out_att,
        row(post_gain), jnp.asarray(turns), jnp.asarray(starts),
    )
    vm = pltpu.VMEM
    dma = pltpu.SemaphoreType.DMA

    def like(x):
        return vm(x.shape, x.dtype)

    scratch = [
        vm((n_tp, rows, feats), BF16), vm((rows, feats), BF16), like(args[1]), like(args[2]),
        vm((width, latent + 2 * channels + q_cols), BF16),
        like(args[5]), like(args[6]), like(args[7]), like(args[8]),
        like(args[11]), like(args[12]), like(args[13]),
        like(args[14]), like(args[15]), like(args[16]), like(args[17]), like(args[18]),
        like(args[19]), like(args[20]),
        vm((rows, latent), F32), vm((rows, LANES), F32), vm((rows, channels), F32),
        vm((rows, channels), F32), vm((rows, q_pad), F32), vm((rows, LANES), F32),
        vm((n_sp, rows, latent + LANES), BF16), vm((heads, rows, NOPE + LANES), BF16),
        vm((rows + 8, channels), F32), vm((rows, channels), F32),
        vm((heads, rows, LANES), F32), vm((heads, rows, LANES), F32), vm((heads, rows, VDIM), F32),
        vm((rows, channels), F32), vm((rows, channels), F32),
        vm((rows, channels), BF16), vm((rows, heads * VDIM), BF16),
        vm((8, channels), F32), vm((8, channels), F32), vm((8, channels), F32),
        vm((n_sp, 8, channels), F32), vm((2, 8, rows), F32), vm((2, n_tp, 8, rows), F32),
        vm((2, rows, LANES), F32),
        vm((n_y, COLS, 2 * rd, cb), F32), vm((2 * rd, cb), F32),
        vm((n_y, COLS + SPLIT, rd, cb), F32), vm((n_y, COLS + SPLIT, rd, cb), BF16),
        vm((n_y, COLS + SPLIT, rd, cb), BF16), vm((n_y, COLS + SPLIT, rd, cb), BF16),
        vm((n_y, COLS + SPLIT, rd, cb), BF16), vm((COLS, rd, cb), F32), vm((rd, width), BF16),
        dma, pltpu.SemaphoreType.REGULAR((max(1, (n_sp - 1) // 4 + 1),)),
        dma((16,)), dma((2, n_tp)), dma((2,)), dma, dma((n_y - 1, CHUNKS)),
        dma, dma((n_y - 1, CHUNKS)),
        dma, dma, dma, dma((n_sp // 2, CHUNKS)), dma((CHUNKS,)), dma((CHUNKS,)),
        dma((2,)), dma, dma, dma, dma((2,)),
        dma, dma((n_y, COLS + SPLIT)), dma, dma((n_y - 1, COLS + SPLIT)),
    ]
    return pl.pallas_call(
        functools.partial(fused_kernel, n_sp, n_tp, heads),
        out_shape=jax.ShapeDtypeStruct((rd, width), BF16),
        in_specs=[pl.BlockSpec(memory_space=pl.ANY)] * len(args),
        out_specs=pl.BlockSpec(memory_space=pl.ANY),
        scratch_shapes=scratch,
        compiler_params=pltpu.CompilerParams(
            collective_id=0, has_side_effects=True, vmem_limit_bytes=67043328
        ),
        name="layer",
    )(*args)


def solution(mesh):
    placed = (
        P("sp", "tp"),
        P(),
        P("sp"),
        P(None, "tp"),
        P(None, "tp"),
        P(None, "tp"),
        P("tp", None, None),
        P("tp", None, None),
        P("tp"),
        P(None, "tp"),
        P(),
        P(),
        P(),
        P(None, "tp"),
        P("tp"),
        P("tp"),
        P("tp", None),
        P("tp", None),
        P(),
    )
    return jax.shard_map(
        shards, mesh=mesh, in_specs=placed, out_specs=P(("sp", "tp"), None), check_vma=False
    )
```

```python
import functools
import math

import jax
import jax.numpy as jnp
import numpy as np
from jax import lax
from jax.experimental import pallas as pl
from jax.experimental.pallas import tpu as pltpu
from jax.sharding import PartitionSpec as P

NOPE = 128
ROPE = 64
VDIM = 128
LANES = 128

EPS = 1e-06
RATE_C = 8.0
THETA = 10000.0
CHUNKS = 4
BATCH = 8
SPLIT = 2
COLS = 4

MESH = pl.DeviceIdType.MESH
F32 = jnp.float32
BF16 = jnp.bfloat16


def one_minus_exp(y):
    series = 1.0 + y * (1.0 / 8.0)
    for order in (7, 6, 5, 4, 3, 2):
        series = 1.0 + y * (1.0 / order) * series
    return jnp.where(y > -0.5, -y * series, 1.0 - jnp.exp(y))


def gelu_tanh(x):
    inner = math.sqrt(2.0 / math.pi) * (x + 0.044715 * (x * x * x))
    return 0.5 * x * (1.0 + jnp.tanh(inner))


def softplus(x):
    z = jnp.exp(-jnp.abs(x))
    w = z / (2.0 + z)
    w2 = w * w
    series = jnp.full_like(w, 1.0 / 17.0)
    for order in (15, 13, 11, 9, 7, 5, 3):
        series = 1.0 / order + w2 * series
    return jnp.maximum(x, 0.0) + 2.0 * (w + w * w2 * series)


def rotate(tile, cosine, sine):
    lane = lax.broadcasted_iota(jnp.int32, tile.shape, 1)
    half = ROPE // 2
    other = jnp.where(
        lane < half, pltpu.roll(tile, tile.shape[1] - half, 1), pltpu.roll(tile, half, 1)
    )
    return tile * cosine + other * sine


def fused_kernel(
    n_sp, n_tp, heads,
    tokens, pre_gain, rate_factor, w_rec, w_gate, taps_in, rmap_in, imap_in, decay_in, w_query,
    w_latent, w_rope, lat_gain_in, w_expand, rec_gain_in, att_gain_in, w_or, w_oa, post_gain_in,
    turns_in, starts_in,
    out_ref,
    tok, scaled, gain, rate, wcat, taps, rmap, imap, decay, wrope, lgain, wexp,
    rgain, again, wor, woa, pgain, turns, starts,
    acc_lat, acc_rope, acc_rec, acc_gate, acc_q, sq, kv, qcat, padded, gated,
    m_ref, l_ref, o_ref, a_ref, b_ref, rb, ab,
    tail_tx, tail_rx, carry_tx, carry_rx, sq_tx, sq_rx, inv,
    prod, held, own, d2d_tx, d2d_rx, y_tx, y_rx, mixed, done, out_sem, known,
    load_sem, weight_sem, own_sem, tok_tx, tok_rx, fwd_tx, fwd_rx,
    kvz_tx, kvx_tx, kvd_tx, kvz_rx, kvx_rx, kvd_rx,
    tail_s, carry_s, carry_r, sq_s, sq_r, d2d_s, d2d_r, y_s, y_r,
):
    me = lax.axis_index("sp")
    tp = lax.axis_index("tp")
    n_y = n_tp // 2
    levels = n_sp // 2
    core = lax.rem(tp, 2)
    yy = lax.div(tp, 2)
    partner = tp + 1 - 2 * core
    column = lax.rem(me, 2)
    level = lax.div(me, 2)
    neighbour = me + 1 - 2 * column
    rows, feats = tokens.shape
    width = feats * n_tp
    latent = w_latent.shape[1]
    channels = w_rec.shape[1]
    rc = rows // CHUNKS
    hc = rc // 2
    rd = rows // n_tp
    cb = width // COLS

    small = (
        (tokens, tok.at[tp]), (pre_gain, gain), (lat_gain_in, lgain), (turns_in, turns),
        (starts_in, starts),
    )
    later = (
        (w_expand, wexp), (rate_factor, rate), (taps_in, taps), (rmap_in, rmap), (imap_in, imap),
        (decay_in, decay), (rec_gain_in, rgain), (att_gain_in, again), (w_or, wor), (w_oa, woa),
        (post_gain_in, pgain),
    )
    projections = []
    for s in (w_latent, w_rec, w_gate, w_query):
        first = projections[-1][2] if projections else 0
        projections.append((s, first, first + s.shape[1]))

    def loads_of(group, first):
        return [
            pltpu.make_async_copy(s, d, load_sem.at[first + i]) for i, (s, d) in enumerate(group)
        ]

    def features(blk):
        return pl.ds(pl.multiple_of(blk * feats, feats), feats)

    def rope_load(blk):
        at = features(blk)
        return pltpu.make_async_copy(w_rope.at[:, at], wrope.at[:, at], weight_sem.at[0, blk])

    def weight_loads(blk):
        at = features(blk)
        return [rope_load(blk)] + [
            pltpu.make_async_copy(s.at[at], wcat.at[at, first:last], weight_sem.at[1, blk])
            for s, first, last in projections
        ]

    def weights_ready(blk):
        at = features(blk)
        rope_load(blk).wait()
        pltpu.make_async_copy(wcat.at[at], wcat.at[at], weight_sem.at[1, blk]).wait()

    first_loads = loads_of(small, 0)
    last_loads = loads_of(later, len(small))
    for copy in first_loads:
        copy.start()

    def start_weights(dy):
        for b in range(2):
            for copy in weight_loads(2 * lax.rem(yy + dy, n_y) + lax.rem(core + b, 2)):
                copy.start()

    barrier = pltpu.get_barrier_semaphore()
    near = [o for step in (1, 2, 4) for o in (step, -step)]
    inside = [(me + o >= 0) & (me + o < n_sp) for o in near]
    near_count = functools.reduce(jnp.add, [x.astype(jnp.int32) for x in inside])

    def tell_near(sem):
        for o, x in zip(near, inside):
            @pl.when(x)
            def _():
                pl.semaphore_signal(
                    sem, inc=1, device_id={"sp": me + o}, device_id_type=MESH
                )

    rounds = known.shape[0]
    tell_near(barrier)
    for d in range(1, n_tp):
        pl.semaphore_signal(
            barrier, inc=1, device_id={"tp": lax.rem(tp + d, n_tp)}, device_id_type=MESH
        )
    with jax.named_scope("entry"):
        for ref in (acc_lat, acc_rope, acc_rec, acc_gate, acc_q, sq):
            ref[...] = jnp.zeros_like(ref)

        def blank(s, _):
            kv[s] = jnp.zeros(kv.shape[1:], BF16)
            return 0

        lax.fori_loop(me + 1, lax.div(me + BATCH - 1, BATCH) * BATCH, blank, 0)
        first_loads[0].wait()
        start_weights(0)
        pl.semaphore_wait(barrier, near_count + n_tp - 1)
        tell_near(known.at[0])

    def remote(src, dst, send, recv, **where):
        return pltpu.make_async_remote_copy(
            src_ref=src, dst_ref=dst, send_sem=send, recv_sem=recv, device_id=where,
            device_id_type=MESH,
        )

    def chunk(r):
        return pl.ds(pl.multiple_of(r * rc, rc), rc)

    def half(r):
        return pl.ds(pl.multiple_of(r * rc + core * hc, hc), hc)

    def own_copy():
        return remote(tok.at[tp], tok.at[tp], own_sem.at[0], own_sem.at[1], tp=partner)

    def tok_copy(dy, r):
        to = 2 * lax.rem(yy + dy, n_y) + core
        part = tok.at[tp, chunk(r)]
        return remote(part, part, tok_tx, tok_rx.at[dy - 1, r], tp=to)

    def fwd_copy(dy, r):
        part = tok.at[2 * lax.rem(yy + n_y - dy, n_y) + core, chunk(r)]
        return remote(part, part, fwd_tx, fwd_rx.at[dy - 1, r], tp=partner)

    for step in range(CHUNKS):
        for dy in range(1, n_y):
            tok_copy(dy, CHUNKS - 1 - step).start()
    own_copy().start()

    @jax.named_scope("tokwait")
    def pass_on(r):
        for dy in range(1, n_y):
            tok_copy(dy, r).wait_recv()
            fwd_copy(dy, r).start()

    def dot(a, b):
        return jnp.dot(a, b, preferred_element_type=F32)

    def dot_t(a, b):
        return lax.dot_general(a, b, (((1,), (1,)), ((), ())), preferred_element_type=F32)

    def tiles(x):
        return [x[:, i : i + LANES] for i in range(0, x.shape[1], LANES)]

    def wide(x, count):
        return jnp.concatenate([x] * count, axis=1) if count > 1 else x

    @jax.named_scope("scale")
    def scale_rows(blk, first, count):
        span = min(count, 32)

        def body(i, _):
            at = pl.ds(pl.multiple_of(first + i * span, span), span)
            x = tok[blk, at, :].astype(F32)
            scaled[at, :] = (x * gain[blk]).astype(BF16)
            sq[at, :] += functools.reduce(jnp.add, tiles(x * x))
            return 0

        lax.fori_loop(0, count // span, body, 0)

    @jax.named_scope("early")
    def project_early(blk, at):
        k = features(blk)
        x = scaled[at, :]
        acc_rope[at, : wrope.shape[0]] += dot_t(x, wrope[:, k])
        acc_lat[at, :] += dot(x, wcat[k, :latent])

    @jax.named_scope("late")
    def project_late(blk, at):
        k = features(blk)
        x = scaled[at, :]
        for (_, first, last), acc in zip(projections[1:], (acc_rec, acc_gate, acc_q)):
            acc[at, : last - first] += dot(x, wcat[k, first:last])

    for copy in first_loads[1:]:
        copy.wait()
    everything = pl.ds(0, rows)

    def own_chip(i, _):
        blk = 2 * yy + lax.rem(core + i, 2)

        @pl.when(i == 1)
        def _():
            own_copy().wait_recv()

        scale_rows(blk, 0, rows)
        with jax.named_scope("weights"):
            weights_ready(blk)

        @pl.when(i == 0)
        def _():
            for dy in range(1, n_y):
                start_weights(dy)

        project_early(blk, everything)
        project_late(blk, everything)
        return 0

    lax.fori_loop(0, 2, own_chip, 0)
    for copy in last_loads:
        copy.start()
    for k in range(rounds - 1):
        pl.semaphore_wait(known.at[k], near_count)
        tell_near(known.at[k + 1])

    def settle(count, most, wait):
        for k in range(1, most + 1):
            @pl.when(count == k)
            def _():
                wait(k)

    def upwards(s, r):
        part = kv.at[s, half(r)]
        for dz in range(1, min(3, levels)):
            @pl.when(level + dz < levels)
            def _():
                (
                    remote(part, part, kvz_tx, kvz_rx.at[level + dz - lax.div(s, 2), r], sp=me + 2 * dz)
                ).start()

    def kvx_copy(s, r):
        part = kv.at[s, half(r)]
        return remote(part, part, kvx_tx, kvx_rx.at[r], sp=neighbour)

    def kvd_copy(s, r):
        part = kv.at[s, half(r)]
        return remote(part, part, kvd_tx, kvd_rx.at[r], tp=partner)

    @jax.named_scope("fwdz")
    def forward_z(r, near, far):
        def body(dz, _):
            s = me - 2 * dz
            part = kv.at[s, half(r)]
            remote(part, part, kvz_tx, kvz_rx.at[dz, r], sp=neighbour).wait_recv()

            @pl.when(lax.rem(dz, 2) == 0)
            def _():
                upwards(s, r)

            kvx_copy(s, r).start()
            kvd_copy(s, r).start()
            return 0

        lax.fori_loop(near, jnp.minimum(far, level + 1), body, 0)

    @jax.named_scope("fwdx")
    def forward_x(r):
        def body(dz, _):
            kvd_copy(neighbour - 2 * dz, r).start()
            return 0

        def arrived(k):
            part = kv.at[0:k, 0:hc]
            remote(part, part, kvx_tx, kvx_rx.at[r], sp=neighbour).wait_recv()

        settle(level + column, levels, arrived)

        lax.fori_loop(1 - column, level + 1, body, 0)

    def angles(at):
        lane = lax.broadcasted_iota(jnp.int32, (1, LANES), 1)
        kept = jnp.where(lane < ROPE, 1.0, 0.0)
        sign = jnp.where(lane < ROPE // 2, -1.0, kept)
        c, s = turns[0, at, :], turns[1, at, :]
        c0, s0 = starts[0, me], starts[1, me]
        return (c * c0 - s * s0) * kept, (s * c0 + c * s0) * sign

    def inverse_of(at):
        total = jnp.sum(sq[at, :], axis=1, keepdims=True)
        return lax.rsqrt(total * (1.0 / width) + EPS)

    @jax.named_scope("latent")
    def finish_latent(r, at):
        inverse = inverse_of(at)
        cosine, sine = angles(at)
        raw = acc_lat[at, :] * inverse
        norm = raw * lax.rsqrt(jnp.mean(raw * raw, axis=1, keepdims=True) + EPS) * lgain[...]
        kv[me, at, :latent] = norm.astype(BF16)
        kv[me, at, latent:] = rotate(acc_rope[at, :] * inverse, cosine, sine).astype(BF16)
        upwards(me, r)

        @pl.when(column == 0)
        def _():
            kvx_copy(me, r).start()

    def tok_step(step, _):
        r = CHUNKS - 1 - step
        at = chunk(r)
        pass_on(r)

        for b in range(2):
            for dy in range(1, n_y):
                blk = 2 * lax.rem(yy + n_y - dy, n_y) + lax.rem(core + b, 2)
                if b == 1:
                    with jax.named_scope("fwdwait"):
                        fwd_copy(dy, r).wait_recv()
                    if dy == 1:
                        @pl.when(step > 1)
                        def _():
                            forward_z(r + 2, 2, 3)

                        @pl.when(step > 2)
                        def _():
                            forward_z(r + 3, 3, levels)

                scale_rows(blk, r * rc, rc)

                @pl.when(step == 0)
                def _():
                    weights_ready(blk)

                project_early(blk, at)
                if b == 1 and dy == n_y - 1:
                    finish_latent(r, at)
                project_late(blk, at)

        with jax.named_scope("finish"):
            inverse = inverse_of(at)
            cosine, sine = angles(at)
            low = (acc_rec[at, :] * inverse).astype(BF16)
            padded[pl.ds(pl.multiple_of(r * rc + 8, 8), rc), :] = low.astype(F32)
            gated[at, :] = gelu_tanh(acc_gate[at, :] * inverse)
            query = acc_q[at, :] * inverse
            total = query.shape[1]
            for h in range(heads):
                start = h * (NOPE + ROPE)
                turned = query if start == 0 else pltpu.roll(query, total - start, 1)
                qcat[h, at, :NOPE] = turned[:, :NOPE].astype(BF16)
                qcat[h, at, NOPE:] = rotate(turned[:, NOPE : NOPE + LANES], cosine, sine).astype(BF16)

        @pl.when(step == 0)
        def _():
            tail_tx[...] = padded[rows : rows + 8, :]

            @pl.when(me + 1 < n_sp)
            def _():
                tail_copy().start()

        @pl.when(step > 0)
        def _():
            forward_z(r + 1, 1, 2)

        return 0

    def tail_copy():
        return remote(tail_tx, tail_rx, tail_s.at[0], tail_s.at[1], sp=me + 1)

    lax.fori_loop(0, CHUNKS, tok_step, 0)

    forward_z(1, 2, 3)

    for copy in last_loads:
        copy.wait()

    @pl.when(me > 0)
    def _():
        tail_copy().wait_recv()
        padded[0:8, :] = tail_rx[...]

    @pl.when(me == 0)
    def _():
        padded[0:8, :] = jnp.zeros((8, channels), F32)

    mark = jax.named_scope("rec")
    mark.__enter__()
    count = taps.shape[0]
    conv = taps[0:1, :] * padded[9 - count : 9 - count + rows, :]
    for k in range(1, count):
        conv = conv + taps[k : k + 1, :] * padded[9 - count + k : 9 - count + k + rows, :]
    low = conv.astype(BF16)
    bw = rmap.shape[1]
    rates, entries = [], []
    for b in range(rmap.shape[0]):
        part = low[:, b * bw : (b + 1) * bw]
        rates.append(dot(part, rmap[b]))
        entries.append(dot(part, imap[b]))
    rate_gate = jax.nn.sigmoid(jnp.concatenate(rates, axis=1))
    entry = jax.nn.sigmoid(jnp.concatenate(entries, axis=1))
    eye = lax.broadcasted_iota(jnp.int32, (rows, rows), 0) == lax.broadcasted_iota(
        jnp.int32, (rows, rows), 1
    )

    def to_column(row):
        return jnp.sum(jnp.where(eye, row, 0.0), axis=1, keepdims=True)

    def to_row(col):
        return jnp.sum(jnp.where(eye, col, 0.0), axis=0, keepdims=True)

    log_keep = -RATE_C * to_column(rate[...]) * rate_gate * softplus(-decay[...])
    a = jnp.exp(log_keep)
    b = jnp.sqrt(one_minus_exp(2.0 * log_keep)) * entry * conv
    row = lax.broadcasted_iota(jnp.int32, (rows, channels), 0)
    d = 1
    while d < rows:
        inside = row >= d
        b = a * jnp.where(inside, pltpu.roll(b, d, 0), 0.0) + b
        a = a * jnp.where(inside, pltpu.roll(a, d, 0), 1.0)
        d *= 2
    a_ref[...] = a
    b_ref[...] = b
    carry_tx[...] = jnp.zeros_like(carry_tx)
    carry_tx[0:1, :] = a[rows - 1 :, :]
    carry_tx[1:2, :] = b[rows - 1 :, :]

    mark.__exit__(None, None, None)

    def carry_copy(d):
        return remote(
            carry_tx, carry_rx.at[me], carry_s, carry_r, sp=me + d
        )

    def carry_start(d, _):
        carry_copy(d).start()
        return 0

    pl.semaphore_wait(known.at[rounds - 1], near_count)
    lax.fori_loop(1, n_sp - me, carry_start, 0)

    power = 1.0 / (math.sqrt(NOPE + ROPE) * math.log(2.0))

    @jax.named_scope("attend")
    def attend(keys_latent, keys_rope, limit):
        expanded = dot(keys_latent, wexp[...]).astype(BF16)
        for h in range(heads):
            at = h * (NOPE + VDIM)
            keys = jnp.concatenate([expanded[:, at : at + NOPE], keys_rope], axis=1)
            values = expanded[:, at + NOPE : at + NOPE + VDIM]
            scores = dot_t(qcat[h], keys)
            if limit is None:
                q_at = lax.broadcasted_iota(jnp.int32, scores.shape, 0)
                k_at = lax.broadcasted_iota(jnp.int32, scores.shape, 1)
                scores = tiles(jnp.where(k_at <= q_at, scores, -jnp.inf))
            else:
                k_at = lax.broadcasted_iota(jnp.int32, (1, scores.shape[1]), 1)
                scores = tiles(scores + jnp.where(k_at < limit, 0.0, -jnp.inf))
            top = jnp.max(functools.reduce(jnp.maximum, scores), axis=1, keepdims=True)
            if limit is not None:
                old = m_ref[h]
                top = jnp.maximum(old, top)
                shrink = jnp.exp2((old - top) * power)
            weights = [jnp.exp2((x - top) * power) for x in scores]
            total = functools.reduce(jnp.add, weights)
            found = dot(jnp.concatenate([x.astype(BF16) for x in weights], axis=1), values)
            if limit is not None:
                total = total + l_ref[h] * shrink
                found = found + o_ref[h] * shrink
            m_ref[h] = jnp.broadcast_to(top, m_ref.shape[1:])
            l_ref[h] = total
            o_ref[h] = found

    @jax.named_scope("kvwait")
    def keys_ready(*chunks):
        for r in chunks:
            def ready(k):
                part = kv.at[0:k, 0:hc]
                remote(part, part, kvd_tx, kvd_rx.at[r], tp=partner).wait_recv()

            settle(me, n_sp - 1, ready)

    def attend_chunks(*chunks):
        span = len(chunks) * rc
        at = pl.ds(min(chunks) * rc, span)

        def several(first, blocks):
            these = pl.ds(first, blocks)
            count = blocks * span
            attend(
                kv[these, at, :latent].reshape(count, latent),
                kv[these, at, latent:].reshape(count, LANES),
                (me - first) * span,
            )

        @pl.when((me > 0) & (me <= BATCH // 2))
        def _():
            several(0, BATCH // 2)

        @pl.when(me > BATCH // 2)
        def _():
            def group(g, _):
                several(g * BATCH, BATCH)
                return 0

            lax.fori_loop(0, lax.div(me + BATCH - 1, BATCH), group, 0)

    def sq_copy(kind, d):
        return remote(
            sq_tx.at[kind], sq_rx.at[kind, d], sq_s, sq_r.at[kind], tp=lax.rem(tp + d, n_tp)
        )

    def share_squares(kind, column):
        sq_tx[kind] = jnp.broadcast_to(to_row(column), sq_tx.shape[1:])
        for d in range(1, n_tp):
            sq_copy(kind, d).start()

    @jax.named_scope("sums")
    def join_squares(kind, count):
        total = sq_tx[kind]
        part = sq_rx.at[kind, 1:n_tp]
        remote(part, part, sq_s, sq_r.at[kind], tp=partner).wait_recv()
        for d in range(1, n_tp):
            total = total + sq_rx[kind, d]
        scale = lax.rsqrt(total * (1.0 / count) + EPS)
        inv[kind] = jnp.broadcast_to(to_column(scale[0:1, :]), inv.shape[1:])

    @jax.named_scope("join")
    def finish_recurrence():
        def join(s, carried):
            return carry_rx[s, 0:1, :] * carried + carry_rx[s, 1:2, :]

        def arrived(k):
            part = carry_rx.at[0:k]
            remote(part, part, carry_s, carry_r, sp=neighbour).wait_recv()

        settle(me, n_sp - 1, arrived)
        carried = lax.fori_loop(0, me, join, jnp.zeros((1, channels), F32))
        rec_out = (b_ref[...] + a_ref[...] * carried) * gated[...]
        rb[...] = (rec_out * rgain[...]).astype(BF16)
        share_squares(0, jnp.sum(rec_out * rec_out, axis=1, keepdims=True))

    def block(dy):
        return pl.ds(pl.multiple_of(2 * rd * lax.rem(yy + dy, n_y), 2 * rd), 2 * rd)

    def cols(c):
        return pl.ds(pl.multiple_of(c * cb, cb), cb)

    @jax.named_scope("multiply")
    def multiply(dy, c, left, right, store):
        store[dy, c] = dot(left[block(dy), :], right[:, cols(c)])

    def d2d_copy(dy, c):
        return remote(
            d2d_tx.at[dy, c], d2d_rx.at[dy, c], d2d_s, d2d_r.at[dy, c], tp=partner
        )

    def y_copy(dy, c):
        to = 2 * lax.rem(yy + dy, n_y) + core
        return remote(y_tx.at[dy, c], y_rx.at[dy, c], y_s, y_r.at[dy - 1, c], tp=to)

    def hand_over(dy, c, value):
        held[...] = value
        theirs = pl.ds(pl.multiple_of((1 - core) * rd, rd), rd)
        mine = pl.ds(pl.multiple_of(core * rd, rd), rd)
        d2d_tx[dy, c] = held[theirs, :].astype(BF16)
        d2d_copy(dy, c).start()
        own[dy, c] = held[mine, :]

    def product(dy, c, left, right):
        return dot(left[block(dy), :], right[:, cols(c)])

    @jax.named_scope("produce")
    def produce(dy, c):
        at, count = block(dy), cb // LANES
        hand_over(
            dy, c,
            prod[dy, c] * wide(inv[0, at, :], count)
            + product(dy, c, ab, woa) * wide(inv[1, at, :], count),
        )

    @jax.named_scope("pair")
    def send_pair(dy, c):
        d2d_copy(dy, c).wait_recv()
        y_tx[dy, c] = (own[dy, c] + d2d_rx[dy, c].astype(F32)).astype(BF16)
        y_copy(dy, c).start()

    @jax.named_scope("multiply")
    def rec_products(dy):
        def body(c, _):
            prod[dy, c] = product(dy, c, rb, wor)
            return 0

        lax.fori_loop(SPLIT, COLS, body, 0)

    forward_z(2, 3, levels)
    forward_x(3)
    attend(kv[me, :, :latent], kv[me, :, latent:], None)
    forward_z(0, 1, 2)
    forward_z(0, 2, 3)
    forward_z(1, 3, levels)
    forward_x(2)
    finish_recurrence()
    for dy in range(1, n_y):
        for c in range(SPLIT):
            hand_over(dy, COLS + c, product(dy, c, rb, wor))
    forward_z(0, 3, levels)
    for dy in range(1, n_y):
        rec_products(dy)
    for c in range(SPLIT):
        hand_over(0, COLS + c, product(0, c, rb, wor))
    rec_products(0)
    keys_ready(3, 2)
    for dy in range(1, n_y):
        for c in range(SPLIT):
            send_pair(dy, COLS + c)
    forward_x(1)
    attend_chunks(3, 2)
    forward_x(0)
    keys_ready(1)
    attend_chunks(1)
    join_squares(0, channels * n_tp)
    keys_ready(0)
    attend_chunks(0)

    def finish_attention(at):
        squares = []
        for h in range(heads):
            att = o_ref[h, at, :] / jnp.sum(l_ref[h, at, :], axis=1, keepdims=True)
            squares.append(att * att)
            these = slice(h * VDIM, (h + 1) * VDIM)
            ab[at, these] = (att * again[:, these]).astype(BF16)
        sq[at, :] = functools.reduce(jnp.add, squares)

    for dy in range(1, n_y):
        finish_attention(block(dy))
        hand_over(dy, 0, product(dy, 0, ab, woa))
    finish_attention(block(0))
    share_squares(1, jnp.sum(sq[...], axis=1, keepdims=True))
    for c in range(SPLIT):
        for dy in range(1, n_y):
            if c > 0:
                hand_over(dy, c, product(dy, c, ab, woa))
    for c in range(SPLIT):
        for dy in range(1, n_y):
            send_pair(dy, c)
    join_squares(1, heads * VDIM * n_tp)

    for dy in range(1, n_y):
        def away(c, _):
            @pl.when(c < COLS)
            def _():
                produce(dy, c)

            @pl.when(c > SPLIT)
            def _():
                send_pair(dy, c - 1)

            return 0

        lax.fori_loop(SPLIT, COLS + 1, away, 0)

    for c in range(SPLIT):
        hand_over(0, c, product(0, c, ab, woa))

    def home(c, _):
        produce(0, c)
        return 0

    lax.fori_loop(SPLIT, COLS, home, 0)

    def gone(part, sem):
        remote(part, part, sem, own_sem.at[1], tp=partner).wait_send()

    with jax.named_scope("drain"):
        gone(tok.at[tp], own_sem.at[0])
        gone(tok.at[0 : n_y - 1], tok_tx)
        gone(tok.at[0 : n_y - 1], fwd_tx)
        for at in range(levels - 1):
            @pl.when(level == at)
            def _():
                count = (1 + at // 2) * min(2, levels - 1 - at)
                gone(kv.at[0:count, 0 : CHUNKS * hc], kvz_tx)

        settle(level + 1 - column, levels, lambda k: gone(kv.at[0:k, 0 : CHUNKS * hc], kvx_tx))
        settle(me, n_sp - 1, lambda k: gone(kv.at[0:k, 0 : CHUNKS * hc], kvd_tx))
        settle(n_sp - 1 - me, n_sp - 1, lambda k: gone(carry_rx.at[0:k], carry_s))
        gone(sq_rx.at[:, 1:n_tp], sq_s)

        @pl.when(me + 1 < n_sp)
        def _():
            tail_copy().wait_send()

    my_rows = pl.ds(pl.multiple_of(tp * rd, rd), rd)

    def summed(c):
        d2d_copy(0, c).wait_recv()
        value = own[0, c] + d2d_rx[0, c].astype(F32)
        for dy in range(1, n_y):
            y_copy(dy, c).wait_recv()
            value = value + y_rx[dy, c].astype(F32)
        return value

    @jax.named_scope("gather")
    def first_columns(c, total):
        count = cb // LANES
        value = summed(COLS + c) * wide(inv[0, my_rows, :], count)
        value = value + summed(c) * wide(inv[1, my_rows, :], count)
        mixed[c] = value
        return total + jnp.sum(value * value, axis=1, keepdims=True)

    @jax.named_scope("gather")
    def gather(c, total):
        value = summed(c)
        mixed[c] = value
        return total + jnp.sum(value * value, axis=1, keepdims=True)

    total = lax.fori_loop(0, SPLIT, first_columns, jnp.zeros((rd, 1), F32))
    total = lax.fori_loop(SPLIT, COLS, gather, total)

    def out_copy(at):
        return pltpu.make_async_copy(done.at[:, at], out_ref.at[:, at], out_sem)

    mark = jax.named_scope("final")
    mark.__enter__()
    last = lax.rsqrt(total * (1.0 / width) + EPS)

    for c in range(COLS):
        at = slice(c * cb, (c + 1) * cb)
        done[:, at] = (mixed[c] * last * pgain[:, at]).astype(BF16)
        out_copy(at).start()

    mark.__exit__(None, None, None)
    with jax.named_scope("outwait"):
        out_copy(slice(0, width)).wait()

    mark = jax.named_scope("sumsdone")
    mark.__enter__()

    gone(d2d_tx, d2d_s)
    gone(y_tx.at[1:n_y], y_s)
    mark.__exit__(None, None, None)


def shards(
    tokens, pre_gain, rate_factor, w_rec_in, w_rec_gate, conv_taps, rate_maps, input_maps,
    decay_param, w_query, w_latent, w_rope_key, latent_gain, w_expand, rec_gain, att_gain,
    w_out_rec, w_out_att, post_gain,
):
    n_sp = lax.axis_size("sp")
    n_tp = lax.axis_size("tp")
    n_y = n_tp // 2
    rows, feats = tokens.shape
    width = feats * n_tp
    channels = w_rec_in.shape[1]
    latent = w_latent.shape[1]
    q_cols = w_query.shape[1]
    heads = q_cols // (NOPE + ROPE)
    q_pad = -(-q_cols // LANES) * LANES
    rd = rows // n_tp
    cb = width // COLS

    lane = np.arange(LANES)
    frequency = np.where(lane < ROPE, THETA ** (-2.0 * (lane % (ROPE // 2)) / ROPE), 0.0)
    within = np.arange(rows)[:, None] * frequency
    start = rows * np.arange(n_sp)[:, None, None] * frequency
    turns = np.stack([np.cos(within), np.sin(within)]).astype(np.float32)
    starts = np.stack([np.cos(start), np.sin(start)]).astype(np.float32)

    def row(v):
        return v.reshape(1, -1)

    args = (
        tokens, pre_gain.reshape(n_tp, 1, feats), row(rate_factor), w_rec_in, w_rec_gate,
        conv_taps, rate_maps, input_maps, row(decay_param), w_query, w_latent, w_rope_key.T,
        row(latent_gain), w_expand, row(rec_gain), row(att_gain), w_out_rec, w_out_att,
        row(post_gain), jnp.asarray(turns), jnp.asarray(starts),
    )
    vm = pltpu.VMEM
    dma = pltpu.SemaphoreType.DMA

    def like(x):
        return vm(x.shape, x.dtype)

    scratch = [
        vm((n_tp, rows, feats), BF16), vm((rows, feats), BF16), like(args[1]), like(args[2]),
        vm((width, latent + 2 * channels + q_cols), BF16),
        like(args[5]), like(args[6]), like(args[7]), like(args[8]),
        like(args[11]), like(args[12]), like(args[13]),
        like(args[14]), like(args[15]), like(args[16]), like(args[17]), like(args[18]),
        like(args[19]), like(args[20]),
        vm((rows, latent), F32), vm((rows, LANES), F32), vm((rows, channels), F32),
        vm((rows, channels), F32), vm((rows, q_pad), F32), vm((rows, LANES), F32),
        vm((n_sp, rows, latent + LANES), BF16), vm((heads, rows, NOPE + LANES), BF16),
        vm((rows + 8, channels), F32), vm((rows, channels), F32),
        vm((heads, rows, LANES), F32), vm((heads, rows, LANES), F32), vm((heads, rows, VDIM), F32),
        vm((rows, channels), F32), vm((rows, channels), F32),
        vm((rows, channels), BF16), vm((rows, heads * VDIM), BF16),
        vm((8, channels), F32), vm((8, channels), F32), vm((8, channels), F32),
        vm((n_sp, 8, channels), F32), vm((2, 8, rows), F32), vm((2, n_tp, 8, rows), F32),
        vm((2, rows, LANES), F32),
        vm((n_y, COLS, 2 * rd, cb), F32), vm((2 * rd, cb), F32),
        vm((n_y, COLS + SPLIT, rd, cb), F32), vm((n_y, COLS + SPLIT, rd, cb), BF16),
        vm((n_y, COLS + SPLIT, rd, cb), BF16), vm((n_y, COLS + SPLIT, rd, cb), BF16),
        vm((n_y, COLS + SPLIT, rd, cb), BF16), vm((COLS, rd, cb), F32), vm((rd, width), BF16),
        dma, pltpu.SemaphoreType.REGULAR((max(1, (n_sp - 1) // 4 + 1),)),
        dma((16,)), dma((2, n_tp)), dma((2,)), dma, dma((n_y - 1, CHUNKS)),
        dma, dma((n_y - 1, CHUNKS)),
        dma, dma, dma, dma((n_sp // 2, CHUNKS)), dma((CHUNKS,)), dma((CHUNKS,)),
        dma((2,)), dma, dma, dma, dma((2,)),
        dma, dma((n_y, COLS + SPLIT)), dma, dma((n_y - 1, COLS + SPLIT)),
    ]
    return pl.pallas_call(
        functools.partial(fused_kernel, n_sp, n_tp, heads),
        out_shape=jax.ShapeDtypeStruct((rd, width), BF16),
        in_specs=[pl.BlockSpec(memory_space=pl.ANY)] * len(args),
        out_specs=pl.BlockSpec(memory_space=pl.ANY),
        scratch_shapes=scratch,
        compiler_params=pltpu.CompilerParams(
            collective_id=0, has_side_effects=True, vmem_limit_bytes=67043328
        ),
        name="layer",
    )(*args)


def solution(mesh):
    placed = (
        P("sp", "tp"),
        P(),
        P("sp"),
        P(None, "tp"),
        P(None, "tp"),
        P(None, "tp"),
        P("tp", None, None),
        P("tp", None, None),
        P("tp"),
        P(None, "tp"),
        P(),
        P(),
        P(),
        P(None, "tp"),
        P("tp"),
        P("tp"),
        P("tp", None),
        P("tp", None),
        P(),
    )
    return jax.shard_map(
        shards, mesh=mesh, in_specs=placed, out_specs=P(("sp", "tp"), None), check_vma=False
    )
```

```python
import functools
import math

import jax
import jax.numpy as jnp
import numpy as np
from jax import lax
from jax.experimental import pallas as pl
from jax.experimental.pallas import tpu as pltpu
from jax.sharding import PartitionSpec as P

NOPE = 128
ROPE = 64
VDIM = 128
LANES = 128

EPS = 1e-06
RATE_C = 8.0
THETA = 10000.0
CHUNKS = 4
BATCH = 8
SPLIT = 2
COLS = 4

MESH = pl.DeviceIdType.MESH
F32 = jnp.float32
BF16 = jnp.bfloat16


def one_minus_exp(y):
    series = 1.0 + y * (1.0 / 8.0)
    for order in (7, 6, 5, 4, 3, 2):
        series = 1.0 + y * (1.0 / order) * series
    return jnp.where(y > -0.5, -y * series, 1.0 - jnp.exp(y))


def gelu_tanh(x):
    inner = math.sqrt(2.0 / math.pi) * (x + 0.044715 * (x * x * x))
    return 0.5 * x * (1.0 + jnp.tanh(inner))


def softplus(x):
    z = jnp.exp(-jnp.abs(x))
    w = z / (2.0 + z)
    w2 = w * w
    series = jnp.full_like(w, 1.0 / 17.0)
    for order in (15, 13, 11, 9, 7, 5, 3):
        series = 1.0 / order + w2 * series
    return jnp.maximum(x, 0.0) + 2.0 * (w + w * w2 * series)


def rotate(tile, cosine, sine):
    lane = lax.broadcasted_iota(jnp.int32, tile.shape, 1)
    half = ROPE // 2
    other = jnp.where(
        lane < half, pltpu.roll(tile, tile.shape[1] - half, 1), pltpu.roll(tile, half, 1)
    )
    return tile * cosine + other * sine


def fused_kernel(
    n_sp, n_tp, heads,
    tokens, pre_gain, rate_factor, w_rec, w_gate, taps_in, rmap_in, imap_in, decay_in, w_query,
    w_latent, w_rope, lat_gain_in, w_expand, rec_gain_in, att_gain_in, w_or, w_oa, post_gain_in,
    turns_in, starts_in,
    out_ref,
    tok, scaled, gain, rate, wcat, taps, rmap, imap, decay, wrope, lgain, wexp,
    rgain, again, wor, woa, pgain, turns, starts,
    acc_lat, acc_rope, acc_rec, acc_gate, acc_q, sq, kv, qcat, padded, gated,
    m_ref, l_ref, o_ref, a_ref, b_ref, rb, ab,
    tail_tx, tail_rx, carry_tx, carry_rx, sq_tx, sq_rx, inv,
    prod, held, own, d2d_tx, d2d_rx, y_tx, y_rx, mixed, done, out_sem, known,
    load_sem, weight_sem, own_sem, tok_tx, tok_rx, fwd_tx, fwd_rx,
    kvz_tx, kvx_tx, kvd_tx, kvz_rx, kvx_rx, kvd_rx,
    tail_s, carry_s, carry_r, sq_s, sq_r, d2d_s, d2d_r, y_s, y_r,
):
    me = lax.axis_index("sp")
    tp = lax.axis_index("tp")
    n_y = n_tp // 2
    levels = n_sp // 2
    core = lax.rem(tp, 2)
    yy = lax.div(tp, 2)
    partner = tp + 1 - 2 * core
    column = lax.rem(me, 2)
    level = lax.div(me, 2)
    neighbour = me + 1 - 2 * column
    rows, feats = tokens.shape
    width = feats * n_tp
    latent = w_latent.shape[1]
    channels = w_rec.shape[1]
    rc = rows // CHUNKS
    hc = rc // 2
    rd = rows // n_tp
    cb = width // COLS

    small = (
        (tokens, tok.at[tp]), (pre_gain, gain), (lat_gain_in, lgain), (turns_in, turns),
        (starts_in, starts),
    )
    later = (
        (w_expand, wexp), (rate_factor, rate), (taps_in, taps), (rmap_in, rmap), (imap_in, imap),
        (decay_in, decay), (rec_gain_in, rgain), (att_gain_in, again), (w_or, wor), (w_oa, woa),
        (post_gain_in, pgain),
    )
    projections = []
    for s in (w_latent, w_rec, w_gate, w_query):
        first = projections[-1][2] if projections else 0
        projections.append((s, first, first + s.shape[1]))

    def loads_of(group, first):
        return [
            pltpu.make_async_copy(s, d, load_sem.at[first + i]) for i, (s, d) in enumerate(group)
        ]

    def features(blk):
        return pl.ds(pl.multiple_of(blk * feats, feats), feats)

    def rope_load(blk):
        at = features(blk)
        return pltpu.make_async_copy(w_rope.at[:, at], wrope.at[:, at], weight_sem.at[0, blk])

    def weight_loads(blk):
        at = features(blk)
        return [rope_load(blk)] + [
            pltpu.make_async_copy(s.at[at], wcat.at[at, first:last], weight_sem.at[1, blk])
            for s, first, last in projections
        ]

    def weights_ready(blk):
        at = features(blk)
        rope_load(blk).wait()
        pltpu.make_async_copy(wcat.at[at], wcat.at[at], weight_sem.at[1, blk]).wait()

    first_loads = loads_of(small, 0)
    last_loads = loads_of(later, len(small))
    for copy in first_loads:
        copy.start()

    def start_weights(dy):
        for b in range(2):
            for copy in weight_loads(2 * lax.rem(yy + dy, n_y) + lax.rem(core + b, 2)):
                copy.start()

    barrier = pltpu.get_barrier_semaphore()
    near = [o for step in (1, 2, 4) for o in (step, -step)]
    inside = [(me + o >= 0) & (me + o < n_sp) for o in near]
    near_count = functools.reduce(jnp.add, [x.astype(jnp.int32) for x in inside])

    def tell_near(sem):
        for o, x in zip(near, inside):
            @pl.when(x)
            def _():
                pl.semaphore_signal(
                    sem, inc=1, device_id={"sp": me + o}, device_id_type=MESH
                )

    rounds = known.shape[0]
    tell_near(barrier)
    for d in range(1, n_tp):
        pl.semaphore_signal(
            barrier, inc=1, device_id={"tp": lax.rem(tp + d, n_tp)}, device_id_type=MESH
        )
    with jax.named_scope("entry"):
        for ref in (acc_lat, acc_rope, acc_rec, acc_gate, acc_q, sq):
            ref[...] = jnp.zeros_like(ref)

        def blank(s, _):
            kv[s] = jnp.zeros(kv.shape[1:], BF16)
            return 0

        lax.fori_loop(me + 1, lax.div(me + BATCH - 1, BATCH) * BATCH, blank, 0)
        first_loads[0].wait()
        start_weights(0)
        pl.semaphore_wait(barrier, near_count + n_tp - 1)
        tell_near(known.at[0])

    def remote(src, dst, send, recv, **where):
        return pltpu.make_async_remote_copy(
            src_ref=src, dst_ref=dst, send_sem=send, recv_sem=recv, device_id=where,
            device_id_type=MESH,
        )

    def chunk(r):
        return pl.ds(pl.multiple_of(r * rc, rc), rc)

    def half(r):
        return pl.ds(pl.multiple_of(r * rc + core * hc, hc), hc)

    def own_copy():
        return remote(tok.at[tp], tok.at[tp], own_sem.at[0], own_sem.at[1], tp=partner)

    def tok_copy(dy, r):
        to = 2 * lax.rem(yy + dy, n_y) + core
        part = tok.at[tp, chunk(r)]
        return remote(part, part, tok_tx, tok_rx.at[dy - 1, r], tp=to)

    def fwd_copy(dy, r):
        part = tok.at[2 * lax.rem(yy + n_y - dy, n_y) + core, chunk(r)]
        return remote(part, part, fwd_tx, fwd_rx.at[dy - 1, r], tp=partner)

    for step in range(CHUNKS):
        for dy in range(1, n_y):
            tok_copy(dy, CHUNKS - 1 - step).start()
    own_copy().start()

    @jax.named_scope("tokwait")
    def pass_on(r):
        for dy in range(1, n_y):
            tok_copy(dy, r).wait_recv()
            fwd_copy(dy, r).start()

    def dot(a, b):
        return jnp.dot(a, b, preferred_element_type=F32)

    def dot_t(a, b):
        return lax.dot_general(a, b, (((1,), (1,)), ((), ())), preferred_element_type=F32)

    def tiles(x):
        return [x[:, i : i + LANES] for i in range(0, x.shape[1], LANES)]

    def wide(x, count):
        return jnp.concatenate([x] * count, axis=1) if count > 1 else x

    @jax.named_scope("scale")
    def scale_rows(blk, first, count):
        span = min(count, 32)

        def body(i, _):
            at = pl.ds(pl.multiple_of(first + i * span, span), span)
            x = tok[blk, at, :].astype(F32)
            scaled[at, :] = (x * gain[blk]).astype(BF16)
            sq[at, :] += functools.reduce(jnp.add, tiles(x * x))
            return 0

        lax.fori_loop(0, count // span, body, 0)

    @jax.named_scope("early")
    def project_early(blk, at):
        k = features(blk)
        x = scaled[at, :]
        acc_rope[at, : wrope.shape[0]] += dot_t(x, wrope[:, k])
        acc_lat[at, :] += dot(x, wcat[k, :latent])

    @jax.named_scope("late")
    def project_late(blk, at):
        k = features(blk)
        x = scaled[at, :]
        for (_, first, last), acc in zip(projections[1:], (acc_rec, acc_gate, acc_q)):
            acc[at, : last - first] += dot(x, wcat[k, first:last])

    for copy in first_loads[1:]:
        copy.wait()
    everything = pl.ds(0, rows)

    def own_chip(i, _):
        blk = 2 * yy + lax.rem(core + i, 2)

        @pl.when(i == 1)
        def _():
            own_copy().wait_recv()

        scale_rows(blk, 0, rows)
        with jax.named_scope("weights"):
            weights_ready(blk)

        @pl.when(i == 0)
        def _():
            for dy in range(1, n_y):
                start_weights(dy)

        project_early(blk, everything)
        project_late(blk, everything)
        return 0

    lax.fori_loop(0, 2, own_chip, 0)
    for copy in last_loads:
        copy.start()
    for k in range(rounds - 1):
        pl.semaphore_wait(known.at[k], near_count)
        tell_near(known.at[k + 1])

    def settle(count, most, wait):
        for k in range(1, most + 1):
            @pl.when(count == k)
            def _():
                wait(k)

    def upwards(s, r):
        part = kv.at[s, half(r)]
        for dz in range(1, min(3, levels)):
            @pl.when(level + dz < levels)
            def _():
                (
                    remote(part, part, kvz_tx, kvz_rx.at[level + dz - lax.div(s, 2), r], sp=me + 2 * dz)
                ).start()

    def kvx_copy(s, r):
        part = kv.at[s, half(r)]
        return remote(part, part, kvx_tx, kvx_rx.at[r], sp=neighbour)

    def kvd_copy(s, r):
        part = kv.at[s, half(r)]
        return remote(part, part, kvd_tx, kvd_rx.at[r], tp=partner)

    @jax.named_scope("fwdz")
    def forward_z(r, near, far):
        def body(dz, _):
            s = me - 2 * dz
            part = kv.at[s, half(r)]
            remote(part, part, kvz_tx, kvz_rx.at[dz, r], sp=neighbour).wait_recv()

            @pl.when(lax.rem(dz, 2) == 0)
            def _():
                upwards(s, r)

            kvx_copy(s, r).start()
            kvd_copy(s, r).start()
            return 0

        lax.fori_loop(near, jnp.minimum(far, level + 1), body, 0)

    @jax.named_scope("fwdx")
    def forward_x(r):
        def body(dz, _):
            kvd_copy(neighbour - 2 * dz, r).start()
            return 0

        def arrived(k):
            part = kv.at[0:k, 0:hc]
            remote(part, part, kvx_tx, kvx_rx.at[r], sp=neighbour).wait_recv()

        settle(level + column, levels, arrived)

        lax.fori_loop(1 - column, level + 1, body, 0)

    def angles(at):
        lane = lax.broadcasted_iota(jnp.int32, (1, LANES), 1)
        kept = jnp.where(lane < ROPE, 1.0, 0.0)
        sign = jnp.where(lane < ROPE // 2, -1.0, kept)
        c, s = turns[0, at, :], turns[1, at, :]
        c0, s0 = starts[0, me], starts[1, me]
        return (c * c0 - s * s0) * kept, (s * c0 + c * s0) * sign

    def inverse_of(at):
        total = jnp.sum(sq[at, :], axis=1, keepdims=True)
        return lax.rsqrt(total * (1.0 / width) + EPS)

    @jax.named_scope("latent")
    def finish_latent(r, at):
        inverse = inverse_of(at)
        cosine, sine = angles(at)
        raw = acc_lat[at, :] * inverse
        norm = raw * lax.rsqrt(jnp.mean(raw * raw, axis=1, keepdims=True) + EPS) * lgain[...]
        kv[me, at, :latent] = norm.astype(BF16)
        kv[me, at, latent:] = rotate(acc_rope[at, :] * inverse, cosine, sine).astype(BF16)
        upwards(me, r)

        @pl.when(column == 0)
        def _():
            kvx_copy(me, r).start()

    def tok_step(step, _):
        r = CHUNKS - 1 - step
        at = chunk(r)
        pass_on(r)

        for b in range(2):
            for dy in range(1, n_y):
                blk = 2 * lax.rem(yy + n_y - dy, n_y) + lax.rem(core + b, 2)
                if b == 1:
                    with jax.named_scope("fwdwait"):
                        fwd_copy(dy, r).wait_recv()
                    if dy == 1:
                        @pl.when(step > 1)
                        def _():
                            forward_z(r + 2, 2, 3)

                        @pl.when(step > 2)
                        def _():
                            forward_z(r + 3, 3, levels)

                scale_rows(blk, r * rc, rc)

                @pl.when(step == 0)
                def _():
                    weights_ready(blk)

                project_early(blk, at)
                if b == 1 and dy == n_y - 1:
                    finish_latent(r, at)
                project_late(blk, at)

        with jax.named_scope("finish"):
            inverse = inverse_of(at)
            cosine, sine = angles(at)
            low = (acc_rec[at, :] * inverse).astype(BF16)
            padded[pl.ds(pl.multiple_of(r * rc + 8, 8), rc), :] = low.astype(F32)
            gated[at, :] = gelu_tanh(acc_gate[at, :] * inverse)
            query = acc_q[at, :] * inverse
            total = query.shape[1]
            for h in range(heads):
                start = h * (NOPE + ROPE)
                turned = query if start == 0 else pltpu.roll(query, total - start, 1)
                qcat[h, at, :NOPE] = turned[:, :NOPE].astype(BF16)
                qcat[h, at, NOPE:] = rotate(turned[:, NOPE : NOPE + LANES], cosine, sine).astype(BF16)

        @pl.when(step == 0)
        def _():
            tail_tx[...] = padded[rows : rows + 8, :]

            @pl.when(me + 1 < n_sp)
            def _():
                tail_copy().start()

        @pl.when(step > 0)
        def _():
            forward_z(r + 1, 1, 2)

        return 0

    def tail_copy():
        return remote(tail_tx, tail_rx, tail_s.at[0], tail_s.at[1], sp=me + 1)

    lax.fori_loop(0, CHUNKS, tok_step, 0)

    forward_z(1, 2, 3)

    for copy in last_loads:
        copy.wait()

    @pl.when(me > 0)
    def _():
        tail_copy().wait_recv()
        padded[0:8, :] = tail_rx[...]

    @pl.when(me == 0)
    def _():
        padded[0:8, :] = jnp.zeros((8, channels), F32)

    mark = jax.named_scope("rec")
    mark.__enter__()
    count = taps.shape[0]
    conv = taps[0:1, :] * padded[9 - count : 9 - count + rows, :]
    for k in range(1, count):
        conv = conv + taps[k : k + 1, :] * padded[9 - count + k : 9 - count + k + rows, :]
    low = conv.astype(BF16)
    bw = rmap.shape[1]
    rates, entries = [], []
    for b in range(rmap.shape[0]):
        part = low[:, b * bw : (b + 1) * bw]
        rates.append(dot(part, rmap[b]))
        entries.append(dot(part, imap[b]))
    rate_gate = jax.nn.sigmoid(jnp.concatenate(rates, axis=1))
    entry = jax.nn.sigmoid(jnp.concatenate(entries, axis=1))
    eye = lax.broadcasted_iota(jnp.int32, (rows, rows), 0) == lax.broadcasted_iota(
        jnp.int32, (rows, rows), 1
    )

    def to_column(row):
        return jnp.sum(jnp.where(eye, row, 0.0), axis=1, keepdims=True)

    def to_row(col):
        return jnp.sum(jnp.where(eye, col, 0.0), axis=0, keepdims=True)

    log_keep = -RATE_C * to_column(rate[...]) * rate_gate * softplus(-decay[...])
    a = jnp.exp(log_keep)
    b = jnp.sqrt(one_minus_exp(2.0 * log_keep)) * entry * conv
    row = lax.broadcasted_iota(jnp.int32, (rows, channels), 0)
    d = 1
    while d < rows:
        inside = row >= d
        b = a * jnp.where(inside, pltpu.roll(b, d, 0), 0.0) + b
        a = a * jnp.where(inside, pltpu.roll(a, d, 0), 1.0)
        d *= 2
    a_ref[...] = a
    b_ref[...] = b
    carry_tx[...] = jnp.zeros_like(carry_tx)
    carry_tx[0:1, :] = a[rows - 1 :, :]
    carry_tx[1:2, :] = b[rows - 1 :, :]

    mark.__exit__(None, None, None)

    def carry_copy(d):
        return remote(
            carry_tx, carry_rx.at[me], carry_s, carry_r, sp=me + d
        )

    def carry_start(d, _):
        carry_copy(d).start()
        return 0

    pl.semaphore_wait(known.at[rounds - 1], near_count)
    lax.fori_loop(1, n_sp - me, carry_start, 0)

    power = 1.0 / (math.sqrt(NOPE + ROPE) * math.log(2.0))

    @jax.named_scope("attend")
    def attend(keys_latent, keys_rope, limit):
        expanded = dot(keys_latent, wexp[...]).astype(BF16)
        for h in range(heads):
            at = h * (NOPE + VDIM)
            keys = jnp.concatenate([expanded[:, at : at + NOPE], keys_rope], axis=1)
            values = expanded[:, at + NOPE : at + NOPE + VDIM]
            scores = dot_t(qcat[h], keys)
            if limit is None:
                q_at = lax.broadcasted_iota(jnp.int32, scores.shape, 0)
                k_at = lax.broadcasted_iota(jnp.int32, scores.shape, 1)
                scores = tiles(jnp.where(k_at <= q_at, scores, -jnp.inf))
            else:
                k_at = lax.broadcasted_iota(jnp.int32, (1, scores.shape[1]), 1)
                scores = tiles(scores + jnp.where(k_at < limit, 0.0, -jnp.inf))
            top = jnp.max(functools.reduce(jnp.maximum, scores), axis=1, keepdims=True)
            if limit is not None:
                old = m_ref[h]
                top = jnp.maximum(old, top)
                shrink = jnp.exp2((old - top) * power)
            weights = [jnp.exp2((x - top) * power) for x in scores]
            total = functools.reduce(jnp.add, weights)
            found = dot(jnp.concatenate([x.astype(BF16) for x in weights], axis=1), values)
            if limit is not None:
                total = total + l_ref[h] * shrink
                found = found + o_ref[h] * shrink
            m_ref[h] = jnp.broadcast_to(top, m_ref.shape[1:])
            l_ref[h] = total
            o_ref[h] = found

    @jax.named_scope("kvwait")
    def keys_ready(*chunks):
        for r in chunks:
            def ready(k):
                part = kv.at[0:k, 0:hc]
                remote(part, part, kvd_tx, kvd_rx.at[r], tp=partner).wait_recv()

            settle(me, n_sp - 1, ready)

    def attend_chunks(*chunks):
        span = len(chunks) * rc
        at = pl.ds(min(chunks) * rc, span)

        def several(first, blocks):
            these = pl.ds(first, blocks)
            count = blocks * span
            attend(
                kv[these, at, :latent].reshape(count, latent),
                kv[these, at, latent:].reshape(count, LANES),
                (me - first) * span,
            )

        @pl.when((me > 0) & (me <= BATCH // 2))
        def _():
            several(0, BATCH // 2)

        @pl.when(me > BATCH // 2)
        def _():
            def group(g, _):
                several(g * BATCH, BATCH)
                return 0

            lax.fori_loop(0, lax.div(me + BATCH - 1, BATCH), group, 0)

    def sq_copy(kind, d):
        return remote(
            sq_tx.at[kind], sq_rx.at[kind, d], sq_s, sq_r.at[kind], tp=lax.rem(tp + d, n_tp)
        )

    def share_squares(kind, column):
        sq_tx[kind] = jnp.broadcast_to(to_row(column), sq_tx.shape[1:])
        for d in range(1, n_tp):
            sq_copy(kind, d).start()

    @jax.named_scope("sums")
    def join_squares(kind, count):
        total = sq_tx[kind]
        part = sq_rx.at[kind, 1:n_tp]
        remote(part, part, sq_s, sq_r.at[kind], tp=partner).wait_recv()
        for d in range(1, n_tp):
            total = total + sq_rx[kind, d]
        scale = lax.rsqrt(total * (1.0 / count) + EPS)
        inv[kind] = jnp.broadcast_to(to_column(scale[0:1, :]), inv.shape[1:])

    @jax.named_scope("join")
    def finish_recurrence():
        def join(s, carried):
            return carry_rx[s, 0:1, :] * carried + carry_rx[s, 1:2, :]

        def arrived(k):
            part = carry_rx.at[0:k]
            remote(part, part, carry_s, carry_r, sp=neighbour).wait_recv()

        settle(me, n_sp - 1, arrived)
        carried = lax.fori_loop(0, me, join, jnp.zeros((1, channels), F32))
        rec_out = (b_ref[...] + a_ref[...] * carried) * gated[...]
        rb[...] = (rec_out * rgain[...]).astype(BF16)
        share_squares(0, jnp.sum(rec_out * rec_out, axis=1, keepdims=True))

    def block(dy):
        return pl.ds(pl.multiple_of(2 * rd * lax.rem(yy + dy, n_y), 2 * rd), 2 * rd)

    def cols(c):
        return pl.ds(pl.multiple_of(c * cb, cb), cb)

    @jax.named_scope("multiply")
    def multiply(dy, c, left, right, store):
        store[dy, c] = dot(left[block(dy), :], right[:, cols(c)])

    def d2d_copy(dy, c):
        return remote(
            d2d_tx.at[dy, c], d2d_rx.at[dy, c], d2d_s, d2d_r.at[dy, c], tp=partner
        )

    def y_copy(dy, c):
        to = 2 * lax.rem(yy + dy, n_y) + core
        return remote(y_tx.at[dy, c], y_rx.at[dy, c], y_s, y_r.at[dy - 1, c], tp=to)

    def hand_over(dy, c, value):
        held[...] = value
        theirs = pl.ds(pl.multiple_of((1 - core) * rd, rd), rd)
        mine = pl.ds(pl.multiple_of(core * rd, rd), rd)
        d2d_tx[dy, c] = held[theirs, :].astype(BF16)
        d2d_copy(dy, c).start()
        own[dy, c] = held[mine, :]

    def product(dy, c, left, right):
        return dot(left[block(dy), :], right[:, cols(c)])

    @jax.named_scope("produce")
    def produce(dy, c):
        at, count = block(dy), cb // LANES
        hand_over(
            dy, c,
            prod[dy, c] * wide(inv[0, at, :], count)
            + product(dy, c, ab, woa) * wide(inv[1, at, :], count),
        )

    @jax.named_scope("pair")
    def send_pair(dy, c):
        d2d_copy(dy, c).wait_recv()
        y_tx[dy, c] = (own[dy, c] + d2d_rx[dy, c].astype(F32)).astype(BF16)
        y_copy(dy, c).start()

    @jax.named_scope("multiply")
    def rec_products(dy):
        def body(c, _):
            prod[dy, c] = product(dy, c, rb, wor)
            return 0

        lax.fori_loop(SPLIT, COLS, body, 0)

    forward_z(2, 3, levels)
    forward_x(3)
    attend(kv[me, :, :latent], kv[me, :, latent:], None)
    forward_z(0, 1, 2)
    forward_z(0, 2, 3)
    forward_z(1, 3, levels)
    forward_x(2)
    finish_recurrence()
    for dy in range(1, n_y):
        for c in range(SPLIT):
            hand_over(dy, COLS + c, product(dy, c, rb, wor))
    forward_z(0, 3, levels)
    for dy in range(1, n_y):
        rec_products(dy)
    for c in range(SPLIT):
        hand_over(0, COLS + c, product(0, c, rb, wor))
    rec_products(0)
    keys_ready(3, 2)
    for dy in range(1, n_y):
        for c in range(SPLIT):
            send_pair(dy, COLS + c)
    forward_x(1)
    attend_chunks(3, 2)
    forward_x(0)
    join_squares(0, channels * n_tp)
    keys_ready(1, 0)
    attend_chunks(1, 0)

    def finish_attention(at):
        squares = []
        for h in range(heads):
            att = o_ref[h, at, :] / jnp.sum(l_ref[h, at, :], axis=1, keepdims=True)
            squares.append(att * att)
            these = slice(h * VDIM, (h + 1) * VDIM)
            ab[at, these] = (att * again[:, these]).astype(BF16)
        sq[at, :] = functools.reduce(jnp.add, squares)

    for dy in range(1, n_y):
        finish_attention(block(dy))
        hand_over(dy, 0, product(dy, 0, ab, woa))
    finish_attention(block(0))
    share_squares(1, jnp.sum(sq[...], axis=1, keepdims=True))
    for c in range(SPLIT):
        for dy in range(1, n_y):
            if c > 0:
                hand_over(dy, c, product(dy, c, ab, woa))
    for c in range(SPLIT):
        for dy in range(1, n_y):
            send_pair(dy, c)
    join_squares(1, heads * VDIM * n_tp)

    for dy in range(1, n_y):
        def away(c, _):
            @pl.when(c < COLS)
            def _():
                produce(dy, c)

            @pl.when(c > SPLIT)
            def _():
                send_pair(dy, c - 1)

            return 0

        lax.fori_loop(SPLIT, COLS + 1, away, 0)

    for c in range(SPLIT):
        hand_over(0, c, product(0, c, ab, woa))

    def home(c, _):
        produce(0, c)
        return 0

    lax.fori_loop(SPLIT, COLS, home, 0)

    def gone(part, sem):
        remote(part, part, sem, own_sem.at[1], tp=partner).wait_send()

    with jax.named_scope("drain"):
        gone(tok.at[tp], own_sem.at[0])
        gone(tok.at[0 : n_y - 1], tok_tx)
        gone(tok.at[0 : n_y - 1], fwd_tx)
        for at in range(levels - 1):
            @pl.when(level == at)
            def _():
                count = (1 + at // 2) * min(2, levels - 1 - at)
                gone(kv.at[0:count, 0 : CHUNKS * hc], kvz_tx)

        settle(level + 1 - column, levels, lambda k: gone(kv.at[0:k, 0 : CHUNKS * hc], kvx_tx))
        settle(me, n_sp - 1, lambda k: gone(kv.at[0:k, 0 : CHUNKS * hc], kvd_tx))
        settle(n_sp - 1 - me, n_sp - 1, lambda k: gone(carry_rx.at[0:k], carry_s))
        gone(sq_rx.at[:, 1:n_tp], sq_s)

        @pl.when(me + 1 < n_sp)
        def _():
            tail_copy().wait_send()

    my_rows = pl.ds(pl.multiple_of(tp * rd, rd), rd)

    def summed(c):
        d2d_copy(0, c).wait_recv()
        value = own[0, c] + d2d_rx[0, c].astype(F32)
        for dy in range(1, n_y):
            y_copy(dy, c).wait_recv()
            value = value + y_rx[dy, c].astype(F32)
        return value

    @jax.named_scope("gather")
    def first_columns(c, total):
        count = cb // LANES
        value = summed(COLS + c) * wide(inv[0, my_rows, :], count)
        value = value + summed(c) * wide(inv[1, my_rows, :], count)
        mixed[c] = value
        return total + jnp.sum(value * value, axis=1, keepdims=True)

    @jax.named_scope("gather")
    def gather(c, total):
        value = summed(c)
        mixed[c] = value
        return total + jnp.sum(value * value, axis=1, keepdims=True)

    total = lax.fori_loop(0, SPLIT, first_columns, jnp.zeros((rd, 1), F32))
    total = lax.fori_loop(SPLIT, COLS, gather, total)

    def out_copy(at):
        return pltpu.make_async_copy(done.at[:, at], out_ref.at[:, at], out_sem)

    mark = jax.named_scope("final")
    mark.__enter__()
    last = lax.rsqrt(total * (1.0 / width) + EPS)

    for c in range(COLS):
        at = slice(c * cb, (c + 1) * cb)
        done[:, at] = (mixed[c] * last * pgain[:, at]).astype(BF16)
        out_copy(at).start()

    mark.__exit__(None, None, None)
    with jax.named_scope("outwait"):
        out_copy(slice(0, width)).wait()

    mark = jax.named_scope("sumsdone")
    mark.__enter__()

    gone(d2d_tx, d2d_s)
    gone(y_tx.at[1:n_y], y_s)
    mark.__exit__(None, None, None)


def shards(
    tokens, pre_gain, rate_factor, w_rec_in, w_rec_gate, conv_taps, rate_maps, input_maps,
    decay_param, w_query, w_latent, w_rope_key, latent_gain, w_expand, rec_gain, att_gain,
    w_out_rec, w_out_att, post_gain,
):
    n_sp = lax.axis_size("sp")
    n_tp = lax.axis_size("tp")
    n_y = n_tp // 2
    rows, feats = tokens.shape
    width = feats * n_tp
    channels = w_rec_in.shape[1]
    latent = w_latent.shape[1]
    q_cols = w_query.shape[1]
    heads = q_cols // (NOPE + ROPE)
    q_pad = -(-q_cols // LANES) * LANES
    rd = rows // n_tp
    cb = width // COLS

    lane = np.arange(LANES)
    frequency = np.where(lane < ROPE, THETA ** (-2.0 * (lane % (ROPE // 2)) / ROPE), 0.0)
    within = np.arange(rows)[:, None] * frequency
    start = rows * np.arange(n_sp)[:, None, None] * frequency
    turns = np.stack([np.cos(within), np.sin(within)]).astype(np.float32)
    starts = np.stack([np.cos(start), np.sin(start)]).astype(np.float32)

    def row(v):
        return v.reshape(1, -1)

    args = (
        tokens, pre_gain.reshape(n_tp, 1, feats), row(rate_factor), w_rec_in, w_rec_gate,
        conv_taps, rate_maps, input_maps, row(decay_param), w_query, w_latent, w_rope_key.T,
        row(latent_gain), w_expand, row(rec_gain), row(att_gain), w_out_rec, w_out_att,
        row(post_gain), jnp.asarray(turns), jnp.asarray(starts),
    )
    vm = pltpu.VMEM
    dma = pltpu.SemaphoreType.DMA

    def like(x):
        return vm(x.shape, x.dtype)

    scratch = [
        vm((n_tp, rows, feats), BF16), vm((rows, feats), BF16), like(args[1]), like(args[2]),
        vm((width, latent + 2 * channels + q_cols), BF16),
        like(args[5]), like(args[6]), like(args[7]), like(args[8]),
        like(args[11]), like(args[12]), like(args[13]),
        like(args[14]), like(args[15]), like(args[16]), like(args[17]), like(args[18]),
        like(args[19]), like(args[20]),
        vm((rows, latent), F32), vm((rows, LANES), F32), vm((rows, channels), F32),
        vm((rows, channels), F32), vm((rows, q_pad), F32), vm((rows, LANES), F32),
        vm((n_sp, rows, latent + LANES), BF16), vm((heads, rows, NOPE + LANES), BF16),
        vm((rows + 8, channels), F32), vm((rows, channels), F32),
        vm((heads, rows, LANES), F32), vm((heads, rows, LANES), F32), vm((heads, rows, VDIM), F32),
        vm((rows, channels), F32), vm((rows, channels), F32),
        vm((rows, channels), BF16), vm((rows, heads * VDIM), BF16),
        vm((8, channels), F32), vm((8, channels), F32), vm((8, channels), F32),
        vm((n_sp, 8, channels), F32), vm((2, 8, rows), F32), vm((2, n_tp, 8, rows), F32),
        vm((2, rows, LANES), F32),
        vm((n_y, COLS, 2 * rd, cb), F32), vm((2 * rd, cb), F32),
        vm((n_y, COLS + SPLIT, rd, cb), F32), vm((n_y, COLS + SPLIT, rd, cb), BF16),
        vm((n_y, COLS + SPLIT, rd, cb), BF16), vm((n_y, COLS + SPLIT, rd, cb), BF16),
        vm((n_y, COLS + SPLIT, rd, cb), BF16), vm((COLS, rd, cb), F32), vm((rd, width), BF16),
        dma, pltpu.SemaphoreType.REGULAR((max(1, (n_sp - 1) // 4 + 1),)),
        dma((16,)), dma((2, n_tp)), dma((2,)), dma, dma((n_y - 1, CHUNKS)),
        dma, dma((n_y - 1, CHUNKS)),
        dma, dma, dma, dma((n_sp // 2, CHUNKS)), dma((CHUNKS,)), dma((CHUNKS,)),
        dma((2,)), dma, dma, dma, dma((2,)),
        dma, dma((n_y, COLS + SPLIT)), dma, dma((n_y - 1, COLS + SPLIT)),
    ]
    return pl.pallas_call(
        functools.partial(fused_kernel, n_sp, n_tp, heads),
        out_shape=jax.ShapeDtypeStruct((rd, width), BF16),
        in_specs=[pl.BlockSpec(memory_space=pl.ANY)] * len(args),
        out_specs=pl.BlockSpec(memory_space=pl.ANY),
        scratch_shapes=scratch,
        compiler_params=pltpu.CompilerParams(
            collective_id=0, has_side_effects=True, vmem_limit_bytes=67043328
        ),
        name="layer",
    )(*args)


def solution(mesh):
    placed = (
        P("sp", "tp"),
        P(),
        P("sp"),
        P(None, "tp"),
        P(None, "tp"),
        P(None, "tp"),
        P("tp", None, None),
        P("tp", None, None),
        P("tp"),
        P(None, "tp"),
        P(),
        P(),
        P(),
        P(None, "tp"),
        P("tp"),
        P("tp"),
        P("tp", None),
        P("tp", None),
        P(),
    )
    return jax.shard_map(
        shards, mesh=mesh, in_specs=placed, out_specs=P(("sp", "tp"), None), check_vma=False
    )
```
